32 devices in a mesh: sp: 4 (over y, x), tp: 8 (over z, core).
Axes of the slice: x: 2, y: 2, z: 4, core: 2. Of those that a mesh axis runs over, the one named last changes fastest.
Arguments:
- queries: bfloat16 [4096, 2048], P('sp', 'tp'), may hold values from -160 to 160
- key_heads: bfloat16 [4096, 512], P('sp'), may hold values from -8 to 8
- value_heads: bfloat16 [4096, 512], P('sp'), may hold values from -4 to 4
- sink_logit: float32 [16], P('tp'), may hold values from -2 to 7
- out_weight: bfloat16 [2048, 2048], P('tp'), may hold values from -0.125 to 0.125
- residual: bfloat16 [4096, 2048], P(('sp', 'tp')), may hold values from -6 to 6
- mixer_gain: float32 [2048], replicated, may hold values from 0.1 to 1.9
- expert_gain: float32 [2048], replicated, may hold values from 0.1 to 1.9
- route_group: int32 [4096], P(('sp', 'tp')), may hold values from 0 to 3, as said below
- route_member: int32 [4096, 2], P(('sp', 'tp')), may hold values from 0 to 2, as said below
- route_weight: bfloat16 [4096, 2], P(('sp', 'tp')), may hold values from 0.19921875 to 1
- gate_weight: bfloat16 [12, 2048, 2048], P('sp', None, 'tp'), may hold values from -0.125 to 0.125
- up_weight: bfloat16 [12, 2048, 2048], P('sp', None, 'tp'), may hold values from -0.125 to 0.125
- down_weight: bfloat16 [12, 2048, 2048], P('sp', 'tp'), may hold values from -0.125 to 0.125
Outputs:
- output: bfloat16 [4096, 2048], P(('sp', 'tp'))
The draws below stay inside these ranges and needn't reach their ends.
Inputs may be any that keep to these rules, and one draw needn't show every extreme that they name: `route_group`: among the tokens of one device, at most 40 name one group; in every draw one group is named by exactly 40 tokens of every device. `route_member`: the two entries of a token are different members of its group.
All inputs are finite; a program needn't handle non-finite values.
Results may differ from the reference program's by a relative error of at most 0.018.
Values may be sent and summed in bfloat16 or wider, within the bound.
A program may use at most 128 MiB of HBM per device.

```python
import jax
import jax.numpy as jnp
from jax import lax

D = 2048
HEADS = 16
KV_HEADS = 4
HEAD_DIM = 128
WINDOW = 128
BLOCK = 128
EXP_HID = 2048
GROUP_EXPERTS = 3
TOP = 2
TOK_DEV = 128
TOKENS = 4096
GROUPS = 4
EXPERTS = 12
GROUP_CAP = 40
N_TP = 8


def draw_key_heads(key, part):
    return jnp.clip(jax.random.normal(jax.random.fold_in(key, 37), (TOKENS, KV_HEADS * HEAD_DIM), jnp.float32), -4.0, 4.0).astype(jnp.bfloat16)


def draw_queries(key, part):
    drawn_rows = jnp.clip(jax.random.normal(jax.random.fold_in(key, 41), (TOKENS, HEADS * HEAD_DIM), jnp.float32), -4.0, 4.0)
    return drawn_rows.astype(jnp.bfloat16)


def route_table(key):
    base_key = jax.random.fold_in(key, 53)
    blocks = TOKENS // TOK_DEV
    slot_count = GROUPS * GROUP_CAP
    favored = jax.random.randint(jax.random.fold_in(base_key, 1), (), 0, GROUPS)

    def one_block(block_key):
        slot_order = jax.random.permutation(jax.random.fold_in(block_key, 1), slot_count)
        ranking = jnp.where(slot_order // GROUP_CAP == favored, 0, 1) * slot_count + jnp.arange(slot_count, dtype=jnp.int32)
        taken_slots = slot_order[jnp.argsort(ranking)][:TOK_DEV]
        shuffled = taken_slots[jax.random.permutation(jax.random.fold_in(block_key, 2), TOK_DEV)]
        chosen = shuffled // GROUP_CAP
        first_member = jax.random.randint(jax.random.fold_in(block_key, 3), (TOK_DEV,), 0, GROUP_EXPERTS)
        stepping = jax.random.randint(jax.random.fold_in(block_key, 4), (TOK_DEV,), 1, GROUP_EXPERTS)
        second = (first_member + stepping) % GROUP_EXPERTS
        return (chosen, jnp.stack([first_member, second], axis=1))
    block_keys = jax.random.split(jax.random.fold_in(base_key, 2), blocks)
    chosen, members = jax.vmap(one_block)(block_keys)
    return (chosen.reshape(TOKENS).astype(jnp.int32), members.reshape(TOKENS, TOP).astype(jnp.int32))


def draw_route_group(key, part):
    return route_table(key)[0]


def draw_route_member(key, part):
    return route_table(key)[1]


def block_scale(key, extent, pieces, smallest, top_value):
    def one(axis_at, shards_of):
        draws = jax.random.uniform(jax.random.fold_in(jax.random.fold_in(key, 6), axis_at), (shards_of,), jnp.float32, smallest / len(pieces), top_value / len(pieces))
        return jnp.repeat(jnp.exp(draws), extent[axis_at] // shards_of).reshape((-1,) + (1,) * (len(extent) - axis_at - 1))

    gain = one(*pieces[0])
    for cut in pieces[1:]:
        gain = gain * one(*cut)
    return gain


def noise(stream_key, extent, scale, most, cuts=(), kind=jnp.bfloat16):
    values = jax.random.normal(stream_key, extent, jnp.float32) * scale
    if len(cuts) > 0:
        values = block_scale(stream_key, extent, cuts, -0.22, 0.18) * values
    return jnp.clip(values, min=-most, max=most).astype(kind)


def setup_inputs(seed: int = 0) -> dict:
    arg_keys = jax.random.split(jax.random.key(seed), 15)
    return {
        "queries": draw_queries(jax.random.fold_in(arg_keys[14], 71), 0),
        "key_heads": draw_key_heads(jax.random.fold_in(arg_keys[14], 71), 0),
        "value_heads": noise(arg_keys[2], (TOKENS, KV_HEADS * HEAD_DIM), 1.0, 4.0, ((0, 4),)),
        "sink_logit": jnp.clip(-2.0 + 9.0 * jax.random.uniform(arg_keys[3], (HEADS,), jnp.float32) ** block_scale(arg_keys[3], (HEADS,), ((0, 8),), -0.2, 0.2), -2.0, 7.0),
        "out_weight": noise(arg_keys[4], (HEADS * HEAD_DIM, D), (HEADS * HEAD_DIM) ** -0.5, 0.125, ((0, 8),)),
        "residual": noise(arg_keys[5], (TOKENS, D), 1.0, 6.0, ((0, 32),)),
        "mixer_gain": jnp.clip(1.0 + 0.18 * jax.random.normal(arg_keys[6], (D,), jnp.float32), 0.1, 1.9),
        "expert_gain": jnp.clip(1.0 + 0.18 * jax.random.normal(arg_keys[7], (D,), jnp.float32), 0.1, 1.9),
        "route_group": draw_route_group(jax.random.fold_in(arg_keys[14], 71), 0),
        "route_member": draw_route_member(jax.random.fold_in(arg_keys[14], 71), 0),
        "route_weight": jnp.clip(0.19921875 + 0.80078125 * jax.random.uniform(arg_keys[10], (TOKENS, TOP), jnp.float32) ** block_scale(arg_keys[10], (TOKENS, TOP), ((0, 32),), -0.2, 0.2), 0.19921875, 1.0).astype(jnp.bfloat16),
        "gate_weight": noise(arg_keys[11], (EXPERTS, D, EXP_HID), D ** -0.5, 0.125, ((0, 4), (2, 8))),
        "up_weight": noise(arg_keys[12], (EXPERTS, D, EXP_HID), D ** -0.5, 0.125, ((0, 4), (2, 8))),
        "down_weight": noise(arg_keys[13], (EXPERTS, EXP_HID, D), EXP_HID ** -0.5, 0.125, ((0, 4), (1, 8))),
    }


EPS = 1e-06
NEG_BIG = -1e+30

def head_attention(queries, key_heads, value_heads, sink_logit):
    blocks = TOKENS // BLOCK
    span_rows = BLOCK + 2 * WINDOW
    key_group = HEADS // KV_HEADS
    query_pos = jnp.arange(TOKENS, dtype=jnp.int32).reshape(blocks, BLOCK)
    key_pos = (jnp.arange(blocks, dtype=jnp.int32) * BLOCK)[:, None] + jnp.arange(span_rows, dtype=jnp.int32)[None, :] - WINDOW
    inside = (jnp.abs(query_pos[:, :, None] - key_pos[:, None, :]) <= WINDOW) & (key_pos >= 0)[:, None, :] & (key_pos < TOKENS)[:, None, :]
    gather_at = jnp.clip(key_pos, 0, TOKENS - 1)

    def one_head(head_index):
        query_cols = lax.dynamic_slice_in_dim(queries, head_index * HEAD_DIM, HEAD_DIM, 1).reshape(blocks, BLOCK, HEAD_DIM)
        kv_start = head_index // key_group * HEAD_DIM
        key_cols = lax.dynamic_slice_in_dim(key_heads, kv_start, HEAD_DIM, 1)[gather_at]
        value_cols = lax.dynamic_slice_in_dim(value_heads, kv_start, HEAD_DIM, 1)[gather_at]
        scores = jnp.einsum('nqd,nkd->nqk', query_cols.astype(jnp.float32), key_cols.astype(jnp.float32)) * HEAD_DIM ** (-0.5)
        scores = jnp.where(inside, scores, NEG_BIG)
        sink_value = sink_logit[head_index].astype(jnp.float32)
        row_top = jnp.maximum(lax.optimization_barrier(jnp.max(scores, axis=2, keepdims=True)), sink_value)
        exp_terms = jnp.exp(scores - row_top)
        row_mass = lax.optimization_barrier(jnp.sum(exp_terms, axis=2, keepdims=True)) + jnp.exp(sink_value - row_top)
        weight = (exp_terms / row_mass).astype(jnp.bfloat16)
        result = jnp.einsum('nqk,nkd->nqd', weight.astype(jnp.float32), value_cols.astype(jnp.float32)).astype(jnp.bfloat16)
        return result.reshape(TOKENS, HEAD_DIM)
    per_head = lax.map(one_head, jnp.arange(HEADS, dtype=jnp.int32))
    return jnp.transpose(per_head, (1, 0, 2)).reshape(TOKENS, HEADS * HEAD_DIM)

def merge_heads(attended, out_weight):
    width = HEADS // N_TP * HEAD_DIM

    def add_block(block_index, running):
        columns = lax.dynamic_slice_in_dim(attended, block_index * width, width, 1)
        weight_rows = lax.dynamic_slice_in_dim(out_weight, block_index * width, width, 0)
        product = jnp.dot(columns, weight_rows, preferred_element_type=jnp.float32).astype(jnp.bfloat16)
        product = lax.optimization_barrier(product)
        return running + product.astype(jnp.float32)
    return lax.fori_loop(0, N_TP, add_block, jnp.zeros((TOKENS, D), jnp.float32))

def reference(queries, key_heads, value_heads, sink_logit, out_weight, residual, mixer_gain, expert_gain, route_group, route_member, route_weight, gate_weight, up_weight, down_weight):
    attended = head_attention(queries, key_heads, value_heads, sink_logit)
    projected = merge_heads(attended, out_weight)
    proj_scale = lax.rsqrt(lax.optimization_barrier(jnp.mean(projected * projected, axis=1, keepdims=True)) + EPS)
    mixed_rows = (residual.astype(jnp.float32) + mixer_gain.astype(jnp.float32) * (projected * proj_scale)).astype(jnp.bfloat16)
    mixed_float = mixed_rows.astype(jnp.float32)
    norm_scale = lax.rsqrt(lax.optimization_barrier(jnp.mean(mixed_float * mixed_float, axis=1, keepdims=True)) + EPS)
    normed = (mixed_float * norm_scale * expert_gain.astype(jnp.float32)).astype(jnp.bfloat16)
    blocks = TOKENS // TOK_DEV
    slots = blocks * GROUP_CAP
    grouped = route_group.reshape(blocks, TOK_DEV)
    chosen = (grouped[:, :, None] == jnp.arange(GROUPS, dtype=jnp.int32)[None, None, :]).astype(jnp.int32)
    group_rank = lax.optimization_barrier(jnp.sum(chosen * (jnp.cumsum(chosen, axis=1) - 1), axis=2))
    block_ids = jnp.arange(blocks, dtype=jnp.int32)[:, None]
    dest = (grouped * slots + block_ids * GROUP_CAP + group_rank).reshape(TOKENS).astype(jnp.int32)
    member_ids = jnp.arange(GROUP_EXPERTS, dtype=jnp.int32)
    token_gates = lax.optimization_barrier(jnp.sum(route_weight.astype(jnp.float32)[:, :, None] * (route_member[:, :, None] == member_ids[None, None, :]).astype(jnp.float32), axis=1))
    slot_rows = jnp.zeros((GROUPS * slots, D), jnp.bfloat16).at[dest].set(normed)
    slot_gates = jnp.zeros((GROUPS * slots, GROUP_EXPERTS), jnp.float32).at[dest].set(token_gates)
    hid_dev = EXP_HID // N_TP

    def group_experts(operands):
        rows_in, gates_in, gate_w, up_w, down_w = operands
        gate_pre = jnp.einsum('md,edh->meh', rows_in.astype(jnp.float32), gate_w.astype(jnp.float32))
        up_pre = jnp.einsum('md,edh->meh', rows_in.astype(jnp.float32), up_w.astype(jnp.float32))
        hidden = (jax.nn.silu(gate_pre) * up_pre * gates_in[:, :, None]).astype(jnp.bfloat16)
        hidden = hidden.reshape(slots, GROUP_EXPERTS, N_TP, hid_dev)
        down_blocks = down_w.reshape(GROUP_EXPERTS, N_TP, hid_dev, D)
        parts = jnp.einsum('mejh,ejhd->mjd', hidden.astype(jnp.float32), down_blocks.astype(jnp.float32))
        parts = lax.optimization_barrier(parts.astype(jnp.bfloat16))
        return lax.optimization_barrier(jnp.sum(parts.astype(jnp.float32), axis=1)).astype(jnp.bfloat16)
    group_out = lax.map(group_experts, (slot_rows.reshape(GROUPS, slots, D), slot_gates.reshape(GROUPS, slots, GROUP_EXPERTS), gate_weight.reshape(GROUPS, GROUP_EXPERTS, D, EXP_HID), up_weight.reshape(GROUPS, GROUP_EXPERTS, D, EXP_HID), down_weight.reshape(GROUPS, GROUP_EXPERTS, EXP_HID, D)))
    expert_out = group_out.reshape(GROUPS * slots, D)[dest]
    return (mixed_float + expert_out.astype(jnp.float32)).astype(jnp.bfloat16)
```

```python
import functools

import jax
import jax.numpy as jnp
from jax import lax
from jax.experimental import pallas as pl
from jax.experimental.pallas import tpu as pltpu
from jax.sharding import PartitionSpec as P

HEADS = 16
KV_HEADS = 4
HEAD_DIM = 128
WINDOW = 128
BLOCK = 128
GROUP_EXPERTS = 3


EPS = 1e-06
NEG_BIG = -1e30


def extended(block, sides, width):
    for axis, dim in sides:
        count = lax.axis_size(axis)
        forward = [(i, i + 1) for i in range(count - 1)]
        backward = [(target, source) for source, target in forward]
        low = lax.ppermute(
            lax.slice_in_dim(block, block.shape[dim] - width, None, axis=dim), axis, forward
        )
        high = lax.ppermute(lax.slice_in_dim(block, 0, width, axis=dim), axis, backward)
        block = jnp.concatenate([low, block, high], axis=dim)
    return block


def window_attention(queries, key_heads, value_heads, sink_logit):
    seq_rows = queries.shape[0]
    heads_dev = sink_logit.shape[0]
    key_group = HEADS // KV_HEADS
    key_start = lax.axis_index("tp") * heads_dev // key_group * HEAD_DIM
    key_own = lax.dynamic_slice_in_dim(key_heads, key_start, HEAD_DIM, 1)
    value_own = lax.dynamic_slice_in_dim(value_heads, key_start, HEAD_DIM, 1)
    padded = extended(jnp.stack([key_own, value_own]), (("sp", 1),), WINDOW)
    blocks = seq_rows // BLOCK
    extent = WINDOW // BLOCK
    tile_rows = padded.reshape(2, blocks + 2 * extent, BLOCK, HEAD_DIM)
    key_spans = jnp.concatenate(
        [tile_rows[:, shifted : shifted + blocks] for shifted in range(2 * extent + 1)], axis=2
    )
    offset = lax.axis_index("sp") * seq_rows
    seq_total = seq_rows * lax.axis_size("sp")
    query_pos = offset + jnp.arange(seq_rows, dtype=jnp.int32).reshape(blocks, BLOCK)
    key_pos = (
        offset
        + (jnp.arange(blocks, dtype=jnp.int32) * BLOCK)[:, None]
        + jnp.arange(BLOCK + 2 * WINDOW, dtype=jnp.int32)[None, :]
        - WINDOW
    )
    inside = (
        (jnp.abs(query_pos[:, :, None] - key_pos[:, None, :]) <= WINDOW)
        & (key_pos >= 0)[:, None, :]
        & (key_pos < seq_total)[:, None, :]
    )
    query_blocks = queries.reshape(blocks, BLOCK, heads_dev, HEAD_DIM)
    scores = jnp.einsum(
        "nqhd,nkd->nhqk", query_blocks, key_spans[0], preferred_element_type=jnp.float32
    ) * HEAD_DIM ** (-0.5)
    scores = jnp.where(inside[:, None], scores, NEG_BIG)
    sink_col = sink_logit[None, :, None, None]
    row_top = jnp.maximum(jnp.max(scores, axis=3, keepdims=True), sink_col)
    exp_terms = jnp.exp(scores - row_top)
    row_mass = jnp.sum(exp_terms, axis=3, keepdims=True) + jnp.exp(sink_col - row_top)
    weight = (exp_terms / row_mass).astype(jnp.bfloat16)
    attended = jnp.einsum(
        "nhqk,nkd->nqhd", weight, key_spans[1], preferred_element_type=jnp.float32
    ).astype(jnp.bfloat16)
    return attended.reshape(seq_rows, heads_dev * HEAD_DIM)


CORES = 2
LANES = 128
VMEM_SPEC = pl.BlockSpec(memory_space=pltpu.VMEM)


def places():
    count = lax.axis_size("tp") // CORES
    me = lax.axis_index("tp")
    chip, core = me // CORES, lax.rem(me, CORES)
    up = lax.rem(chip + 1, count) * CORES + core
    down = lax.rem(chip + count - 1, count) * CORES + core
    partner = chip * CORES + 1 - core
    return count, chip, core, (up, down), partner


def greet(neighbours, partner, peers):
    barrier = pltpu.get_barrier_semaphore()
    for target in (*neighbours, partner):
        pl.semaphore_signal(barrier, inc=1, device_id={"tp": target})
    for peer in peers:
        pl.semaphore_signal(barrier, inc=1, device_id={"sp": peer})
    pl.semaphore_wait(barrier, 3 + len(peers))


def column_halves(width):
    low = (width // LANES + 1) // 2 * LANES
    return (pl.ds(0, low), pl.ds(low, width - low)), (low, width - low)


def gather_sum_kernel(
    home, part_ref, out_ref, pair0, pair1, hold0, hold1, got0, got1, done,
    core_send, core_recv, ring_send, ring_recv, swap_send, swap_recv,
):
    count, chip, core, neighbours, partner = places()
    pieces = part_ref.shape[1]
    groups = lax.axis_size("sp")
    group = lax.axis_index("sp")
    if home:
        order = [lax.rem(group + j, groups) for j in range(groups)]
        order = order[1:] + order[:1]
        peers = order[:-1]
    else:
        order = list(range(pieces))
        peers = []
    greet(neighbours, partner, peers)
    halves, _ = column_halves(part_ref.shape[3])
    pair, hold, got = (pair0, pair1), (hold0, hold1), (got0, got1)

    def target(side, step):
        shift = count - 1 - step if side == 0 else 1 + step
        return lax.rem(chip + shift, count) * CORES

    def across(side, step, j):
        return pltpu.make_async_remote_copy(
            src_ref=part_ref.at[target(side, step) + 1 - core, order[j], :, halves[side]],
            dst_ref=pair[side].at[step, j],
            send_sem=core_send.at[side, step, j],
            recv_sem=core_recv.at[side, step, j],
            device_id={"tp": partner},
        )

    def ring(side, step, j):
        return pltpu.make_async_remote_copy(
            src_ref=hold[side].at[step, j],
            dst_ref=got[side].at[step, j],
            send_sem=ring_send.at[side, step, j],
            recv_sem=ring_recv.at[side, step, j],
            device_id={"tp": neighbours[side]},
        )

    def swap(j):
        return pltpu.make_async_remote_copy(
            src_ref=done.at[j],
            dst_ref=out_ref.at[group],
            send_sem=swap_send.at[j],
            recv_sem=swap_recv.at[j],
            device_id={"sp": order[j]},
        )

    for step in range(count):
        for j in range(pieces):
            for side in range(2):
                across(side, step, j).start()
    for step in range(count):
        for j in range(pieces):
            for side in range(2):
                across(side, step, j).wait_recv()
                value = part_ref[target(side, step) + core, order[j], :, halves[side]].astype(
                    jnp.float32
                ) + pair[side][step, j].astype(jnp.float32)
                if step > 0:
                    ring(side, step - 1, j).wait_recv()
                    value = value + got[side][step - 1, j].astype(jnp.float32)
                if step < count - 1:
                    hold[side][step, j] = value.astype(hold[side].dtype)
                    ring(side, step, j).start()
                elif home and j < pieces - 1:
                    done[j, :, halves[side]] = value.astype(done.dtype)
                else:
                    out_ref[order[j], :, halves[side]] = value.astype(out_ref.dtype)
            if home and step == count - 1 and j < pieces - 1:
                swap(j).start()
    for step in range(count):
        for j in range(pieces):
            for side in range(2):
                across(side, step, j).wait_send()
                if step < count - 1:
                    ring(side, step, j).wait_send()
    if home:
        for j in range(pieces - 1):
            swap(j).wait()


def gather_sum(part, home, out_type, collective_id):
    total, pieces, rows, width = part.shape
    count = total // CORES
    _, widths = column_halves(width)
    sem = pltpu.SemaphoreType.DMA
    kind = part.dtype
    return pl.pallas_call(
        functools.partial(gather_sum_kernel, home),
        out_shape=jax.ShapeDtypeStruct((pieces, rows, width), out_type),
        in_specs=[VMEM_SPEC],
        out_specs=VMEM_SPEC,
        scratch_shapes=[
            *[pltpu.VMEM((count, pieces, rows, w), kind) for w in widths],
            *[pltpu.VMEM((count, pieces, rows, w), kind) for w in widths],
            *[pltpu.VMEM((count, pieces, rows, w), kind) for w in widths],
            pltpu.VMEM((pieces, rows, width), kind),
            *[sem((2, count, pieces)) for _ in range(4)],
            sem((pieces,)),
            sem((pieces,)),
        ],
        compiler_params=pltpu.CompilerParams(
            collective_id=collective_id, has_side_effects=True
        ),
        name="home_sum" if home else "row_sum",
    )(part)


def line_sequence(i, position, length, side):
    reach = length - 1 - position if side == 0 else position
    early = i < reach
    offset = jnp.where(early, i + 1, 2 * reach - i)
    home = position + offset if side == 0 else position - offset
    return home, jnp.where(early, 0, 1)


def partner_slot(mine, j, groups):
    total, bit = 0, 1
    while bit < groups:
        total = total + lax.rem(mine // bit + j // bit, 2) * bit
        bit *= 2
    return total


def moe_kernel(
    send_ref, gate_hbm, up_hbm, down_hbm, out_ref,
    rows, res, pair, inc, gate_ref, up_ref, down_ref,
    weight_sem, own_sem, swap_send, swap_recv, line_send, line_recv, core_send, core_recv,
    pair_send, pair_recv, sum_send, sum_recv, home_send, home_recv,
):
    length = lax.axis_size("tp") // CORES
    tp = lax.axis_index("tp")
    z, core = tp // CORES, lax.rem(tp, CORES)
    partner = z * CORES + 1 - core
    groups = lax.axis_size("sp")
    group = lax.axis_index("sp")
    near = groups // 2
    width = out_ref.shape[2]
    last = length - 1
    sides = (
        (lax.rem(z + length - 1, length) * CORES + core, z > 0),
        (lax.rem(z + 1, length) * CORES + core, z < last),
    )
    peers = [partner_slot(group, j, groups) for j in range(groups)]

    weights = [
        pltpu.make_async_copy(source, place, weight_sem.at[n])
        for n, (source, place) in enumerate(
            ((gate_hbm, gate_ref), (up_hbm, up_ref), (down_hbm, down_ref))
        )
    ]
    for copy in weights:
        copy.start()

    @pl.when((z == 0) | (z == last))
    def _():
        for slot in range(length):
            @pl.when(slot != last * (z // last))
            def _():
                inc[slot] = jnp.zeros_like(inc[slot])

        @pl.when(z == 0)
        def _():
            inc[0] = jnp.zeros_like(inc[0])

        @pl.when(z == last)
        def _():
            inc[length] = jnp.zeros_like(inc[length])

    greet((sides[0][0], sides[1][0]), partner, peers[1:])

    def swap(j):
        return pltpu.make_async_remote_copy(
            src_ref=send_ref.at[peers[j]],
            dst_ref=rows.at[z * 2 + j // near, core, j % near],
            send_sem=swap_send.at[j],
            recv_sem=swap_recv.at[j],
            device_id={"sp": peers[j]},
        )

    def line(side, index, j):
        place = rows.at[index, core, j]
        return pltpu.make_async_remote_copy(
            src_ref=place,
            dst_ref=place,
            send_sem=line_send.at[side, index, j],
            recv_sem=line_recv.at[index, j],
            device_id={"tp": sides[side][0]},
        )

    def across(index, j):
        place = rows.at[index, core, j]
        return pltpu.make_async_remote_copy(
            src_ref=place,
            dst_ref=place,
            send_sem=core_send.at[index, j],
            recv_sem=core_recv.at[index, j],
            device_id={"tp": partner},
        )

    def share(index):
        return pltpu.make_async_remote_copy(
            src_ref=res.at[index, 1 - core],
            dst_ref=pair.at[index],
            send_sem=pair_send.at[index],
            recv_sem=pair_recv.at[index],
            device_id={"tp": partner},
        )

    def slot_of(side, target):
        if side == 1:
            return target
        return jnp.where(target == z - 1, length, target)

    def add_on(side, target, half, j):
        slot = slot_of(side, target)
        return pltpu.make_async_remote_copy(
            src_ref=res.at[target * 2 + half, core, j],
            dst_ref=inc.at[slot, half, j],
            send_sem=sum_send.at[target * 2 + half, j],
            recv_sem=sum_recv.at[slot, half, j],
            device_id={"tp": sides[side][0]},
        )

    def added(slot, half, j):
        return pltpu.make_async_remote_copy(
            src_ref=inc.at[slot, half, j],
            dst_ref=inc.at[slot, half, j],
            send_sem=sum_send.at[0, j],
            recv_sem=sum_recv.at[slot, half, j],
            device_id={"tp": partner},
        )

    def back(half, j):
        return pltpu.make_async_remote_copy(
            src_ref=res.at[z * 2 + half, core, j],
            dst_ref=out_ref.at[group],
            send_sem=home_send.at[half * near + j],
            recv_sem=home_recv.at[half * near + j],
            device_id={"sp": peers_at(half, j)},
        )

    def peers_at(half, j):
        return peers[half * near + j]

    def forward(side, index, j):
        @pl.when(sides[side][1])
        def _():
            line(side, index, j).start()

    own = pltpu.make_async_copy(send_ref.at[group], rows.at[z * 2, core, 0], own_sem)
    own.start()
    for j in range(1, groups):
        swap(j).start()
    for j in range(near):
        if j == 0:
            own.wait()
        else:
            swap(j).wait_recv()
        for side in range(2):
            forward(side, z * 2, j)
        across(z * 2, j).start()
    for j in range(near):
        swap(near + j).wait_recv()
        across(z * 2 + 1, j).start()
    for copy in weights:
        copy.wait()

    def expert_rows(index):
        for j in range(near):
            across(index, j).wait_recv()
        block = rows[index].reshape(2 * near * rows.shape[3], rows.shape[4])
        values = block[:, :width]
        gates = block[:, width:].astype(jnp.float32)
        hidden = []
        for member in range(gate_ref.shape[0]):
            gate_pre = jnp.dot(values, gate_ref[member], preferred_element_type=jnp.float32)
            up_pre = jnp.dot(values, up_ref[member], preferred_element_type=jnp.float32)
            value = gate_pre / (1.0 + jnp.exp(-gate_pre)) * up_pre * gates[:, member : member + 1]
            hidden.append(value.astype(jnp.bfloat16))
        total = jnp.dot(
            jnp.concatenate(hidden, axis=1), down_ref[...], preferred_element_type=jnp.float32
        )
        res[index] = total.astype(res.dtype).reshape(res.shape[1:])
        share(index).start()

    def pass_on(side, i):
        target, half = line_sequence(i, z, length, 1 - side)
        index = target * 2 + half
        share(index).wait_recv()
        for j in range(near):
            @pl.when(sides[1 - side][1])
            def _():
                added(target, half, j).wait_recv()
            value = (
                res[index, core, j].astype(jnp.float32)
                + pair[index, j].astype(jnp.float32)
                + inc[target, half, j].astype(jnp.float32)
            )
            res[index, core, j] = value.astype(res.dtype)
            add_on(side, target, half, j).start()

    def finish(half):
        index = z * 2 + half
        share(index).wait_recv()
        for j in range(near):
            @pl.when(z > 0)
            def _():
                added(z, half, j).wait_recv()

            @pl.when(z < last)
            def _():
                added(length, half, j).wait_recv()
            value = (
                res[index, core, j].astype(jnp.float32)
                + pair[index, j].astype(jnp.float32)
                + inc[z, half, j].astype(jnp.float32)
                + inc[length, half, j].astype(jnp.float32)
            ).astype(res.dtype)
            if half == 0 and j == 0:
                out_ref[group] = value
            else:
                res[index, core, j] = value
                back(half, j).start()

    reaches = (last - z, z)
    lags = tuple(jnp.where(depth == 0, 0, 2 * depth + 1) for depth in (last - z, z))

    def step(k, carry):
        for j in range(near):
            for side in range(2):
                home, half = line_sequence(k, z, length, side)

                @pl.when(k < 2 * reaches[side])
                def _(side=side, index=home * 2 + half, j=j):
                    line(side, index, j).wait_recv()
                    forward(side, index, j)
                    across(index, j).start()

                @pl.when(k == 2 * reaches[side])
                def _(side=side, j=j):
                    forward(side, z * 2 + 1, j)
        for side in range(2):
            i = k - lags[side]

            @pl.when((lags[side] > 0) & (i >= 0) & (i < 2 * reaches[1 - side]))
            def _(side=side, i=i):
                pass_on(side, i)

        def job(d, inner):
            home0, half0 = line_sequence(k, z, length, 0)
            home1, half1 = line_sequence(k, z, length, 1)
            index = jnp.where(
                d == 0, home0 * 2 + half0, jnp.where(d == 1, home1 * 2 + half1, z * 2 + k // 2)
            )
            live = jnp.where(
                d == 0, k < 2 * reaches[0],
                jnp.where(d == 1, k < 2 * reaches[1], (k == 0) | (k == 2)),
            )

            @pl.when(live)
            def _():
                expert_rows(index)

            return inner

        lax.fori_loop(0, 3, job, 0)
        for side in range(2):
            @pl.when((lags[side] == 0) & (k < 2 * reaches[1 - side]))
            def _(side=side):
                pass_on(side, k)

        @pl.when(k == 2 * jnp.maximum(z, last - z))
        def _():
            finish(0)

        return carry

    lax.fori_loop(0, 2 * length - 1, step, 0)
    finish(1)

    for j in range(1, groups):
        swap(j).wait_send()
        back(j // near, j % near).wait()

    def drain(index, carry):
        home = index // 2
        for j in range(near):
            @pl.when((home >= z) & sides[0][1])
            def _(j=j):
                line(0, index, j).wait_send()

            @pl.when((home <= z) & sides[1][1])
            def _(j=j):
                line(1, index, j).wait_send()

            across(index, j).wait_send()

            @pl.when(home != z)
            def _(j=j):
                add_on(1, home, lax.rem(index, 2), j).wait_send()
        share(index).wait_send()
        return carry

    lax.fori_loop(0, 2 * length, drain, 0)


def moe(send_rows, gate_weight, up_weight, down_weight):
    groups, capacity, padded = send_rows.shape
    members, width, hidden = gate_weight.shape
    length = lax.axis_size("tp") // CORES
    near = groups // 2
    kind = send_rows.dtype
    sem = pltpu.SemaphoreType.DMA
    hbm = pl.BlockSpec(memory_space=pl.ANY)
    total = 2 * length * groups * capacity
    return pl.pallas_call(
        moe_kernel,
        out_shape=jax.ShapeDtypeStruct((groups, capacity, width), kind),
        in_specs=[VMEM_SPEC, hbm, hbm, hbm],
        out_specs=VMEM_SPEC,
        scratch_shapes=[
            pltpu.VMEM((2 * length, 2, near, capacity, padded), kind),
            pltpu.VMEM((2 * length, 2, near, capacity, width), kind),
            pltpu.VMEM((2 * length, near, capacity, width), kind),
            pltpu.VMEM((length + 1, 2, near, capacity, width), kind),
            pltpu.VMEM((members, width, hidden), kind),
            pltpu.VMEM((members, width, hidden), kind),
            pltpu.VMEM((members * hidden, width), kind),
            sem((3,)),
            sem,
            sem((groups,)),
            sem((groups,)),
            sem((2, 2 * length, near)),
            sem((2 * length, near)),
            sem((2 * length, near)),
            sem((2 * length, near)),
            sem((2 * length,)),
            sem((2 * length,)),
            sem((2 * length, near)),
            sem((length + 1, 2, near)),
            sem((groups,)),
            sem((groups,)),
        ],
        compiler_params=pltpu.CompilerParams(
            collective_id=1, has_side_effects=True, vmem_limit_bytes=62 * 1024 * 1024
        ),
        cost_estimate=pl.CostEstimate(
            flops=6 * total * width * members * hidden,
            bytes_accessed=6 * members * hidden * width,
            transcendentals=total * members * hidden,
        ),
        name="moe",
    )(send_rows, gate_weight, up_weight, down_weight.reshape(members * hidden, width))


def per_device(
    queries,
    key_heads,
    value_heads,
    sink_logit,
    out_weight,
    residual,
    mixer_gain,
    expert_gain,
    route_group,
    route_member,
    route_weight,
    gate_weight,
    up_weight,
    down_weight,
):
    attended = window_attention(queries, key_heads, value_heads, sink_logit)
    tok_rows = residual.shape[0]
    width = out_weight.shape[1]
    parts = lax.axis_size("tp")
    pieces = 4 if tok_rows % 64 == 0 else 1
    product = jnp.dot(attended, out_weight, preferred_element_type=jnp.float32).astype(jnp.bfloat16)
    projected = gather_sum(
        product.reshape(parts, pieces, tok_rows // pieces, width), False, jnp.float32, 0
    ).reshape(tok_rows, width)
    proj_scale = lax.rsqrt(jnp.mean(projected * projected, axis=1, keepdims=True) + EPS)
    mixed_rows = (residual.astype(jnp.float32) + mixer_gain * (projected * proj_scale)).astype(
        jnp.bfloat16
    )
    mixed_float = mixed_rows.astype(jnp.float32)
    norm_scale = lax.rsqrt(jnp.mean(mixed_float * mixed_float, axis=1, keepdims=True) + EPS)
    normed = (mixed_float * norm_scale * expert_gain).astype(jnp.bfloat16)
    groups = lax.axis_size("sp")
    capacity = max(2, (5 * tok_rows + 4 * groups - 1) // (4 * groups))
    capacity = (capacity + 7) // 8 * 8
    group_ids = jnp.arange(groups, dtype=jnp.int32)
    chosen = (route_group[:, None] == group_ids[None, :]).astype(jnp.int32)
    group_rank = jnp.sum(chosen * (jnp.cumsum(chosen, axis=0) - 1), axis=1)
    slot_ids = route_group * capacity + group_rank
    placing = (jnp.arange(groups * capacity, dtype=jnp.int32)[:, None] == slot_ids[None, :]).astype(
        jnp.bfloat16
    )
    member_ids = jnp.arange(GROUP_EXPERTS, dtype=jnp.int32)
    token_gates = jnp.sum(
        route_weight.astype(jnp.float32)[:, :, None]
        * (route_member[:, :, None] == member_ids[None, None, :]).astype(jnp.float32),
        axis=1,
    ).astype(jnp.bfloat16)
    tail = jnp.pad(token_gates, ((0, 0), (0, LANES - GROUP_EXPERTS)))
    send_rows = (
        jnp.dot(placing, jnp.concatenate([normed, tail], axis=1), preferred_element_type=jnp.float32)
        .astype(jnp.bfloat16)
        .reshape(groups, capacity, width + LANES)
    )
    returned = moe(send_rows, gate_weight, up_weight, down_weight)
    expert_out = lax.dot_general(
        placing,
        returned.reshape(groups * capacity, width),
        (((0,), (0,)), ((), ())),
        preferred_element_type=jnp.float32,
    )
    return (mixed_float + expert_out).astype(jnp.bfloat16)


def solution(mesh):
    placed = (
        P("sp", "tp"),
        P("sp", None),
        P("sp", None),
        P("tp"),
        P("tp", None),
        P(("sp", "tp"), None),
        P(),
        P(),
        P(("sp", "tp")),
        P(("sp", "tp"), None),
        P(("sp", "tp"), None),
        P("sp", None, "tp"),
        P("sp", None, "tp"),
        P("sp", "tp", None),
    )
    return jax.shard_map(
        per_device, mesh=mesh, in_specs=placed, out_specs=P(("sp", "tp"), None), check_vma=False
    )
```

```python
import jax
import jax.numpy as jnp
from jax import lax
from jax.experimental import pallas as pl
from jax.experimental.pallas import tpu as pltpu
from jax.sharding import PartitionSpec as P

HEADS = 16
KV_HEADS = 4
HEAD_DIM = 128
WINDOW = 128
BLOCK = 128


EPS = 1e-06
NEG_BIG = -1e30


CORES = 2
LANES = 128
VMEM_BYTES = 67043328
VMEM_SPEC = pl.BlockSpec(memory_space=pltpu.VMEM)


def greet(neighbours, partner, peers):
    barrier = pltpu.get_barrier_semaphore()
    for target in (*neighbours, partner):
        pl.semaphore_signal(barrier, inc=1, device_id={"tp": target})
    for peer in peers:
        pl.semaphore_signal(barrier, inc=1, device_id={"sp": peer})
    pl.semaphore_wait(barrier, 3 + len(peers))


def line_sequence(i, position, length, side):
    reach = length - 1 - position if side == 0 else position
    early = i < reach
    offset = jnp.where(early, i + 1, 2 * reach - i)
    home = position + offset if side == 0 else position - offset
    return home, jnp.where(early, 0, 1)


def partner_slot(mine, j, groups):
    total, bit = 0, 1
    while bit < groups:
        total = total + lax.rem(mine // bit + j // bit, 2) * bit
        bit *= 2
    return total


def moe_kernel(
    send_ref, gate_hbm, up_hbm, down_hbm, out_ref,
    rows, res, pair, inc, gate_ref, up_ref, down_ref,
    weight_sem, own_sem, swap_send, swap_recv, line_send, line_recv, core_send, core_recv,
    pair_send, pair_recv, sum_send, sum_recv, home_send, home_recv,
):
    length = lax.axis_size("tp") // CORES
    tp = lax.axis_index("tp")
    z, core = tp // CORES, lax.rem(tp, CORES)
    partner = z * CORES + 1 - core
    groups = lax.axis_size("sp")
    group = lax.axis_index("sp")
    near = groups // 2
    width = out_ref.shape[2]
    last = length - 1
    sides = (
        (lax.rem(z + length - 1, length) * CORES + core, z > 0),
        (lax.rem(z + 1, length) * CORES + core, z < last),
    )
    peers = [partner_slot(group, j, groups) for j in range(groups)]

    weights = [
        pltpu.make_async_copy(source, place, weight_sem.at[n])
        for n, (source, place) in enumerate(
            ((gate_hbm, gate_ref), (up_hbm, up_ref), (down_hbm, down_ref))
        )
    ]
    for copy in weights:
        copy.start()

    @pl.when((z == 0) | (z == last))
    def _():
        for slot in range(length):
            @pl.when(slot != last * (z // last))
            def _():
                inc[slot] = jnp.zeros_like(inc[slot])

        @pl.when(z == 0)
        def _():
            inc[0] = jnp.zeros_like(inc[0])

        @pl.when(z == last)
        def _():
            inc[length] = jnp.zeros_like(inc[length])

    greet((sides[0][0], sides[1][0]), partner, peers[1:])

    def swap(j):
        return pltpu.make_async_remote_copy(
            src_ref=send_ref.at[peers[j]],
            dst_ref=rows.at[z * 2 + j // near, core, j % near],
            send_sem=swap_send.at[j],
            recv_sem=swap_recv.at[j],
            device_id={"sp": peers[j]},
        )

    def line(side, index, j):
        place = rows.at[index, core, j]
        return pltpu.make_async_remote_copy(
            src_ref=place,
            dst_ref=place,
            send_sem=line_send.at[side, index, j],
            recv_sem=line_recv.at[index, j],
            device_id={"tp": sides[side][0]},
        )

    def across(index, j):
        place = rows.at[index, core, j]
        return pltpu.make_async_remote_copy(
            src_ref=place,
            dst_ref=place,
            send_sem=core_send.at[index, j],
            recv_sem=core_recv.at[index, j],
            device_id={"tp": partner},
        )

    def share(index):
        return pltpu.make_async_remote_copy(
            src_ref=res.at[index, 1 - core],
            dst_ref=pair.at[index],
            send_sem=pair_send.at[index],
            recv_sem=pair_recv.at[index],
            device_id={"tp": partner},
        )

    def slot_of(side, target):
        if side == 1:
            return target
        return jnp.where(target == z - 1, length, target)

    def add_on(side, target, half, j):
        slot = slot_of(side, target)
        return pltpu.make_async_remote_copy(
            src_ref=res.at[target * 2 + half, core, j],
            dst_ref=inc.at[slot, half, j],
            send_sem=sum_send.at[target * 2 + half, j],
            recv_sem=sum_recv.at[slot, half, j],
            device_id={"tp": sides[side][0]},
        )

    def added(slot, half, j):
        return pltpu.make_async_remote_copy(
            src_ref=inc.at[slot, half, j],
            dst_ref=inc.at[slot, half, j],
            send_sem=sum_send.at[0, j],
            recv_sem=sum_recv.at[slot, half, j],
            device_id={"tp": partner},
        )

    def back(half, j):
        return pltpu.make_async_remote_copy(
            src_ref=res.at[z * 2 + half, core, j],
            dst_ref=out_ref.at[group],
            send_sem=home_send.at[half * near + j],
            recv_sem=home_recv.at[half * near + j],
            device_id={"sp": peers_at(half, j)},
        )

    def peers_at(half, j):
        return peers[half * near + j]

    def forward(side, index, j):
        @pl.when(sides[side][1])
        def _():
            line(side, index, j).start()

    own = pltpu.make_async_copy(send_ref.at[group], rows.at[z * 2, core, 0], own_sem)
    own.start()
    for j in range(1, groups):
        swap(j).start()
    for j in range(near):
        if j == 0:
            own.wait()
        else:
            swap(j).wait_recv()
        for side in range(2):
            forward(side, z * 2, j)
        across(z * 2, j).start()
    for j in range(near):
        swap(near + j).wait_recv()
        across(z * 2 + 1, j).start()
    for copy in weights:
        copy.wait()

    def expert_rows(index):
        for j in range(near):
            across(index, j).wait_recv()
        block = rows[index].reshape(2 * near * rows.shape[3], rows.shape[4])
        values = block[:, :width]
        gates = block[:, width:].astype(jnp.float32)
        hidden = []
        for member in range(gate_ref.shape[0]):
            gate_pre = jnp.dot(values, gate_ref[member], preferred_element_type=jnp.float32)
            up_pre = jnp.dot(values, up_ref[member], preferred_element_type=jnp.float32)
            value = gate_pre / (1.0 + jnp.exp(-gate_pre)) * up_pre * gates[:, member : member + 1]
            hidden.append(value.astype(jnp.bfloat16))
        total = jnp.dot(
            jnp.concatenate(hidden, axis=1), down_ref[...], preferred_element_type=jnp.float32
        )
        res[index] = total.astype(res.dtype).reshape(res.shape[1:])
        share(index).start()

    def pass_on(side, i):
        target, half = line_sequence(i, z, length, 1 - side)
        index = target * 2 + half
        share(index).wait_recv()
        for j in range(near):
            @pl.when(sides[1 - side][1])
            def _():
                added(target, half, j).wait_recv()
            value = (
                res[index, core, j].astype(jnp.float32)
                + pair[index, j].astype(jnp.float32)
                + inc[target, half, j].astype(jnp.float32)
            )
            res[index, core, j] = value.astype(res.dtype)
            add_on(side, target, half, j).start()

    def finish(half):
        index = z * 2 + half
        share(index).wait_recv()
        for j in range(near):
            @pl.when(z > 0)
            def _():
                added(z, half, j).wait_recv()

            @pl.when(z < last)
            def _():
                added(length, half, j).wait_recv()
            value = (
                res[index, core, j].astype(jnp.float32)
                + pair[index, j].astype(jnp.float32)
                + inc[z, half, j].astype(jnp.float32)
                + inc[length, half, j].astype(jnp.float32)
            ).astype(res.dtype)
            if half == 0 and j == 0:
                out_ref[group] = value
            else:
                res[index, core, j] = value
                back(half, j).start()

    reaches = (last - z, z)
    lags = tuple(jnp.where(depth == 0, 0, 2 * depth + 1) for depth in (last - z, z))

    def step(k, carry):
        for j in range(near):
            for side in range(2):
                home, half = line_sequence(k, z, length, side)

                @pl.when(k < 2 * reaches[side])
                def _(side=side, index=home * 2 + half, j=j):
                    line(side, index, j).wait_recv()
                    forward(side, index, j)
                    across(index, j).start()

                @pl.when(k == 2 * reaches[side])
                def _(side=side, j=j):
                    forward(side, z * 2 + 1, j)
        for side in range(2):
            i = k - lags[side]

            @pl.when((lags[side] > 0) & (i >= 0) & (i < 2 * reaches[1 - side]))
            def _(side=side, i=i):
                pass_on(side, i)

        def job(d, inner):
            home0, half0 = line_sequence(k, z, length, 0)
            home1, half1 = line_sequence(k, z, length, 1)
            index = jnp.where(
                d == 0, home0 * 2 + half0, jnp.where(d == 1, home1 * 2 + half1, z * 2 + k // 2)
            )
            live = jnp.where(
                d == 0, k < 2 * reaches[0],
                jnp.where(d == 1, k < 2 * reaches[1], (k == 0) | (k == 2)),
            )

            @pl.when(live)
            def _():
                expert_rows(index)

            return inner

        lax.fori_loop(0, 3, job, 0)
        for side in range(2):
            @pl.when((lags[side] == 0) & (k < 2 * reaches[1 - side]))
            def _(side=side):
                pass_on(side, k)

        @pl.when(k == 2 * jnp.maximum(z, last - z))
        def _():
            finish(0)

        return carry

    lax.fori_loop(0, 2 * length - 1, step, 0)
    finish(1)

    for j in range(1, groups):
        swap(j).wait_send()
        back(j // near, j % near).wait()

    def drain(index, carry):
        home = index // 2
        for j in range(near):
            @pl.when((home >= z) & sides[0][1])
            def _(j=j):
                line(0, index, j).wait_send()

            @pl.when((home <= z) & sides[1][1])
            def _(j=j):
                line(1, index, j).wait_send()

            across(index, j).wait_send()

            @pl.when(home != z)
            def _(j=j):
                add_on(1, home, lax.rem(index, 2), j).wait_send()
        share(index).wait_send()
        return carry

    lax.fori_loop(0, 2 * length, drain, 0)


def moe(send_rows, gate_weight, up_weight, down_weight):
    groups, capacity, padded = send_rows.shape
    members, width, hidden = gate_weight.shape
    length = lax.axis_size("tp") // CORES
    near = groups // 2
    kind = send_rows.dtype
    sem = pltpu.SemaphoreType.DMA
    hbm = pl.BlockSpec(memory_space=pltpu.HBM)
    total = 2 * length * groups * capacity
    return pl.pallas_call(
        moe_kernel,
        out_shape=jax.ShapeDtypeStruct((groups, capacity, width), kind),
        in_specs=[VMEM_SPEC, hbm, hbm, hbm],
        out_specs=VMEM_SPEC,
        scratch_shapes=[
            pltpu.VMEM((2 * length, 2, near, capacity, padded), kind),
            pltpu.VMEM((2 * length, 2, near, capacity, width), kind),
            pltpu.VMEM((2 * length, near, capacity, width), kind),
            pltpu.VMEM((length + 1, 2, near, capacity, width), kind),
            pltpu.VMEM((members, width, hidden), kind),
            pltpu.VMEM((members, width, hidden), kind),
            pltpu.VMEM((members * hidden, width), kind),
            sem((3,)),
            sem,
            sem((groups,)),
            sem((groups,)),
            sem((2, 2 * length, near)),
            sem((2 * length, near)),
            sem((2 * length, near)),
            sem((2 * length, near)),
            sem((2 * length,)),
            sem((2 * length,)),
            sem((2 * length, near)),
            sem((length + 1, 2, near)),
            sem((groups,)),
            sem((groups,)),
        ],
        compiler_params=pltpu.CompilerParams(
            collective_id=1, has_side_effects=True, vmem_limit_bytes=VMEM_BYTES
        ),
        cost_estimate=pl.CostEstimate(
            flops=6 * total * width * members * hidden,
            bytes_accessed=6 * members * hidden * width,
            transcendentals=total * members * hidden,
        ),
        name="moe",
    )(send_rows, gate_weight, up_weight, down_weight.reshape(members * hidden, width))


def front_kernel(
    query_hbm, key_hbm, value_hbm, sink_ref, weight_hbm, residual_hbm, mixer_hbm, expert_hbm,
    group_ref, member_ref, gate_ref,
    mixed_ref, rows_ref, placing_ref,
    query, span, attended, received, full, total, residual, gains,
    load_sem, halo_send, halo_recv, line_send, line_recv, plane_send, plane_recv,
    core_send, core_recv, row_send, row_recv,
):
    parts = lax.axis_size("tp")
    length = parts // CORES
    tp = lax.axis_index("tp")
    z, core = tp // CORES, lax.rem(tp, CORES)
    partner = z * CORES + 1 - core
    groups = lax.axis_size("sp")
    group = lax.axis_index("sp")
    last = length - 1
    halves = full.shape[2]
    relayed = groups == 4
    seq_rows = query.shape[0]
    heads_dev = query.shape[1] // HEAD_DIM
    blocks = seq_rows // BLOCK
    peers = [partner_slot(group, j, groups) for j in range(groups)]
    sides = (
        (lax.rem(z + length - 1, length) * CORES + core, z > 0),
        (lax.rem(z + 1, length) * CORES + core, z < last),
    )
    head_start = pl.multiple_of(tp * heads_dev // (HEADS // KV_HEADS) * HEAD_DIM, HEAD_DIM)
    inner = pl.ds(WINDOW, seq_rows)

    loads = [
        pltpu.make_async_copy(source, place, load_sem.at[n])
        for n, (source, place) in enumerate(
            (
                (weight_hbm, full.at[tp]),
                (key_hbm.at[:, pl.ds(head_start, HEAD_DIM)], span.at[0, inner]),
                (value_hbm.at[:, pl.ds(head_start, HEAD_DIM)], span.at[1, inner]),
                (query_hbm, query),
                (residual_hbm, residual),
                (mixer_hbm, gains.at[0]),
                (expert_hbm, gains.at[1]),
            )
        )
    ]
    for copy in loads:
        copy.start()

    @pl.when(group == 0)
    def _():
        span[:, :WINDOW] = jnp.zeros((2, WINDOW, HEAD_DIM), span.dtype)

    @pl.when(group == groups - 1)
    def _():
        span[:, WINDOW + seq_rows :] = jnp.zeros((2, WINDOW, HEAD_DIM), span.dtype)

    barrier = pltpu.get_barrier_semaphore()
    for shift in range(1, parts):
        pl.semaphore_signal(barrier, inc=1, device_id={"tp": lax.rem(tp + shift, parts)})
    for peer in peers[1:]:
        pl.semaphore_signal(barrier, inc=1, device_id={"sp": peer})
    pl.semaphore_wait(barrier, parts + groups - 2)

    def line(side, home, half):
        place = full.at[home * CORES + core, group, half]
        return pltpu.make_async_remote_copy(
            src_ref=place,
            dst_ref=place,
            send_sem=line_send.at[side, home, half],
            recv_sem=line_recv.at[home, half],
            device_id={"tp": sides[side][0]},
        )

    def plane(home, j, half, target, source):
        place = full.at[home * CORES + core, source, half]
        return pltpu.make_async_remote_copy(
            src_ref=place,
            dst_ref=place,
            send_sem=plane_send.at[home, j, half],
            recv_sem=plane_recv.at[home, j, half],
            device_id={"sp": target},
        )

    def relay(home, half):
        target, source = (peers[2], peers[1]) if half == 0 else (peers[1], peers[2])
        return plane(home, 3, half, target, source)

    def across(home):
        place = full.at[home * CORES + core]
        return pltpu.make_async_remote_copy(
            src_ref=place,
            dst_ref=place,
            send_sem=core_send.at[home],
            recv_sem=core_recv.at[home],
            device_id={"tp": partner},
        )

    def halo(side):
        start = WINDOW if side == 0 else seq_rows
        landing = WINDOW + seq_rows if side == 0 else 0
        return pltpu.make_async_remote_copy(
            src_ref=span.at[:, pl.ds(start, WINDOW)],
            dst_ref=span.at[:, pl.ds(landing, WINDOW)],
            send_sem=halo_send.at[side],
            recv_sem=halo_recv.at[side],
            device_id={"sp": lax.rem(group + (groups - 1 if side == 0 else 1), groups)},
        )

    def row_block(shift):
        target = lax.rem(tp + shift, parts)
        return pltpu.make_async_remote_copy(
            src_ref=attended.at[target],
            dst_ref=received.at[tp],
            send_sem=row_send.at[shift],
            recv_sem=row_recv.at[shift],
            device_id={"tp": target},
        )

    inward = (group > 0, group < groups - 1)
    loads[0].wait()
    for half in range(halves):
        for side in range(2):
            @pl.when(sides[side][1])
            def _(side=side, half=half):
                line(side, z, half).start()
    loads[1].wait()
    loads[2].wait()
    for side in range(2):
        @pl.when(inward[side])
        def _(side=side):
            halo(side).start()
    across(z).start()
    loads[3].wait()

    def attend(n, carry):
        b = jnp.where(n < blocks - 2, n + 1, jnp.where(n == blocks - 2, 0, blocks - 1))

        @pl.when(n == blocks - 2)
        def _():
            for side in range(2):
                @pl.when(inward[1 - side])
                def _(side=side):
                    halo(side).wait_recv()

        start = pl.multiple_of(b * BLOCK, BLOCK)
        wide = query[pl.ds(start, BLOCK), :]
        tall = jnp.concatenate(
            [wide[:, h * HEAD_DIM : (h + 1) * HEAD_DIM] for h in range(heads_dev)], axis=0
        )
        reach = BLOCK + 2 * WINDOW
        keys = span[0, pl.ds(start, reach), :]
        values = span[1, pl.ds(start, reach), :]
        scores = lax.dot_general(
            tall, keys, (((1,), (1,)), ((), ())), preferred_element_type=jnp.float32
        ) * HEAD_DIM ** (-0.5)
        shape = (heads_dev * BLOCK, reach)
        row = lax.broadcasted_iota(jnp.int32, shape, 0) % BLOCK
        column = lax.broadcasted_iota(jnp.int32, shape, 1)
        place = column + (group * seq_rows + b * BLOCK - WINDOW)
        inside = (
            (column >= row) & (column <= row + 2 * WINDOW)
            & (place >= 0) & (place < seq_rows * groups)
        )
        scores = jnp.where(inside, scores, NEG_BIG)
        which = lax.broadcasted_iota(jnp.int32, (heads_dev * BLOCK, 1), 0) // BLOCK
        sink = jnp.zeros((heads_dev * BLOCK, 1), jnp.float32)
        for h in range(heads_dev):
            sink = jnp.where(which == h, sink_ref[h], sink)
        top = jnp.maximum(jnp.max(scores, axis=1, keepdims=True), sink)
        terms = jnp.exp(scores - top)
        mass = jnp.sum(terms, axis=1, keepdims=True) + jnp.exp(sink - top)
        weight = (terms / mass).astype(jnp.bfloat16)
        result = jnp.dot(weight, values, preferred_element_type=jnp.float32).astype(jnp.bfloat16)
        attended[b] = jnp.concatenate(
            [result[h * BLOCK : (h + 1) * BLOCK] for h in range(heads_dev)], axis=1
        )
        return carry

    lax.fori_loop(0, blocks, attend, 0)
    received[tp] = attended[tp]

    def homes(i):
        return ((z + 1 + i, z + 1 + i <= last), (z - 1 - i, z - 1 - i >= 0))

    def spread_step(i):
        for side in range(2):
            home, live = homes(i)[side]

            @pl.when(live)
            def _(side=side, home=home):
                for half in range(halves):
                    line(side, home, half).wait_recv()

                    @pl.when(sides[side][1])
                    def _(half=half):
                        line(side, home, half).start()

                    if not relayed:
                        for j in range(1, groups):
                            plane(home, j, half, peers[j], group).start()
                if relayed:
                    for half in range(halves):
                        plane(home, 1, half, peers[1], group).start()
                        plane(home, 2, 1 - half, peers[2], group).start()

        if relayed:
            for side in range(2):
                home, live = homes(i)[side]

                @pl.when(live)
                def _(home=home):
                    for half in range(halves):
                        plane(home, 1 + half, half, peers[1], group).wait_recv()
                        relay(home, half).start()

    spread_step(0)
    for shift in range(1, parts):
        row_block(shift).start()
    for i in range(1, last):
        spread_step(i)

    slots = groups * rows_ref.shape[1]
    tok_rows = residual.shape[0]
    width = residual.shape[1]
    names = lax.broadcasted_iota(jnp.int32, (groups * (8 // min(groups, 8)), tok_rows), 0)
    chosen = (names == group_ref[...]).astype(jnp.float32)
    earlier = (
        lax.broadcasted_iota(jnp.int32, (tok_rows, tok_rows), 0)
        < lax.broadcasted_iota(jnp.int32, (tok_rows, tok_rows), 1)
    ).astype(jnp.bfloat16)
    rank = jnp.dot(chosen.astype(jnp.bfloat16), earlier, preferred_element_type=jnp.float32)
    slot_row = jnp.sum(
        chosen * (rank + (names * rows_ref.shape[1]).astype(jnp.float32)), axis=0, keepdims=True
    )
    placing = (
        lax.broadcasted_iota(jnp.int32, (slots, tok_rows), 0).astype(jnp.float32) == slot_row
    ).astype(jnp.bfloat16)
    placing_ref[...] = placing
    members = lax.broadcasted_iota(jnp.int32, (LANES, tok_rows), 0)
    tail = jnp.zeros((LANES, tok_rows), jnp.float32)
    for k in range(member_ref.shape[0]):
        tail = tail + jnp.where(
            members == member_ref[k : k + 1, :], gate_ref[k : k + 1, :].astype(jnp.float32), 0.0
        )
    rows_ref[:, :, width:] = (
        lax.dot_general(
            placing, tail.astype(jnp.bfloat16), (((1,), (1,)), ((), ())),
            preferred_element_type=jnp.float32,
        )
        .astype(rows_ref.dtype)
        .reshape(groups, rows_ref.shape[1], LANES)
    )

    def project(home, first):
        pieces = [received[home * CORES + c] for c in range(CORES)]
        lhs = jnp.concatenate(pieces, axis=1)
        rhs = jnp.concatenate(
            [full[home * CORES + c].reshape(-1, width) for c in range(CORES)], axis=0
        )
        part = jnp.dot(lhs, rhs, preferred_element_type=jnp.float32)
        if first:
            total[...] = part
        else:
            total[...] += part

    def rows_from(home):
        for c in range(CORES):
            source = home * CORES + c

            @pl.when(source != tp)
            def _(source=source):
                shift = lax.rem(tp - source + parts, parts)
                pltpu.make_async_remote_copy(
                    src_ref=attended.at[source],
                    dst_ref=received.at[source],
                    send_sem=row_send.at[0],
                    recv_sem=row_recv.at[lax.rem(parts + tp - source, parts)],
                    device_id={"tp": partner},
                ).wait_recv()

    across(z).wait_recv()
    rows_from(z)
    project(z, True)

    def gather_step(i, carry):
        for side in range(2):
            home, live = homes(i)[side]

            @pl.when(live)
            def _(home=home):
                for half in range(halves):
                    for j in range(1, groups):
                        if not (relayed and j == 1 + half and j < 3):
                            plane(home, j, half, peers[1], group).wait_recv()
                across(home).start()

        for side in range(2):
            home, live = homes(i)[side]

            @pl.when(live)
            def _(home=home):
                across(home).wait_recv()
                rows_from(home)
                project(home, False)

        return carry

    lax.fori_loop(0, last, gather_step, 0)

    for copy in loads[4:]:
        copy.wait()
    projected = total[...]
    scale = lax.rsqrt(jnp.mean(projected * projected, axis=1, keepdims=True) + EPS)
    mixed = (
        residual[...].astype(jnp.float32) + gains[0] * (projected * scale)
    ).astype(jnp.bfloat16)
    mixed_ref[...] = mixed
    mixed_float = mixed.astype(jnp.float32)
    norm = lax.rsqrt(jnp.mean(mixed_float * mixed_float, axis=1, keepdims=True) + EPS)
    normed = (mixed_float * norm * gains[1]).astype(jnp.bfloat16)
    rows_ref[:, :, :width] = (
        jnp.dot(placing, normed, preferred_element_type=jnp.float32)
        .astype(rows_ref.dtype)
        .reshape(groups, rows_ref.shape[1], width)
    )

    for side in range(2):
        @pl.when(inward[side])
        def _(side=side):
            halo(side).wait_send()
    for shift in range(1, parts):
        row_block(shift).wait_send()

    def drain(home, carry):
        for half in range(halves):
            @pl.when((home >= z) & sides[0][1])
            def _(half=half):
                line(0, home, half).wait_send()

            @pl.when((home <= z) & sides[1][1])
            def _(half=half):
                line(1, home, half).wait_send()

            @pl.when(home != z)
            def _(half=half):
                for j in range(1, groups):
                    plane(home, j, half, peers[1], group).wait_send()

        across(home).wait_send()
        return carry

    lax.fori_loop(0, length, drain, 0)


def front(
    queries, key_heads, value_heads, sink_logit, out_weight, residual, mixer_gain, expert_gain,
    route_group, route_member, route_weight, capacity,
):
    parts, groups = lax.axis_size("tp"), lax.axis_size("sp")
    length = parts // CORES
    seq_rows, columns = queries.shape
    tok_rows, width = residual.shape
    halves = 2 if groups == 4 else 1
    piece = columns // (groups * halves)
    sem = pltpu.SemaphoreType.DMA
    kind = queries.dtype
    hbm = pl.BlockSpec(memory_space=pltpu.HBM)
    return pl.pallas_call(
        front_kernel,
        out_shape=(
            jax.ShapeDtypeStruct((tok_rows, width), kind),
            jax.ShapeDtypeStruct((groups, capacity, width + LANES), kind),
            jax.ShapeDtypeStruct((groups * capacity, tok_rows), kind),
        ),
        in_specs=[hbm, hbm, hbm, pl.BlockSpec(memory_space=pltpu.SMEM), hbm, hbm, hbm, hbm,
                  VMEM_SPEC, VMEM_SPEC, VMEM_SPEC],
        out_specs=(VMEM_SPEC, VMEM_SPEC, VMEM_SPEC),
        scratch_shapes=[
            pltpu.VMEM((seq_rows, columns), kind),
            pltpu.VMEM((2, seq_rows + 2 * WINDOW, HEAD_DIM), kind),
            pltpu.VMEM((parts, tok_rows, columns), kind),
            pltpu.VMEM((parts, tok_rows, columns), kind),
            pltpu.VMEM((parts, groups, halves, piece, width), kind),
            pltpu.VMEM((tok_rows, width), jnp.float32),
            pltpu.VMEM((tok_rows, width), kind),
            pltpu.VMEM((2, 1, width), jnp.float32),
            sem((7,)),
            sem((2,)),
            sem((2,)),
            sem((2, length, halves)),
            sem((length, halves)),
            sem((length, groups, halves)),
            sem((length, groups, halves)),
            sem((length,)),
            sem((length,)),
            sem((parts,)),
            sem((parts,)),
        ],
        compiler_params=pltpu.CompilerParams(
            collective_id=0, has_side_effects=True, vmem_limit_bytes=VMEM_BYTES
        ),
        name="front",
    )(
        queries, key_heads, value_heads, sink_logit,
        out_weight.reshape(groups, halves, piece, width),
        residual, mixer_gain.reshape(1, width), expert_gain.reshape(1, width),
        route_group.reshape(1, tok_rows), route_member.T, route_weight.T,
    )


def per_device(
    queries,
    key_heads,
    value_heads,
    sink_logit,
    out_weight,
    residual,
    mixer_gain,
    expert_gain,
    route_group,
    route_member,
    route_weight,
    gate_weight,
    up_weight,
    down_weight,
):
    tok_rows, width = residual.shape
    groups = lax.axis_size("sp")
    capacity = max(2, (5 * tok_rows + 4 * groups - 1) // (4 * groups))
    capacity = (capacity + 7) // 8 * 8
    mixed_rows, send_rows, placing = front(
        queries, key_heads, value_heads, sink_logit, out_weight, residual, mixer_gain,
        expert_gain, route_group, route_member, route_weight, capacity,
    )
    returned = moe(send_rows, gate_weight, up_weight, down_weight)
    expert_out = lax.dot_general(
        placing,
        returned.reshape(groups * capacity, width),
        (((0,), (0,)), ((), ())),
        preferred_element_type=jnp.float32,
    )
    return (mixed_rows.astype(jnp.float32) + expert_out).astype(jnp.bfloat16)


def solution(mesh):
    placed = (
        P("sp", "tp"),
        P("sp", None),
        P("sp", None),
        P("tp"),
        P("tp", None),
        P(("sp", "tp"), None),
        P(),
        P(),
        P(("sp", "tp")),
        P(("sp", "tp"), None),
        P(("sp", "tp"), None),
        P("sp", None, "tp"),
        P("sp", None, "tp"),
        P("sp", "tp", None),
    )
    return jax.shard_map(
        per_device, mesh=mesh, in_specs=placed, out_specs=P(("sp", "tp"), None), check_vma=False
    )
```

```python
import functools
import math

import jax
import jax.numpy as jnp
from jax import lax
from jax.experimental import pallas as pl
from jax.experimental.pallas import tpu as pltpu
from jax.sharding import PartitionSpec as P

HEADS = 16
KV_HEADS = 4
HEAD_DIM = 128
WINDOW = 128
BLOCK = 128


EPS = 1e-06
NEG_BIG = -1e30


CORES = 2
LANES = 128
VMEM_BYTES = 67043328
SUMMED_EIGHTHS = 3
VMEM_SPEC = pl.BlockSpec(memory_space=pltpu.VMEM)


def greet(neighbours, partner, peers):
    barrier = pltpu.get_barrier_semaphore()
    for target in (*neighbours, partner):
        pl.semaphore_signal(barrier, inc=1, device_id={"tp": target})
    for peer in peers:
        pl.semaphore_signal(barrier, inc=1, device_id={"sp": peer})
    pl.semaphore_wait(barrier, 3 + len(peers))


def line_sequence(i, position, length, side):
    reach = length - 1 - position if side == 0 else position
    early = i < reach
    offset = jnp.where(early, i + 1, 2 * reach - i)
    home = position + offset if side == 0 else position - offset
    return home, jnp.where(early, 0, 1)


def partner_slot(mine, j, groups):
    total, bit = 0, 1
    while bit < groups:
        total = total + lax.rem(mine // bit + j // bit, 2) * bit
        bit *= 2
    return total


def moe_setup(gate_hbm, up_hbm, down_hbm, inc, gate_ref, up_ref, down_ref, weight_sem):
    length = lax.axis_size("tp") // CORES
    z, last = lax.axis_index("tp") // CORES, length - 1
    weights = [
        pltpu.make_async_copy(source, place, weight_sem.at[n])
        for n, (source, place) in enumerate(
            ((gate_hbm, gate_ref), (up_hbm, up_ref), (down_hbm, down_ref))
        )
    ]
    for copy in weights:
        copy.start()

    @pl.when((z == 0) | (z == last))
    def _():
        for slot in range(length):
            @pl.when(slot != last * (z // last))
            def _():
                inc[slot] = jnp.zeros_like(inc[slot])

        @pl.when(z == 0)
        def _():
            inc[0] = jnp.zeros_like(inc[0])

        @pl.when(z == last)
        def _():
            inc[length] = jnp.zeros_like(inc[length])
    return weights


def moe_body(
    weights, landed, send_ref, out_ref,
    rows, res, pair, inc, gate_ref, up_ref, down_ref,
    own_sem, swap_send, swap_recv, line_send, line_recv, core_send, core_recv,
    pair_send, pair_recv, sum_send, sum_recv, home_send, home_recv,
):
    length = lax.axis_size("tp") // CORES
    tp = lax.axis_index("tp")
    z, core = tp // CORES, lax.rem(tp, CORES)
    partner = z * CORES + 1 - core
    groups = lax.axis_size("sp")
    group = lax.axis_index("sp")
    near = groups // 2
    width = out_ref.shape[2]
    last = length - 1
    sides = (
        (lax.rem(z + length - 1, length) * CORES + core, z > 0),
        (lax.rem(z + 1, length) * CORES + core, z < last),
    )
    peers = [partner_slot(group, -j % groups, groups) for j in range(groups)]

    def swap(j):
        return pltpu.make_async_remote_copy(
            src_ref=send_ref.at[peers[j]],
            dst_ref=rows.at[z * 2 + j // near, core, j % near],
            send_sem=swap_send.at[j],
            recv_sem=swap_recv.at[j],
            device_id={"sp": peers[j]},
        )

    def line(side, index, j):
        place = rows.at[index, core, j]
        return pltpu.make_async_remote_copy(
            src_ref=place,
            dst_ref=place,
            send_sem=line_send.at[side, index, j],
            recv_sem=line_recv.at[index, j],
            device_id={"tp": sides[side][0]},
        )

    def across(index, j):
        place = rows.at[index, core, j]
        return pltpu.make_async_remote_copy(
            src_ref=place,
            dst_ref=place,
            send_sem=core_send.at[index, j],
            recv_sem=core_recv.at[index, j],
            device_id={"tp": partner},
        )

    def share(index):
        return pltpu.make_async_remote_copy(
            src_ref=res.at[index, 1 - core],
            dst_ref=pair.at[index],
            send_sem=pair_send.at[index],
            recv_sem=pair_recv.at[index],
            device_id={"tp": partner},
        )

    def slot_of(side, target):
        if side == 1:
            return target
        return jnp.where(target == z - 1, length, target)

    def add_on(side, target, half, j):
        slot = slot_of(side, target)
        return pltpu.make_async_remote_copy(
            src_ref=res.at[target * 2 + half, core, j],
            dst_ref=inc.at[slot, half, j],
            send_sem=sum_send.at[target * 2 + half, j],
            recv_sem=sum_recv.at[slot, half, j],
            device_id={"tp": sides[side][0]},
        )

    def added(slot, half, j):
        return pltpu.make_async_remote_copy(
            src_ref=inc.at[slot, half, j],
            dst_ref=inc.at[slot, half, j],
            send_sem=sum_send.at[0, j],
            recv_sem=sum_recv.at[slot, half, j],
            device_id={"tp": partner},
        )

    def back(half, j):
        return pltpu.make_async_remote_copy(
            src_ref=res.at[z * 2 + half, core, j],
            dst_ref=out_ref.at[group],
            send_sem=home_send.at[half * near + j],
            recv_sem=home_recv.at[half * near + j],
            device_id={"sp": peers_at(half, j)},
        )

    def peers_at(half, j):
        return peers[half * near + j]

    def forward(side, index, j):
        @pl.when(sides[side][1])
        def _():
            line(side, index, j).start()

    own = pltpu.make_async_copy(send_ref.at[group], rows.at[z * 2, core, 0], own_sem)
    own.start()
    for j in range(1, groups):
        swap(j).start()
    for j in range(near):
        if j == 0:
            own.wait()
        else:
            swap(j).wait_recv()
        for side in range(2):
            forward(side, z * 2, j)
        across(z * 2, j).start()
    for j in range(near):
        swap(near + j).wait_recv()
        across(z * 2 + 1, j).start()
    for copy in weights:
        copy.wait()

    def expert_rows(index):
        for j in range(near):
            across(index, j).wait_recv()
        block = rows[index].reshape(2 * near * rows.shape[3], rows.shape[4])
        values = block[:, :width]
        gates = block[:, width:].astype(jnp.float32)
        hidden = []
        for member in range(gate_ref.shape[0]):
            gate_pre = jnp.dot(values, gate_ref[member], preferred_element_type=jnp.float32)
            up_pre = jnp.dot(values, up_ref[member], preferred_element_type=jnp.float32)
            value = gate_pre / (1.0 + jnp.exp(-gate_pre)) * up_pre * gates[:, member : member + 1]
            hidden.append(value.astype(jnp.bfloat16))
        total = jnp.dot(
            jnp.concatenate(hidden, axis=1), down_ref[...], preferred_element_type=jnp.float32
        )
        res[index] = total.astype(res.dtype).reshape(res.shape[1:])
        share(index).start()

    def pass_on(side, i):
        target, half = line_sequence(i, z, length, 1 - side)
        index = target * 2 + half
        share(index).wait_recv()
        for j in range(near):
            @pl.when(sides[1 - side][1])
            def _():
                added(target, half, j).wait_recv()
            value = (
                res[index, core, j].astype(jnp.float32)
                + pair[index, j].astype(jnp.float32)
                + inc[target, half, j].astype(jnp.float32)
            )
            res[index, core, j] = value.astype(res.dtype)
            add_on(side, target, half, j).start()

    def finish(half):
        index = z * 2 + half
        share(index).wait_recv()
        for j in range(near):
            @pl.when(z > 0)
            def _():
                added(z, half, j).wait_recv()

            @pl.when(z < last)
            def _():
                added(length, half, j).wait_recv()
            value = (
                res[index, core, j].astype(jnp.float32)
                + pair[index, j].astype(jnp.float32)
                + inc[z, half, j].astype(jnp.float32)
                + inc[length, half, j].astype(jnp.float32)
            ).astype(res.dtype)
            if half == 0 and j == 0:
                out_ref[group] = value
            else:
                res[index, core, j] = value
                back(half, j).start()

    reaches = (last - z, z)
    lags = tuple(jnp.where(depth == 0, 0, 2 * depth + 1) for depth in (last - z, z))

    def step(k, carry):
        for j in range(near):
            for side in range(2):
                home, half = line_sequence(k, z, length, side)

                @pl.when(k < 2 * reaches[side])
                def _(side=side, index=home * 2 + half, j=j):
                    line(side, index, j).wait_recv()
                    forward(side, index, j)
                    across(index, j).start()

                @pl.when(k == 2 * reaches[side])
                def _(side=side, j=j):
                    forward(side, z * 2 + 1, j)
        for side in range(2):
            i = k - lags[side]

            @pl.when((lags[side] > 0) & (i >= 0) & (i < 2 * reaches[1 - side]))
            def _(side=side, i=i):
                pass_on(side, i)

        def job(d, inner):
            home0, half0 = line_sequence(k, z, length, 0)
            home1, half1 = line_sequence(k, z, length, 1)
            index = jnp.where(
                d == 0, home0 * 2 + half0, jnp.where(d == 1, home1 * 2 + half1, z * 2 + k // 2)
            )
            live = jnp.where(
                d == 0, k < 2 * reaches[0],
                jnp.where(d == 1, k < 2 * reaches[1], (k == 0) | (k == 2)),
            )

            @pl.when(live)
            def _():
                expert_rows(index)

            return inner

        lax.fori_loop(0, 3, job, 0)
        for side in range(2):
            @pl.when((lags[side] == 0) & (k < 2 * reaches[1 - side]))
            def _(side=side):
                pass_on(side, k)

        @pl.when(k == 2 * jnp.maximum(z, last - z))
        def _():
            finish(0)

        return carry

    lax.fori_loop(0, 2 * length - 1, step, 0)
    finish(1)

    for j in range(groups):
        if j > 0:
            back(j // near, j % near).wait_recv()
        landed(peers[j])
    for j in range(1, groups):
        swap(j).wait_send()
        back(j // near, j % near).wait_send()

    def drain(index, carry):
        home = index // 2
        for j in range(near):
            @pl.when((home >= z) & sides[0][1])
            def _(j=j):
                line(0, index, j).wait_send()

            @pl.when((home <= z) & sides[1][1])
            def _(j=j):
                line(1, index, j).wait_send()

            across(index, j).wait_send()

            @pl.when(home != z)
            def _(j=j):
                add_on(1, home, lax.rem(index, 2), j).wait_send()
        share(index).wait_send()
        return carry

    lax.fori_loop(0, 2 * length, drain, 0)


def moe_kernel(send_ref, gate_hbm, up_hbm, down_hbm, out_ref, *scratch):
    *buffers, weight_sem = scratch
    inc, places = buffers[3], buffers[4:7]
    weights = moe_setup(gate_hbm, up_hbm, down_hbm, inc, *places, weight_sem)
    z, core = lax.axis_index("tp") // CORES, lax.rem(lax.axis_index("tp"), CORES)
    length, groups = lax.axis_size("tp") // CORES, lax.axis_size("sp")
    around = [lax.rem(z + shift, length) * CORES + core for shift in (length - 1, 1)]
    others = [lax.rem(lax.axis_index("sp") + shift, groups) for shift in range(1, groups)]
    greet(around, z * CORES + 1 - core, others)
    moe_body(weights, lambda group: None, send_ref, out_ref, *buffers)


def moe_scratch(length, groups, capacity, padded, gate_weight):
    members, width, hidden = gate_weight.shape
    near = groups // 2
    kind = gate_weight.dtype
    sem = pltpu.SemaphoreType.DMA
    return [
        pltpu.VMEM((2 * length, 2, near, capacity, padded), kind),
        pltpu.VMEM((2 * length, 2, near, capacity, width), kind),
        pltpu.VMEM((2 * length, near, capacity, width), kind),
        pltpu.VMEM((length + 1, 2, near, capacity, width), kind),
        pltpu.VMEM((members, width, hidden), kind),
        pltpu.VMEM((members, width, hidden), kind),
        pltpu.VMEM((members * hidden, width), kind),
        sem,
        sem((groups,)),
        sem((groups,)),
        sem((2, 2 * length, near)),
        sem((2 * length, near)),
        sem((2 * length, near)),
        sem((2 * length, near)),
        sem((2 * length,)),
        sem((2 * length,)),
        sem((2 * length, near)),
        sem((length + 1, 2, near)),
        sem((groups,)),
        sem((groups,)),
        sem((3,)),
    ]


def moe(send_rows, gate_weight, up_weight, down_weight):
    groups, capacity, padded = send_rows.shape
    members, width, hidden = gate_weight.shape
    length = lax.axis_size("tp") // CORES
    hbm = pl.BlockSpec(memory_space=pltpu.HBM)
    return pl.pallas_call(
        moe_kernel,
        out_shape=jax.ShapeDtypeStruct((groups, capacity, width), send_rows.dtype),
        in_specs=[VMEM_SPEC, hbm, hbm, hbm],
        out_specs=VMEM_SPEC,
        scratch_shapes=moe_scratch(length, groups, capacity, padded, gate_weight),
        compiler_params=pltpu.CompilerParams(
            collective_id=1, has_side_effects=True, vmem_limit_bytes=VMEM_BYTES
        ),
        name="moe",
    )(send_rows, gate_weight, up_weight, down_weight.reshape(members * hidden, width))


def front_body(
    setup, query_hbm, key_hbm, value_hbm, sink_ref, weight_hbm, residual_hbm, mixer_hbm, expert_hbm,
    group_ref, member_ref, gate_ref,
    mixed_ref, rows_ref, placing_ref,
    query, span, attended, received, full, total, residual, gains,
    own_weight, prod, prod_pair, prod_inc,
    load_sem, halo_send, halo_recv, line_send, line_recv, plane_send, plane_recv,
    core_send, core_recv, row_send, row_recv, pair_send, pair_recv, sum_send, sum_recv,
):
    parts = lax.axis_size("tp")
    length = parts // CORES
    tp = lax.axis_index("tp")
    z, core = tp // CORES, lax.rem(tp, CORES)
    partner = z * CORES + 1 - core
    groups = lax.axis_size("sp")
    group = lax.axis_index("sp")
    last = length - 1
    halves = full.shape[2]
    relayed = groups == 4
    seq_rows = query.shape[0]
    heads_dev = query.shape[1] // HEAD_DIM
    blocks = seq_rows // BLOCK
    peers = [partner_slot(group, j, groups) for j in range(groups)]
    sides = (
        (lax.rem(z + length - 1, length) * CORES + core, z > 0),
        (lax.rem(z + 1, length) * CORES + core, z < last),
    )
    head_start = pl.multiple_of(tp * heads_dev // (HEADS // KV_HEADS) * HEAD_DIM, HEAD_DIM)
    inner = pl.ds(WINDOW, seq_rows)
    summed, gathered = own_weight.shape[3], full.shape[4]

    loads = [
        pltpu.make_async_copy(source, place, load_sem.at[n])
        for n, (source, place) in enumerate(
            (
                (weight_hbm.at[:, :, :, pl.ds(summed, gathered)], full.at[tp]),
                (key_hbm.at[:, pl.ds(head_start, HEAD_DIM)], span.at[0, inner]),
                (value_hbm.at[:, pl.ds(head_start, HEAD_DIM)], span.at[1, inner]),
                (query_hbm, query),
                (weight_hbm.at[:, :, :, pl.ds(0, summed)], own_weight),
                (residual_hbm, residual),
                (mixer_hbm, gains.at[0]),
                (expert_hbm, gains.at[1]),
            )
        )
    ]
    for copy in loads:
        copy.start()

    @pl.when(group == 0)
    def _():
        span[:, :WINDOW] = jnp.zeros((2, WINDOW, HEAD_DIM), span.dtype)

    @pl.when(z == 0)
    def _():
        for slot in range(length):
            prod_inc[slot] = jnp.zeros_like(prod_inc[slot])

    @pl.when(z == last)
    def _():
        for slot in [*range(last), length]:
            prod_inc[slot] = jnp.zeros_like(prod_inc[slot])

    @pl.when(group == groups - 1)
    def _():
        span[:, WINDOW + seq_rows :] = jnp.zeros((2, WINDOW, HEAD_DIM), span.dtype)

    started = setup()
    barrier = pltpu.get_barrier_semaphore()
    for shift in range(1, parts):
        pl.semaphore_signal(barrier, inc=1, device_id={"tp": lax.rem(tp + shift, parts)})
    for peer in peers[1:]:
        pl.semaphore_signal(barrier, inc=1, device_id={"sp": peer})
    pl.semaphore_wait(barrier, parts + groups - 2)

    def line(side, home, half):
        place = full.at[home * CORES + core, group, half]
        return pltpu.make_async_remote_copy(
            src_ref=place,
            dst_ref=place,
            send_sem=line_send.at[side, home, half],
            recv_sem=line_recv.at[home, half],
            device_id={"tp": sides[side][0]},
        )

    def plane(home, j, half, target, source):
        place = full.at[home * CORES + core, source, half]
        return pltpu.make_async_remote_copy(
            src_ref=place,
            dst_ref=place,
            send_sem=plane_send.at[home, j, half],
            recv_sem=plane_recv.at[home, j, half],
            device_id={"sp": target},
        )

    def relay(home, half):
        target, source = (peers[2], peers[1]) if half == 0 else (peers[1], peers[2])
        return plane(home, 3, half, target, source)

    def across(home):
        place = full.at[home * CORES + core]
        return pltpu.make_async_remote_copy(
            src_ref=place,
            dst_ref=place,
            send_sem=core_send.at[home],
            recv_sem=core_recv.at[home],
            device_id={"tp": partner},
        )

    def halo(side):
        start = WINDOW if side == 0 else seq_rows
        landing = WINDOW + seq_rows if side == 0 else 0
        return pltpu.make_async_remote_copy(
            src_ref=span.at[:, pl.ds(start, WINDOW)],
            dst_ref=span.at[:, pl.ds(landing, WINDOW)],
            send_sem=halo_send.at[side],
            recv_sem=halo_recv.at[side],
            device_id={"sp": lax.rem(group + (groups - 1 if side == 0 else 1), groups)},
        )

    def row_block(shift):
        target = lax.rem(tp + shift, parts)
        return pltpu.make_async_remote_copy(
            src_ref=attended.at[target],
            dst_ref=received.at[tp],
            send_sem=row_send.at[shift],
            recv_sem=row_recv.at[shift],
            device_id={"tp": target},
        )

    def share(home):
        return pltpu.make_async_remote_copy(
            src_ref=prod.at[home, 1 - core],
            dst_ref=prod_pair.at[home],
            send_sem=pair_send.at[home],
            recv_sem=pair_recv.at[home],
            device_id={"tp": partner},
        )

    def add_on(side, home):
        slot = home if side == 1 else jnp.where(home == z - 1, length, home)
        return pltpu.make_async_remote_copy(
            src_ref=prod.at[home, core],
            dst_ref=prod_inc.at[slot],
            send_sem=sum_send.at[home],
            recv_sem=sum_recv.at[slot],
            device_id={"tp": sides[side][0]},
        )

    def added(slot):
        return pltpu.make_async_remote_copy(
            src_ref=prod_inc.at[slot],
            dst_ref=prod_inc.at[slot],
            send_sem=sum_send.at[0],
            recv_sem=sum_recv.at[slot],
            device_id={"tp": partner},
        )

    def pass_on(side, home):
        share(home).wait_recv()

        @pl.when(sides[1 - side][1])
        def _():
            added(home).wait_recv()

        prod[home, core] = (
            prod[home, core].astype(jnp.float32)
            + prod_pair[home].astype(jnp.float32)
            + prod_inc[home].astype(jnp.float32)
        ).astype(prod.dtype)
        add_on(side, home).start()

    inward = (group > 0, group < groups - 1)
    loads[0].wait()
    for half in range(halves):
        for side in range(2):
            @pl.when(sides[side][1])
            def _(side=side, half=half):
                line(side, z, half).start()
    loads[1].wait()
    loads[2].wait()
    for side in range(2):
        @pl.when(inward[side])
        def _(side=side):
            halo(side).start()
    across(z).start()
    loads[3].wait()
    loads[4].wait()

    def attend(n, carry):
        b = jnp.where(n < blocks - 2, n + 1, jnp.where(n == blocks - 2, 0, blocks - 1))

        @pl.when(n == blocks - 2)
        def _():
            for side in range(2):
                @pl.when(inward[1 - side])
                def _(side=side):
                    halo(side).wait_recv()

        start = pl.multiple_of(b * BLOCK, BLOCK)
        wide = query[pl.ds(start, BLOCK), :]
        tall = jnp.concatenate(
            [wide[:, h * HEAD_DIM : (h + 1) * HEAD_DIM] for h in range(heads_dev)], axis=0
        )
        reach = BLOCK + 2 * WINDOW
        keys = span[0, pl.ds(start, reach), :]
        values = span[1, pl.ds(start, reach), :]
        scores = lax.dot_general(
            tall, keys, (((1,), (1,)), ((), ())), preferred_element_type=jnp.float32
        ) * HEAD_DIM ** (-0.5)
        shape = (heads_dev * BLOCK, reach)
        row = lax.broadcasted_iota(jnp.int32, shape, 0) % BLOCK
        column = lax.broadcasted_iota(jnp.int32, shape, 1)
        place = column + (group * seq_rows + b * BLOCK - WINDOW)
        inside = (
            (column >= row) & (column <= row + 2 * WINDOW)
            & (place >= 0) & (place < seq_rows * groups)
        )
        scores = jnp.where(inside, scores, NEG_BIG)
        which = lax.broadcasted_iota(jnp.int32, (heads_dev * BLOCK, 1), 0) // BLOCK
        sink = jnp.zeros((heads_dev * BLOCK, 1), jnp.float32)
        for h in range(heads_dev):
            sink = jnp.where(which == h, sink_ref[h], sink)
        top = jnp.maximum(jnp.max(scores, axis=1, keepdims=True), sink)
        terms = jnp.exp(scores - top)
        mass = jnp.sum(terms, axis=1, keepdims=True) + jnp.exp(sink - top)
        weight = (terms / mass).astype(jnp.bfloat16)
        result = jnp.dot(weight, values, preferred_element_type=jnp.float32).astype(jnp.bfloat16)
        attended[b] = jnp.concatenate(
            [result[h * BLOCK : (h + 1) * BLOCK] for h in range(heads_dev)], axis=1
        )
        return carry


    def homes(i):
        return ((z + 1 + i, z + 1 + i <= last), (z - 1 - i, z - 1 - i >= 0))

    def spread_half(i, half):
        for side in range(2):
            home, live = homes(i)[side]

            @pl.when(live)
            def _(side=side, home=home):
                line(side, home, half).wait_recv()

                @pl.when(sides[side][1])
                def _():
                    line(side, home, half).start()

                if not relayed:
                    for j in range(1, groups):
                        plane(home, j, half, peers[j], group).start()
                elif half == 0:
                    plane(home, 1, 0, peers[1], group).start()
                else:
                    plane(home, 2, 1, peers[2], group).start()
                    plane(home, 1, 1, peers[1], group).start()
                    plane(home, 2, 0, peers[2], group).start()

    def relay_half(i, half):
        for side in range(2):
            home, live = homes(i)[side]

            @pl.when(live)
            def _(home=home):
                plane(home, 1 + half, half, peers[1], group).wait_recv()
                relay(home, half).start()

    def multiply(home, carry):
        lhs = jnp.concatenate([attended[home * CORES + c] for c in range(CORES)], axis=0)
        part = jnp.dot(
            lhs, own_weight[...].reshape(-1, summed), preferred_element_type=jnp.float32
        )
        prod[home] = part.astype(prod.dtype).reshape(CORES, -1, summed)
        share(home).start()
        return carry

    depths = (last - z, z)

    def add_step(r):
        for side in range(2):
            event = r - (depths[side] - 1)
            home = last - event if side == 1 else event

            @pl.when((depths[side] > 0) & (event >= 0) & (event < depths[1 - side]))
            def _(side=side, home=home):
                pass_on(side, home)

    def spread(i):
        for half in range(halves):
            spread_half(i, half)
        if relayed:
            for half in range(halves):
                relay_half(i, half)

    def first_sums():
        for side in range(2):
            @pl.when(depths[side] == 0)
            def _(side=side):
                for event in range(last):
                    pass_on(side, last - event if side == 1 else event)

    def send_rows():
        for shift in range(1, parts):
            row_block(shift).start()

    lax.fori_loop(0, blocks, attend, 0)
    received[tp] = attended[tp]
    send_rows()
    lax.fori_loop(0, length, multiply, 0)
    spread(0)
    first_sums()
    for i in range(1, last):
        add_step(i - 1)
        spread(i)
    capacity = rows_ref.shape[1]
    slots = groups * capacity
    tok_rows = residual.shape[0]
    width = residual.shape[1]
    names = lax.broadcasted_iota(jnp.int32, (groups * (8 // min(groups, 8)), tok_rows), 0)
    chosen = (names == group_ref[...]).astype(jnp.float32)
    earlier = (
        lax.broadcasted_iota(jnp.int32, (tok_rows, tok_rows), 0)
        < lax.broadcasted_iota(jnp.int32, (tok_rows, tok_rows), 1)
    ).astype(jnp.bfloat16)
    rank = jnp.dot(chosen.astype(jnp.bfloat16), earlier, preferred_element_type=jnp.float32)
    slot_row = jnp.sum(
        chosen * (rank + (names * rows_ref.shape[1]).astype(jnp.float32)), axis=0, keepdims=True
    )
    placing = (
        lax.broadcasted_iota(jnp.int32, (slots, tok_rows), 0).astype(jnp.float32) == slot_row
    ).astype(jnp.bfloat16)
    placing_ref[...] = placing.reshape(placing_ref.shape)
    members = lax.broadcasted_iota(jnp.int32, (LANES, tok_rows), 0)
    tail = jnp.zeros((LANES, tok_rows), jnp.float32)
    for k in range(member_ref.shape[0]):
        tail = tail + jnp.where(
            members == member_ref[k : k + 1, :], gate_ref[k : k + 1, :].astype(jnp.float32), 0.0
        )
    rows_ref[:, :, width:] = (
        lax.dot_general(
            placing, tail.astype(jnp.bfloat16), (((1,), (1,)), ((), ())),
            preferred_element_type=jnp.float32,
        )
        .astype(rows_ref.dtype)
        .reshape(groups, rows_ref.shape[1], LANES)
    )

    def project(home, first):
        pieces = [received[home * CORES + c] for c in range(CORES)]
        lhs = jnp.concatenate(pieces, axis=1)
        rhs = jnp.concatenate(
            [full[home * CORES + c].reshape(-1, gathered) for c in range(CORES)], axis=0
        )
        part = jnp.dot(lhs, rhs, preferred_element_type=jnp.float32)
        if first:
            total[:, summed:] = part
        else:
            total[:, summed:] += part

    def rows_from(home):
        for c in range(CORES):
            source = home * CORES + c

            @pl.when(source != tp)
            def _(source=source):
                shift = lax.rem(tp - source + parts, parts)
                pltpu.make_async_remote_copy(
                    src_ref=attended.at[source],
                    dst_ref=received.at[source],
                    send_sem=row_send.at[0],
                    recv_sem=row_recv.at[lax.rem(parts + tp - source, parts)],
                    device_id={"tp": partner},
                ).wait_recv()

    across(z).wait_recv()
    rows_from(z)
    project(z, True)

    def gather_step(i, carry):
        for side in range(2):
            home, live = homes(i)[side]

            @pl.when(live)
            def _(home=home):
                for half in range(halves):
                    for j in range(1, groups):
                        if not (relayed and j == 1 + half and j < 3):
                            plane(home, j, half, peers[1], group).wait_recv()
                across(home).start()

        for side in range(2):
            home, live = homes(i)[side]

            @pl.when(live)
            def _(home=home):
                across(home).wait_recv()
                rows_from(home)
                project(home, False)

        return carry

    lax.fori_loop(0, last, gather_step, 0)

    share(z).wait_recv()

    @pl.when(z > 0)
    def _():
        added(z).wait_recv()

    @pl.when(z < last)
    def _():
        added(length).wait_recv()

    total[:, :summed] = (
        prod[z, core].astype(jnp.float32)
        + prod_pair[z].astype(jnp.float32)
        + prod_inc[z].astype(jnp.float32)
        + prod_inc[length].astype(jnp.float32)
    )
    for copy in loads[5:]:
        copy.wait()
    projected = total[...]
    scale = lax.rsqrt(jnp.mean(projected * projected, axis=1, keepdims=True) + EPS)
    mixed = (
        residual[...].astype(jnp.float32) + gains[0] * (projected * scale)
    ).astype(jnp.bfloat16)
    mixed_ref[...] = mixed
    mixed_float = mixed.astype(jnp.float32)
    norm = lax.rsqrt(jnp.mean(mixed_float * mixed_float, axis=1, keepdims=True) + EPS)
    normed = (mixed_float * norm * gains[1]).astype(jnp.bfloat16)
    rows_ref[:, :, :width] = (
        jnp.dot(placing, normed, preferred_element_type=jnp.float32)
        .astype(rows_ref.dtype)
        .reshape(groups, rows_ref.shape[1], width)
    )

    def settle():
        for side in range(2):
            @pl.when(inward[side])
            def _(side=side):
                halo(side).wait_send()
        for shift in range(1, parts):
            row_block(shift).wait_send()

        def drain(home, carry):
            for half in range(halves):
                @pl.when((home >= z) & sides[0][1])
                def _(half=half):
                    line(0, home, half).wait_send()

                @pl.when((home <= z) & sides[1][1])
                def _(half=half):
                    line(1, home, half).wait_send()

                @pl.when(home != z)
                def _(half=half):
                    for j in range(1, groups):
                        plane(home, j, half, peers[1], group).wait_send()

            @pl.when(home != z)
            def _():
                add_on(1, home).wait_send()

            across(home).wait_send()
            share(home).wait_send()
            return carry

        lax.fori_loop(0, length, drain, 0)

    return started, settle


def front_kernel(*refs):
    _, settle = front_body(lambda: None, *refs)
    settle()


def front_scratch(parts, groups, queries, residual):
    length = parts // CORES
    seq_rows, columns = queries.shape
    tok_rows, width = residual.shape
    halves = 2 if groups == 4 else 1
    piece = columns // (groups * halves)
    summed = SUMMED_EIGHTHS * width // 8 // LANES * LANES
    sem = pltpu.SemaphoreType.DMA
    kind = queries.dtype
    return [
        pltpu.VMEM((seq_rows, columns), kind),
        pltpu.VMEM((2, seq_rows + 2 * WINDOW, HEAD_DIM), kind),
        pltpu.VMEM((parts, tok_rows, columns), kind),
        pltpu.VMEM((parts, tok_rows, columns), kind),
        pltpu.VMEM((parts, groups, halves, piece, width - summed), kind),
        pltpu.VMEM((tok_rows, width), jnp.float32),
        pltpu.VMEM((tok_rows, width), kind),
        pltpu.VMEM((2, 1, width), jnp.float32),
        pltpu.VMEM((groups, halves, piece, summed), kind),
        pltpu.VMEM((length, CORES, tok_rows, summed), kind),
        pltpu.VMEM((length, tok_rows, summed), kind),
        pltpu.VMEM((length + 1, tok_rows, summed), kind),
        sem((8,)),
        sem((2,)),
        sem((2,)),
        sem((2, length, halves)),
        sem((length, halves)),
        sem((length, groups, halves)),
        sem((length, groups, halves)),
        sem((length,)),
        sem((length,)),
        sem((parts,)),
        sem((parts,)),
        sem((length,)),
        sem((length,)),
        sem((length,)),
        sem((length + 1,)),
    ]


HBM_SPEC = pl.BlockSpec(memory_space=pltpu.HBM)
FRONT_SPECS = (
    *[HBM_SPEC] * 3, pl.BlockSpec(memory_space=pltpu.SMEM), *[HBM_SPEC] * 4, *[VMEM_SPEC] * 3
)


def front_made(groups, capacity, residual):
    tok_rows, width = residual.shape
    return (
        ((tok_rows, width), residual.dtype),
        ((groups, capacity, width + LANES), residual.dtype),
        ((groups, capacity, tok_rows), residual.dtype),
    )


def front(arguments, capacity):
    parts, groups = lax.axis_size("tp"), lax.axis_size("sp")
    made = front_made(groups, capacity, arguments[5])
    return pl.pallas_call(
        front_kernel,
        out_shape=[jax.ShapeDtypeStruct(*each) for each in made],
        in_specs=FRONT_SPECS,
        out_specs=[VMEM_SPEC] * 3,
        scratch_shapes=front_scratch(parts, groups, arguments[0], arguments[5]),
        compiler_params=pltpu.CompilerParams(
            collective_id=0, has_side_effects=True, vmem_limit_bytes=VMEM_BYTES
        ),
        name="front",
    )(*arguments)


def layer_kernel(inputs, front_count, moe_count, *refs):
    front_in, refs = refs[:inputs], refs[inputs:]
    weights_in, out_ref, refs = refs[:3], refs[3], refs[4:]
    front_refs, refs = refs[:front_count], refs[front_count:]
    *buffers, weight_sem = refs[:moe_count]
    mixed_ref, rows_ref, placing_ref, returned = refs[moe_count:]

    def setup():
        return moe_setup(*weights_in, buffers[3], *buffers[4:7], weight_sem)

    weights, settle = front_body(
        setup, *front_in, mixed_ref, rows_ref, placing_ref, *front_refs
    )
    total = front_refs[5]
    total[...] = mixed_ref[...].astype(jnp.float32)

    def landed(group):
        total[...] += lax.dot_general(
            placing_ref[group], returned[group], (((0,), (0,)), ((), ())),
            preferred_element_type=jnp.float32,
        )

    moe_body(weights, landed, rows_ref, returned, *buffers)
    out_ref[...] = total[...].astype(out_ref.dtype)
    settle()


def layer(arguments, capacity, gate_weight, up_weight, down_weight, front_bufs, moe_bufs):
    residual = arguments[5]
    groups = lax.axis_size("sp")
    kept = front_made(groups, capacity, residual)
    returned = ((groups, capacity, residual.shape[1]), residual.dtype)
    return pl.pallas_call(
        functools.partial(layer_kernel, len(arguments), len(front_bufs), len(moe_bufs)),
        out_shape=jax.ShapeDtypeStruct(residual.shape, residual.dtype),
        in_specs=[*FRONT_SPECS, *[HBM_SPEC] * 3],
        out_specs=VMEM_SPEC,
        scratch_shapes=[
            *front_bufs, *moe_bufs, *[pltpu.VMEM(*each) for each in (*kept, returned)]
        ],
        compiler_params=pltpu.CompilerParams(
            collective_id=2, has_side_effects=True, vmem_limit_bytes=VMEM_BYTES
        ),
        name="layer",
    )(*arguments, gate_weight, up_weight, down_weight.reshape(-1, residual.shape[1]))


def per_device(
    queries,
    key_heads,
    value_heads,
    sink_logit,
    out_weight,
    residual,
    mixer_gain,
    expert_gain,
    route_group,
    route_member,
    route_weight,
    gate_weight,
    up_weight,
    down_weight,
):
    tok_rows, width = residual.shape
    parts, groups = lax.axis_size("tp"), lax.axis_size("sp")
    capacity = max(2, (5 * tok_rows + 4 * groups - 1) // (4 * groups))
    capacity = (capacity + 7) // 8 * 8
    halves = 2 if groups == 4 else 1
    arguments = (
        queries, key_heads, value_heads, sink_logit,
        out_weight.reshape(groups, halves, -1, width), residual,
        mixer_gain.reshape(1, width), expert_gain.reshape(1, width),
        route_group.reshape(1, tok_rows), route_member.T, route_weight.T,
    )
    front_bufs = front_scratch(parts, groups, queries, residual)
    moe_bufs = moe_scratch(parts // CORES, groups, capacity, width + LANES, gate_weight)
    held = sum(
        math.prod(each.shape) * jnp.dtype(each.dtype).itemsize
        for each in (*front_bufs, *moe_bufs)
        if getattr(each, "memory_space", None) == pltpu.VMEM
    )
    if held < VMEM_BYTES * 3 // 4:
        return layer(
            arguments, capacity, gate_weight, up_weight, down_weight, front_bufs, moe_bufs
        )
    mixed_rows, send_rows, placing = front(arguments, capacity)
    returned = moe(send_rows, gate_weight, up_weight, down_weight)
    expert_out = lax.dot_general(
        placing.reshape(-1, tok_rows),
        returned.reshape(-1, width),
        (((0,), (0,)), ((), ())),
        preferred_element_type=jnp.float32,
    )
    return (mixed_rows.astype(jnp.float32) + expert_out).astype(jnp.bfloat16)


def solution(mesh):
    placed = (
        P("sp", "tp"),
        P("sp", None),
        P("sp", None),
        P("tp"),
        P("tp", None),
        P(("sp", "tp"), None),
        P(),
        P(),
        P(("sp", "tp")),
        P(("sp", "tp"), None),
        P(("sp", "tp"), None),
        P("sp", None, "tp"),
        P("sp", None, "tp"),
        P("sp", "tp", None),
    )
    return jax.shard_map(
        per_device, mesh=mesh, in_specs=placed, out_specs=P(("sp", "tp"), None), check_vma=False
    )
```

```python
import functools
import math

import jax
import jax.numpy as jnp
from jax import lax
from jax.experimental import pallas as pl
from jax.experimental.pallas import tpu as pltpu
from jax.sharding import PartitionSpec as P

HEADS = 16
KV_HEADS = 4
HEAD_DIM = 128
WINDOW = 128
BLOCK = 128


EPS = 1e-06
NEG_BIG = -1e30


CORES = 2
LANES = 128
VMEM_BYTES = 67043328
SUMMED_EIGHTHS = 3
GATE_ROWS = 8
VMEM_SPEC = pl.BlockSpec(memory_space=pltpu.VMEM)


def greet(neighbours, partner, peers):
    barrier = pltpu.get_barrier_semaphore()
    for target in (*neighbours, partner):
        pl.semaphore_signal(barrier, inc=1, device_id={"tp": target})
    for peer in peers:
        pl.semaphore_signal(barrier, inc=1, device_id={"sp": peer})
    pl.semaphore_wait(barrier, 3 + len(peers))


def line_sequence(i, position, length, side):
    reach = length - 1 - position if side == 0 else position
    early = i < reach
    offset = jnp.where(early, i + 1, 2 * reach - i)
    home = position + offset if side == 0 else position - offset
    return home, jnp.where(early, 0, 1)


def partner_slot(mine, j, groups):
    total, bit = 0, 1
    while bit < groups:
        total = total + lax.rem(mine // bit + j // bit, 2) * bit
        bit *= 2
    return total


def moe_setup(gate_hbm, up_hbm, down_hbm, inc, gate_ref, up_ref, down_ref, weight_sem):
    length = lax.axis_size("tp") // CORES
    z, last = lax.axis_index("tp") // CORES, length - 1
    weights = [
        pltpu.make_async_copy(source, place, weight_sem.at[n])
        for n, (source, place) in enumerate(
            ((gate_hbm, gate_ref), (up_hbm, up_ref), (down_hbm, down_ref))
        )
    ]
    for copy in weights:
        copy.start()

    @pl.when((z == 0) | (z == last))
    def _():
        for slot in range(length):
            @pl.when(slot != last * (z // last))
            def _():
                inc[slot] = jnp.zeros_like(inc[slot])

        @pl.when(z == 0)
        def _():
            inc[0] = jnp.zeros_like(inc[0])

        @pl.when(z == last)
        def _():
            inc[length] = jnp.zeros_like(inc[length])
    return weights


def moe_body(
    weights, landed, send_ref, gates_ref, out_ref,
    rows, res, pair, inc, gate_ref, up_ref, down_ref,
    own_sem, swap_send, swap_recv, line_send, line_recv, core_send, core_recv,
    pair_send, pair_recv, sum_send, sum_recv, home_send, home_recv,
):
    length = lax.axis_size("tp") // CORES
    tp = lax.axis_index("tp")
    z, core = tp // CORES, lax.rem(tp, CORES)
    partner = z * CORES + 1 - core
    groups = lax.axis_size("sp")
    group = lax.axis_index("sp")
    near = groups // 2
    width = out_ref.shape[2]
    last = length - 1
    sides = (
        (lax.rem(z + length - 1, length) * CORES + core, z > 0),
        (lax.rem(z + 1, length) * CORES + core, z < last),
    )
    peers = [partner_slot(group, -j % groups, groups) for j in range(groups)]

    def swap(j):
        return pltpu.make_async_remote_copy(
            src_ref=send_ref.at[peers[j]],
            dst_ref=rows.at[z * 2 + j // near, core, j % near],
            send_sem=swap_send.at[j],
            recv_sem=swap_recv.at[j],
            device_id={"sp": peers[j]},
        )

    def line(side, index, j):
        place = rows.at[index, core, j]
        return pltpu.make_async_remote_copy(
            src_ref=place,
            dst_ref=place,
            send_sem=line_send.at[side, index, j],
            recv_sem=line_recv.at[index, j],
            device_id={"tp": sides[side][0]},
        )

    def across(index, j):
        place = rows.at[index, core, j]
        return pltpu.make_async_remote_copy(
            src_ref=place,
            dst_ref=place,
            send_sem=core_send.at[index, j],
            recv_sem=core_recv.at[index, j],
            device_id={"tp": partner},
        )

    def share(index):
        return pltpu.make_async_remote_copy(
            src_ref=res.at[index, 1 - core],
            dst_ref=pair.at[index],
            send_sem=pair_send.at[index],
            recv_sem=pair_recv.at[index],
            device_id={"tp": partner},
        )

    def slot_of(side, target):
        if side == 1:
            return target
        return jnp.where(target == z - 1, length, target)

    def add_on(side, target, half, j):
        slot = slot_of(side, target)
        return pltpu.make_async_remote_copy(
            src_ref=res.at[target * 2 + half, core, j],
            dst_ref=inc.at[slot, half, j],
            send_sem=sum_send.at[target * 2 + half, j],
            recv_sem=sum_recv.at[slot, half, j],
            device_id={"tp": sides[side][0]},
        )

    def added(slot, half, j):
        return pltpu.make_async_remote_copy(
            src_ref=inc.at[slot, half, j],
            dst_ref=inc.at[slot, half, j],
            send_sem=sum_send.at[0, j],
            recv_sem=sum_recv.at[slot, half, j],
            device_id={"tp": partner},
        )

    def back(half, j):
        return pltpu.make_async_remote_copy(
            src_ref=res.at[z * 2 + half, core, j],
            dst_ref=out_ref.at[group],
            send_sem=home_send.at[half * near + j],
            recv_sem=home_recv.at[half * near + j],
            device_id={"sp": peers_at(half, j)},
        )

    def peers_at(half, j):
        return peers[half * near + j]

    def forward(side, index, j):
        @pl.when(sides[side][1])
        def _():
            line(side, index, j).start()

    own = pltpu.make_async_copy(send_ref.at[group], rows.at[z * 2, core, 0], own_sem)
    own.start()
    for j in range(1, groups):
        swap(j).start()
    for j in range(near):
        if j == 0:
            own.wait()
        else:
            swap(j).wait_recv()
        for side in range(2):
            forward(side, z * 2, j)
        across(z * 2, j).start()
    for j in range(near):
        swap(near + j).wait_recv()
        across(z * 2 + 1, j).start()
    for copy in weights:
        copy.wait()

    def expert_rows(index):
        for j in range(near):
            across(index, j).wait_recv()
        block = rows[index].reshape(2 * near * rows.shape[3], rows.shape[4])
        home, half = index // 2, lax.rem(index, 2)
        gates = jnp.concatenate(
            [
                gates_ref[home * CORES + c, half * near + j].astype(jnp.float32).T[: rows.shape[3]]
                for c in range(CORES) for j in range(near)
            ],
            axis=0,
        )
        hidden = []
        for member in range(gate_ref.shape[0]):
            gate_pre = jnp.dot(block, gate_ref[member], preferred_element_type=jnp.float32)
            up_pre = jnp.dot(block, up_ref[member], preferred_element_type=jnp.float32)
            value = gate_pre / (1.0 + jnp.exp(-gate_pre)) * up_pre * gates[:, member : member + 1]
            hidden.append(value.astype(jnp.bfloat16))
        total = jnp.dot(
            jnp.concatenate(hidden, axis=1), down_ref[...], preferred_element_type=jnp.float32
        )
        res[index] = total.astype(res.dtype).reshape(res.shape[1:])
        share(index).start()

    def pass_on(side, i):
        target, half = line_sequence(i, z, length, 1 - side)
        index = target * 2 + half
        share(index).wait_recv()
        for j in range(near):
            @pl.when(sides[1 - side][1])
            def _():
                added(target, half, j).wait_recv()
            value = (
                res[index, core, j].astype(jnp.float32)
                + pair[index, j].astype(jnp.float32)
                + inc[target, half, j].astype(jnp.float32)
            )
            res[index, core, j] = value.astype(res.dtype)
            add_on(side, target, half, j).start()

    def finish(half):
        index = z * 2 + half
        share(index).wait_recv()
        for j in range(near):
            @pl.when(z > 0)
            def _():
                added(z, half, j).wait_recv()

            @pl.when(z < last)
            def _():
                added(length, half, j).wait_recv()
            value = (
                res[index, core, j].astype(jnp.float32)
                + pair[index, j].astype(jnp.float32)
                + inc[z, half, j].astype(jnp.float32)
                + inc[length, half, j].astype(jnp.float32)
            ).astype(res.dtype)
            if half == 0 and j == 0:
                out_ref[group] = value
            else:
                res[index, core, j] = value
                back(half, j).start()

    reaches = (last - z, z)
    lags = tuple(jnp.where(depth == 0, 0, 2 * depth + 1) for depth in (last - z, z))

    spare = max(0, 2 * last - 3)

    def step(k, carry):
        for j in range(near):
            for side in range(2):
                home, half = line_sequence(k, z, length, side)

                @pl.when(k < 2 * reaches[side])
                def _(side=side, index=home * 2 + half, j=j):
                    line(side, index, j).wait_recv()
                    forward(side, index, j)
                    across(index, j).start()

                @pl.when(k == 2 * reaches[side])
                def _(side=side, j=j):
                    forward(side, z * 2 + 1, j)
        for side in range(2):
            i = k - lags[side]

            @pl.when((lags[side] > 0) & (i >= 0) & (i < 2 * reaches[1 - side]))
            def _(side=side, i=i):
                pass_on(side, i)

        def job(d, inner):
            home0, half0 = line_sequence(k, z, length, 0)
            home1, half1 = line_sequence(k, z, length, 1)
            index = jnp.where(
                d == 0, home0 * 2 + half0, jnp.where(d == 1, home1 * 2 + half1, z * 2 + k - spare)
            )
            live = jnp.where(
                d == 0, k < 2 * reaches[0],
                jnp.where(d == 1, k < 2 * reaches[1], (k == spare) | (k == spare + 1)),
            )

            @pl.when(live)
            def _():
                expert_rows(index)

            return inner

        lax.fori_loop(0, 3, job, 0)
        for side in range(2):
            @pl.when((lags[side] == 0) & (k < 2 * reaches[1 - side]))
            def _(side=side):
                pass_on(side, k)

        @pl.when(k == 2 * jnp.maximum(z, last - z))
        def _():
            finish(0)

        return carry

    lax.fori_loop(0, 2 * length - 1, step, 0)
    finish(1)

    for j in range(groups):
        if j > 0:
            back(j // near, j % near).wait_recv()
        landed(j, peers[j])
    for j in range(1, groups):
        swap(j).wait_send()
        back(j // near, j % near).wait_send()

    def drain(index, carry):
        home = index // 2
        for j in range(near):
            @pl.when((home >= z) & sides[0][1])
            def _(j=j):
                line(0, index, j).wait_send()

            @pl.when((home <= z) & sides[1][1])
            def _(j=j):
                line(1, index, j).wait_send()

            across(index, j).wait_send()

            @pl.when(home != z)
            def _(j=j):
                add_on(1, home, lax.rem(index, 2), j).wait_send()
        share(index).wait_send()
        return carry

    lax.fori_loop(0, 2 * length, drain, 0)


def moe_kernel(send_ref, gates_ref, gate_hbm, up_hbm, down_hbm, out_ref, *scratch):
    *buffers, weight_sem = scratch
    inc, places = buffers[3], buffers[4:7]
    weights = moe_setup(gate_hbm, up_hbm, down_hbm, inc, *places, weight_sem)
    z, core = lax.axis_index("tp") // CORES, lax.rem(lax.axis_index("tp"), CORES)
    length, groups = lax.axis_size("tp") // CORES, lax.axis_size("sp")
    around = [lax.rem(z + shift, length) * CORES + core for shift in (length - 1, 1)]
    others = [lax.rem(lax.axis_index("sp") + shift, groups) for shift in range(1, groups)]
    greet(around, z * CORES + 1 - core, others)
    moe_body(weights, lambda j, group: None, send_ref, gates_ref, out_ref, *buffers)


def moe_scratch(length, groups, capacity, gate_weight):
    members, width, hidden = gate_weight.shape
    near = groups // 2
    kind = gate_weight.dtype
    sem = pltpu.SemaphoreType.DMA
    return [
        pltpu.VMEM((2 * length, 2, near, capacity, width), kind),
        pltpu.VMEM((2 * length, 2, near, capacity, width), kind),
        pltpu.VMEM((2 * length, near, capacity, width), kind),
        pltpu.VMEM((length + 1, 2, near, capacity, width), kind),
        pltpu.VMEM((members, width, hidden), kind),
        pltpu.VMEM((members, width, hidden), kind),
        pltpu.VMEM((members * hidden, width), kind),
        sem,
        sem((groups,)),
        sem((groups,)),
        sem((2, 2 * length, near)),
        sem((2 * length, near)),
        sem((2 * length, near)),
        sem((2 * length, near)),
        sem((2 * length,)),
        sem((2 * length,)),
        sem((2 * length, near)),
        sem((length + 1, 2, near)),
        sem((groups,)),
        sem((groups,)),
        sem((3,)),
    ]


def moe(send_rows, gates, gate_weight, up_weight, down_weight):
    groups, capacity, _ = send_rows.shape
    members, width, hidden = gate_weight.shape
    length = lax.axis_size("tp") // CORES
    hbm = pl.BlockSpec(memory_space=pltpu.HBM)
    return pl.pallas_call(
        moe_kernel,
        out_shape=jax.ShapeDtypeStruct((groups, capacity, width), send_rows.dtype),
        in_specs=[VMEM_SPEC, VMEM_SPEC, hbm, hbm, hbm],
        out_specs=VMEM_SPEC,
        scratch_shapes=moe_scratch(length, groups, capacity, gate_weight),
        compiler_params=pltpu.CompilerParams(
            collective_id=1, has_side_effects=True, vmem_limit_bytes=VMEM_BYTES
        ),
        name="moe",
    )(send_rows, gates, gate_weight, up_weight, down_weight.reshape(members * hidden, width))


def front_body(
    setup, query_hbm, key_hbm, value_hbm, sink_ref, weight_hbm, residual_hbm, mixer_hbm, expert_hbm,
    group_ref, member_ref, gate_ref,
    mixed_ref, rows_ref, placing_ref, gates_ref,
    query, span, attended, received, full, total, residual, gains,
    own_weight, prod, prod_pair, prod_inc, gate_rows,
    load_sem, halo_send, halo_recv, line_send, line_recv, plane_send, plane_recv,
    core_send, core_recv, row_send, row_recv, pair_send, pair_recv, sum_send, sum_recv,
    gate_send, gate_recv, gates_send, gates_recv,
):
    parts = lax.axis_size("tp")
    length = parts // CORES
    tp = lax.axis_index("tp")
    z, core = tp // CORES, lax.rem(tp, CORES)
    partner = z * CORES + 1 - core
    groups = lax.axis_size("sp")
    group = lax.axis_index("sp")
    last = length - 1
    halves = full.shape[2]
    relayed = groups == 4
    seq_rows = query.shape[0]
    heads_dev = query.shape[1] // HEAD_DIM
    blocks = seq_rows // BLOCK
    peers = [partner_slot(group, j, groups) for j in range(groups)]
    sides = (
        (lax.rem(z + length - 1, length) * CORES + core, z > 0),
        (lax.rem(z + 1, length) * CORES + core, z < last),
    )
    head_start = pl.multiple_of(tp * heads_dev // (HEADS // KV_HEADS) * HEAD_DIM, HEAD_DIM)
    inner = pl.ds(WINDOW, seq_rows)
    summed, gathered = own_weight.shape[3], full.shape[4]

    loads = [
        pltpu.make_async_copy(source, place, load_sem.at[n])
        for n, (source, place) in enumerate(
            (
                (weight_hbm.at[:, :, :, pl.ds(summed, gathered)], full.at[tp]),
                (key_hbm.at[:, pl.ds(head_start, HEAD_DIM)], span.at[0, inner]),
                (value_hbm.at[:, pl.ds(head_start, HEAD_DIM)], span.at[1, inner]),
                (query_hbm, query),
                (weight_hbm.at[:, :, :, pl.ds(0, summed)], own_weight),
                (residual_hbm, residual),
                (mixer_hbm, gains.at[0]),
                (expert_hbm, gains.at[1]),
            )
        )
    ]
    for copy in loads:
        copy.start()

    @pl.when(group == 0)
    def _():
        span[:, :WINDOW] = jnp.zeros((2, WINDOW, HEAD_DIM), span.dtype)

    @pl.when(z == 0)
    def _():
        for slot in range(length):
            prod_inc[slot] = jnp.zeros_like(prod_inc[slot])

    @pl.when(z == last)
    def _():
        for slot in [*range(last), length]:
            prod_inc[slot] = jnp.zeros_like(prod_inc[slot])

    @pl.when(group == groups - 1)
    def _():
        span[:, WINDOW + seq_rows :] = jnp.zeros((2, WINDOW, HEAD_DIM), span.dtype)

    started = setup()
    barrier = pltpu.get_barrier_semaphore()
    for shift in range(1, parts):
        pl.semaphore_signal(barrier, inc=1, device_id={"tp": lax.rem(tp + shift, parts)})
    for peer in peers[1:]:
        pl.semaphore_signal(barrier, inc=1, device_id={"sp": peer})
    pl.semaphore_wait(barrier, parts + groups - 2)

    def line(side, home, half):
        place = full.at[home * CORES + core, group, half]
        return pltpu.make_async_remote_copy(
            src_ref=place,
            dst_ref=place,
            send_sem=line_send.at[side, home, half],
            recv_sem=line_recv.at[home, half],
            device_id={"tp": sides[side][0]},
        )

    def plane(home, j, half, target, source):
        place = full.at[home * CORES + core, source, half]
        return pltpu.make_async_remote_copy(
            src_ref=place,
            dst_ref=place,
            send_sem=plane_send.at[home, j, half],
            recv_sem=plane_recv.at[home, j, half],
            device_id={"sp": target},
        )

    def relay(home, half):
        target, source = (peers[2], peers[1]) if half == 0 else (peers[1], peers[2])
        return plane(home, 3, half, target, source)

    def across(home):
        place = full.at[home * CORES + core]
        return pltpu.make_async_remote_copy(
            src_ref=place,
            dst_ref=place,
            send_sem=core_send.at[home],
            recv_sem=core_recv.at[home],
            device_id={"tp": partner},
        )

    def across_part(home, part, half):
        place = full.at[home * CORES + core, part, half]
        return pltpu.make_async_remote_copy(
            src_ref=place,
            dst_ref=place,
            send_sem=core_send.at[home],
            recv_sem=core_recv.at[home],
            device_id={"tp": partner},
        )

    def halo(side):
        start = WINDOW if side == 0 else seq_rows
        landing = WINDOW + seq_rows if side == 0 else 0
        return pltpu.make_async_remote_copy(
            src_ref=span.at[:, pl.ds(start, WINDOW)],
            dst_ref=span.at[:, pl.ds(landing, WINDOW)],
            send_sem=halo_send.at[side],
            recv_sem=halo_recv.at[side],
            device_id={"sp": lax.rem(group + (groups - 1 if side == 0 else 1), groups)},
        )

    def row_block(shift):
        target = lax.rem(tp + shift, parts)
        return pltpu.make_async_remote_copy(
            src_ref=attended.at[target],
            dst_ref=received.at[tp],
            send_sem=row_send.at[shift],
            recv_sem=row_recv.at[shift],
            device_id={"tp": target},
        )

    def share(home):
        return pltpu.make_async_remote_copy(
            src_ref=prod.at[home, 1 - core],
            dst_ref=prod_pair.at[home],
            send_sem=pair_send.at[home],
            recv_sem=pair_recv.at[home],
            device_id={"tp": partner},
        )

    def add_on(side, home):
        slot = home if side == 1 else jnp.where(home == z - 1, length, home)
        return pltpu.make_async_remote_copy(
            src_ref=prod.at[home, core],
            dst_ref=prod_inc.at[slot],
            send_sem=sum_send.at[home],
            recv_sem=sum_recv.at[slot],
            device_id={"tp": sides[side][0]},
        )

    def added(slot):
        return pltpu.make_async_remote_copy(
            src_ref=prod_inc.at[slot],
            dst_ref=prod_inc.at[slot],
            send_sem=sum_send.at[0],
            recv_sem=sum_recv.at[slot],
            device_id={"tp": partner},
        )

    def pass_on(side, home):
        share(home).wait_recv()

        @pl.when(sides[1 - side][1])
        def _():
            added(home).wait_recv()

        prod[home, core] = (
            prod[home, core].astype(jnp.float32)
            + prod_pair[home].astype(jnp.float32)
            + prod_inc[home].astype(jnp.float32)
        ).astype(prod.dtype)
        add_on(side, home).start()

    mirrored = [partner_slot(group, -j % groups, groups) for j in range(groups)]

    def gate_swap(j):
        return pltpu.make_async_remote_copy(
            src_ref=gate_rows.at[mirrored[j]],
            dst_ref=gates_ref.at[tp, j],
            send_sem=gate_send.at[j],
            recv_sem=gate_recv.at[j],
            device_id={"sp": mirrored[j]},
        )

    def gate_block(shift):
        place = gates_ref.at[tp]
        return pltpu.make_async_remote_copy(
            src_ref=place,
            dst_ref=place,
            send_sem=gates_send.at[shift],
            recv_sem=gates_recv.at[shift],
            device_id={"tp": lax.rem(tp + shift, parts)},
        )

    inward = (group > 0, group < groups - 1)
    loads[0].wait()
    for half in range(halves):
        for side in range(2):
            @pl.when(sides[side][1])
            def _(side=side, half=half):
                line(side, z, half).start()
    loads[1].wait()
    loads[2].wait()
    for side in range(2):
        @pl.when(inward[side])
        def _(side=side):
            halo(side).start()
    across(z).start()
    loads[3].wait()
    loads[4].wait()

    def attend(n, carry):
        b = jnp.where(n < blocks - 2, n + 1, jnp.where(n == blocks - 2, 0, blocks - 1))

        @pl.when(n == blocks - 2)
        def _():
            for side in range(2):
                @pl.when(inward[1 - side])
                def _(side=side):
                    halo(side).wait_recv()

        start = pl.multiple_of(b * BLOCK, BLOCK)
        wide = query[pl.ds(start, BLOCK), :]
        tall = jnp.concatenate(
            [wide[:, h * HEAD_DIM : (h + 1) * HEAD_DIM] for h in range(heads_dev)], axis=0
        )
        reach = BLOCK + 2 * WINDOW
        keys = span[0, pl.ds(start, reach), :]
        values = span[1, pl.ds(start, reach), :]
        scores = lax.dot_general(
            tall, keys, (((1,), (1,)), ((), ())), preferred_element_type=jnp.float32
        ) * HEAD_DIM ** (-0.5)
        shape = (heads_dev * BLOCK, reach)
        row = lax.broadcasted_iota(jnp.int32, shape, 0) % BLOCK
        column = lax.broadcasted_iota(jnp.int32, shape, 1)
        place = column + (group * seq_rows + b * BLOCK - WINDOW)
        inside = (
            (column >= row) & (column <= row + 2 * WINDOW)
            & (place >= 0) & (place < seq_rows * groups)
        )
        scores = jnp.where(inside, scores, NEG_BIG)
        which = lax.broadcasted_iota(jnp.int32, (heads_dev * BLOCK, 1), 0) // BLOCK
        sink = jnp.zeros((heads_dev * BLOCK, 1), jnp.float32)
        for h in range(heads_dev):
            sink = jnp.where(which == h, sink_ref[h], sink)
        top = jnp.maximum(jnp.max(scores, axis=1, keepdims=True), sink)
        terms = jnp.exp(scores - top)
        mass = jnp.sum(terms, axis=1, keepdims=True) + jnp.exp(sink - top)
        weight = (terms / mass).astype(jnp.bfloat16)
        result = jnp.dot(weight, values, preferred_element_type=jnp.float32).astype(jnp.bfloat16)
        attended[b] = jnp.concatenate(
            [result[h * BLOCK : (h + 1) * BLOCK] for h in range(heads_dev)], axis=1
        )
        return carry


    def homes(i):
        return ((z + 1 + i, z + 1 + i <= last), (z - 1 - i, z - 1 - i >= 0))

    def spread_half(i, half):
        for side in range(2):
            home, live = homes(i)[side]

            @pl.when(live)
            def _(side=side, home=home):
                line(side, home, half).wait_recv()

                @pl.when(sides[side][1])
                def _():
                    line(side, home, half).start()

                across_part(home, group, half).start()
                if not relayed:
                    for j in range(1, groups):
                        plane(home, j, half, peers[j], group).start()
                elif half == 0:
                    plane(home, 1, 0, peers[1], group).start()
                else:
                    plane(home, 2, 1, peers[2], group).start()
                    plane(home, 1, 1, peers[1], group).start()
                    plane(home, 2, 0, peers[2], group).start()

    def relay_half(i, half):
        for side in range(2):
            home, live = homes(i)[side]

            @pl.when(live)
            def _(home=home):
                plane(home, 1 + half, half, peers[1], group).wait_recv()
                relay(home, half).start()
                across_part(home, peers[1 + half], half).start()

    def multiply(home, carry):
        lhs = jnp.concatenate([attended[home * CORES + c] for c in range(CORES)], axis=0)
        part = jnp.dot(
            lhs, own_weight[...].reshape(-1, summed), preferred_element_type=jnp.float32
        )
        prod[home] = part.astype(prod.dtype).reshape(CORES, -1, summed)
        share(home).start()
        return carry

    depths = (last - z, z)

    def add_step(r):
        for side in range(2):
            event = r - (depths[side] - 1)
            home = last - event if side == 1 else event

            @pl.when((depths[side] > 0) & (event >= 0) & (event < depths[1 - side]))
            def _(side=side, home=home):
                pass_on(side, home)

    def spread(i):
        for half in range(halves):
            spread_half(i, half)
        if relayed:
            for half in range(halves):
                relay_half(i, half)

    def first_sums():
        for side in range(2):
            @pl.when(depths[side] == 0)
            def _(side=side):
                for event in range(last):
                    pass_on(side, last - event if side == 1 else event)

    def send_rows():
        for shift in range(1, parts):
            row_block(shift).start()

    lax.fori_loop(0, blocks, attend, 0)
    received[tp] = attended[tp]
    send_rows()
    lax.fori_loop(0, length, multiply, 0)
    spread(0)
    first_sums()
    capacity = rows_ref.shape[1]
    slots = groups * capacity
    tok_rows = residual.shape[0]
    width = residual.shape[1]
    names = lax.broadcasted_iota(jnp.int32, (groups * (8 // min(groups, 8)), tok_rows), 0)
    chosen = (names == group_ref[...]).astype(jnp.float32)
    earlier = (
        lax.broadcasted_iota(jnp.int32, (tok_rows, tok_rows), 0)
        < lax.broadcasted_iota(jnp.int32, (tok_rows, tok_rows), 1)
    ).astype(jnp.bfloat16)
    rank = jnp.dot(chosen.astype(jnp.bfloat16), earlier, preferred_element_type=jnp.float32)
    slot_row = jnp.sum(
        chosen * (rank + (names * capacity).astype(jnp.float32)), axis=0, keepdims=True
    )
    placing = (
        lax.broadcasted_iota(jnp.int32, (slots, tok_rows), 0).astype(jnp.float32) == slot_row
    ).astype(jnp.bfloat16)
    placing_ref[...] = placing.reshape(placing_ref.shape)
    members = lax.broadcasted_iota(jnp.int32, (GATE_ROWS, tok_rows), 0)
    tail = jnp.zeros((GATE_ROWS, tok_rows), jnp.float32)
    for k in range(member_ref.shape[0]):
        tail = tail + jnp.where(
            members == member_ref[k : k + 1, :], gate_ref[k : k + 1, :].astype(jnp.float32), 0.0
        )
    place = lax.broadcasted_iota(jnp.int32, (LANES, tok_rows), 0)
    for g in range(groups):
        chosen_slot = jnp.where(place < capacity, place + g * capacity, slots).astype(jnp.float32)
        gate_rows[g] = lax.dot_general(
            tail.astype(jnp.bfloat16), (chosen_slot == slot_row).astype(jnp.bfloat16),
            (((1,), (1,)), ((), ())), preferred_element_type=jnp.float32,
        ).astype(gate_rows.dtype)
    gates_ref[tp, 0] = gate_rows[group]
    for j in range(1, groups):
        gate_swap(j).start()
    for i in range(1, last):
        add_step(i - 1)
        spread(i)

    def project(home, first):
        pieces = [received[home * CORES + c] for c in range(CORES)]
        lhs = jnp.concatenate(pieces, axis=1)
        rhs = jnp.concatenate(
            [full[home * CORES + c].reshape(-1, gathered) for c in range(CORES)], axis=0
        )
        part = jnp.dot(lhs, rhs, preferred_element_type=jnp.float32)
        if first:
            total[:, summed:] = part
        else:
            total[:, summed:] += part

    def rows_from(home):
        for c in range(CORES):
            source = home * CORES + c

            @pl.when(source != tp)
            def _(source=source):
                shift = lax.rem(tp - source + parts, parts)
                pltpu.make_async_remote_copy(
                    src_ref=attended.at[source],
                    dst_ref=received.at[source],
                    send_sem=row_send.at[0],
                    recv_sem=row_recv.at[lax.rem(parts + tp - source, parts)],
                    device_id={"tp": partner},
                ).wait_recv()

    for j in range(1, groups):
        gate_swap(j).wait_recv()
    for shift in range(1, parts):
        gate_block(shift).start()
    across(z).wait_recv()
    rows_from(z)
    project(z, True)

    def gather_step(i, carry):
        for side in range(2):
            home, live = homes(i)[side]

            @pl.when(live)
            def _(home=home):
                for half in range(halves):
                    for j in range(1, groups):
                        if not (relayed and j == 1 + half and j < 3):
                            plane(home, j, half, peers[1], group).wait_recv()
                            across_part(home, peers[j], half).start()

        for side in range(2):
            home, live = homes(i)[side]

            @pl.when(live)
            def _(home=home):
                across(home).wait_recv()
                rows_from(home)
                project(home, False)

        return carry

    lax.fori_loop(0, last, gather_step, 0)

    share(z).wait_recv()

    @pl.when(z > 0)
    def _():
        added(z).wait_recv()

    @pl.when(z < last)
    def _():
        added(length).wait_recv()

    total[:, :summed] = (
        prod[z, core].astype(jnp.float32)
        + prod_pair[z].astype(jnp.float32)
        + prod_inc[z].astype(jnp.float32)
        + prod_inc[length].astype(jnp.float32)
    )
    for copy in loads[5:]:
        copy.wait()
    projected = total[...]
    scale = lax.rsqrt(jnp.mean(projected * projected, axis=1, keepdims=True) + EPS)
    mixed = (
        residual[...].astype(jnp.float32) + gains[0] * (projected * scale)
    ).astype(jnp.bfloat16)
    mixed_ref[...] = mixed
    mixed_float = mixed.astype(jnp.float32)
    norm = lax.rsqrt(jnp.mean(mixed_float * mixed_float, axis=1, keepdims=True) + EPS)
    normed = (mixed_float * norm * gains[1]).astype(jnp.bfloat16)
    rows_ref[...] = (
        jnp.dot(placing, normed, preferred_element_type=jnp.float32)
        .astype(rows_ref.dtype)
        .reshape(rows_ref.shape)
    )

    for shift in range(1, parts):
        gate_block(shift).wait_recv()

    def settle():
        for side in range(2):
            @pl.when(inward[side])
            def _(side=side):
                halo(side).wait_send()
        for shift in range(1, parts):
            row_block(shift).wait_send()
            gate_block(shift).wait_send()
        for j in range(1, groups):
            gate_swap(j).wait_send()

        def drain(home, carry):
            for half in range(halves):
                @pl.when((home >= z) & sides[0][1])
                def _(half=half):
                    line(0, home, half).wait_send()

                @pl.when((home <= z) & sides[1][1])
                def _(half=half):
                    line(1, home, half).wait_send()

                @pl.when(home != z)
                def _(half=half):
                    for j in range(1, groups):
                        plane(home, j, half, peers[1], group).wait_send()

            @pl.when(home != z)
            def _():
                add_on(1, home).wait_send()

            across(home).wait_send()
            share(home).wait_send()
            return carry

        lax.fori_loop(0, length, drain, 0)

    return started, settle


def front_kernel(*refs):
    _, settle = front_body(lambda: None, *refs)
    settle()


def front_scratch(parts, groups, queries, residual):
    length = parts // CORES
    seq_rows, columns = queries.shape
    tok_rows, width = residual.shape
    halves = 2 if groups == 4 else 1
    piece = columns // (groups * halves)
    summed = SUMMED_EIGHTHS * width // 8 // LANES * LANES
    sem = pltpu.SemaphoreType.DMA
    kind = queries.dtype
    return [
        pltpu.VMEM((seq_rows, columns), kind),
        pltpu.VMEM((2, seq_rows + 2 * WINDOW, HEAD_DIM), kind),
        pltpu.VMEM((parts, tok_rows, columns), kind),
        pltpu.VMEM((parts, tok_rows, columns), kind),
        pltpu.VMEM((parts, groups, halves, piece, width - summed), kind),
        pltpu.VMEM((tok_rows, width), jnp.float32),
        pltpu.VMEM((tok_rows, width), kind),
        pltpu.VMEM((2, 1, width), jnp.float32),
        pltpu.VMEM((groups, halves, piece, summed), kind),
        pltpu.VMEM((length, CORES, tok_rows, summed), kind),
        pltpu.VMEM((length, tok_rows, summed), kind),
        pltpu.VMEM((length + 1, tok_rows, summed), kind),
        pltpu.VMEM((groups, GATE_ROWS, LANES), kind),
        sem((8,)),
        sem((2,)),
        sem((2,)),
        sem((2, length, halves)),
        sem((length, halves)),
        sem((length, groups, halves)),
        sem((length, groups, halves)),
        sem((length,)),
        sem((length,)),
        sem((parts,)),
        sem((parts,)),
        sem((length,)),
        sem((length,)),
        sem((length,)),
        sem((length + 1,)),
        sem((groups,)),
        sem((groups,)),
        sem((parts,)),
        sem((parts,)),
    ]


HBM_SPEC = pl.BlockSpec(memory_space=pltpu.HBM)
FRONT_SPECS = (
    *[HBM_SPEC] * 3, pl.BlockSpec(memory_space=pltpu.SMEM), *[HBM_SPEC] * 4, *[VMEM_SPEC] * 3
)


def front_made(groups, capacity, residual):
    tok_rows, width = residual.shape
    return (
        ((tok_rows, width), residual.dtype),
        ((groups, capacity, width), residual.dtype),
        ((groups, capacity, tok_rows), residual.dtype),
        ((lax.axis_size("tp"), groups, GATE_ROWS, LANES), residual.dtype),
    )


def front(arguments, capacity):
    parts, groups = lax.axis_size("tp"), lax.axis_size("sp")
    made = front_made(groups, capacity, arguments[5])
    return pl.pallas_call(
        front_kernel,
        out_shape=[jax.ShapeDtypeStruct(*each) for each in made],
        in_specs=FRONT_SPECS,
        out_specs=[VMEM_SPEC] * 4,
        scratch_shapes=front_scratch(parts, groups, arguments[0], arguments[5]),
        compiler_params=pltpu.CompilerParams(
            collective_id=0, has_side_effects=True, vmem_limit_bytes=VMEM_BYTES
        ),
        name="front",
    )(*arguments)


def layer_kernel(inputs, front_count, moe_count, *refs):
    front_in, refs = refs[:inputs], refs[inputs:]
    weights_in, out_ref, refs = refs[:3], refs[3], refs[4:]
    front_refs, refs = refs[:front_count], refs[front_count:]
    *buffers, weight_sem = refs[:moe_count]
    mixed_ref, rows_ref, placing_ref, gates_ref, returned = refs[moe_count:]

    def setup():
        return moe_setup(*weights_in, buffers[3], *buffers[4:7], weight_sem)

    weights, settle = front_body(
        setup, *front_in, mixed_ref, rows_ref, placing_ref, gates_ref, *front_refs
    )
    total = front_refs[5]

    def landed(j, group):
        part = lax.dot_general(
            placing_ref[group], returned[group], (((0,), (0,)), ((), ())),
            preferred_element_type=jnp.float32,
        )
        total[...] = (mixed_ref[...].astype(jnp.float32) if j == 0 else total[...]) + part

    moe_body(weights, landed, rows_ref, gates_ref, returned, *buffers)
    out_ref[...] = total[...].astype(out_ref.dtype)
    settle()


def layer(arguments, capacity, gate_weight, up_weight, down_weight, front_bufs, moe_bufs):
    residual = arguments[5]
    groups = lax.axis_size("sp")
    kept = front_made(groups, capacity, residual)
    returned = ((groups, capacity, residual.shape[1]), residual.dtype)
    return pl.pallas_call(
        functools.partial(layer_kernel, len(arguments), len(front_bufs), len(moe_bufs)),
        out_shape=jax.ShapeDtypeStruct(residual.shape, residual.dtype),
        in_specs=[*FRONT_SPECS, *[HBM_SPEC] * 3],
        out_specs=VMEM_SPEC,
        scratch_shapes=[
            *front_bufs, *moe_bufs, *[pltpu.VMEM(*each) for each in (*kept, returned)]
        ],
        compiler_params=pltpu.CompilerParams(
            collective_id=2, has_side_effects=True, vmem_limit_bytes=VMEM_BYTES
        ),
        name="layer",
    )(*arguments, gate_weight, up_weight, down_weight.reshape(-1, residual.shape[1]))


def per_device(
    queries,
    key_heads,
    value_heads,
    sink_logit,
    out_weight,
    residual,
    mixer_gain,
    expert_gain,
    route_group,
    route_member,
    route_weight,
    gate_weight,
    up_weight,
    down_weight,
):
    tok_rows, width = residual.shape
    parts, groups = lax.axis_size("tp"), lax.axis_size("sp")
    capacity = max(2, (5 * tok_rows + 4 * groups - 1) // (4 * groups))
    capacity = (capacity + 7) // 8 * 8
    halves = 2 if groups == 4 else 1
    arguments = (
        queries, key_heads, value_heads, sink_logit,
        out_weight.reshape(groups, halves, -1, width), residual,
        mixer_gain.reshape(1, width), expert_gain.reshape(1, width),
        route_group.reshape(1, tok_rows), route_member.T, route_weight.T,
    )
    front_bufs = front_scratch(parts, groups, queries, residual)
    moe_bufs = moe_scratch(parts // CORES, groups, capacity, gate_weight)
    held = sum(
        math.prod(each.shape) * jnp.dtype(each.dtype).itemsize
        for each in (*front_bufs, *moe_bufs)
        if getattr(each, "memory_space", None) == pltpu.VMEM
    )
    if held < VMEM_BYTES * 3 // 4:
        return layer(
            arguments, capacity, gate_weight, up_weight, down_weight, front_bufs, moe_bufs
        )
    mixed_rows, send_rows, placing, gates = front(arguments, capacity)
    returned = moe(send_rows, gates, gate_weight, up_weight, down_weight)
    expert_out = lax.dot_general(
        placing.reshape(-1, tok_rows),
        returned.reshape(-1, width),
        (((0,), (0,)), ((), ())),
        preferred_element_type=jnp.float32,
    )
    return (mixed_rows.astype(jnp.float32) + expert_out).astype(jnp.bfloat16)


def solution(mesh):
    placed = (
        P("sp", "tp"),
        P("sp", None),
        P("sp", None),
        P("tp"),
        P("tp", None),
        P(("sp", "tp"), None),
        P(),
        P(),
        P(("sp", "tp")),
        P(("sp", "tp"), None),
        P(("sp", "tp"), None),
        P("sp", None, "tp"),
        P("sp", None, "tp"),
        P("sp", "tp", None),
    )
    return jax.shard_map(
        per_device, mesh=mesh, in_specs=placed, out_specs=P(("sp", "tp"), None), check_vma=False
    )
```

```python
import functools
import math

import jax
import jax.numpy as jnp
from jax import lax
from jax.experimental import pallas as pl
from jax.experimental.pallas import tpu as pltpu
from jax.sharding import PartitionSpec as P

HEADS = 16
KV_HEADS = 4
HEAD_DIM = 128
WINDOW = 128
BLOCK = 128


EPS = 1e-06
NEG_BIG = -1e30


CORES = 2
LANES = 128
VMEM_BYTES = 67043328
SUMMED_EIGHTHS = 3
GATE_ROWS = 8
VMEM_SPEC = pl.BlockSpec(memory_space=pltpu.VMEM)


def greet(neighbours, partner, peers):
    barrier = pltpu.get_barrier_semaphore()
    for target in (*neighbours, partner):
        pl.semaphore_signal(barrier, inc=1, device_id={"tp": target})
    for peer in peers:
        pl.semaphore_signal(barrier, inc=1, device_id={"sp": peer})
    pl.semaphore_wait(barrier, 3 + len(peers))


def line_sequence(i, position, length, side):
    reach = length - 1 - position if side == 0 else position
    early = i < reach
    offset = jnp.where(early, i + 1, 2 * reach - i)
    home = position + offset if side == 0 else position - offset
    return home, jnp.where(early, 0, 1)


def partner_slot(mine, j, groups):
    total, bit = 0, 1
    while bit < groups:
        total = total + lax.rem(mine // bit + j // bit, 2) * bit
        bit *= 2
    return total


def moe_setup(gate_hbm, up_hbm, down_hbm, inc, gate_ref, up_ref, down_ref, weight_sem):
    length = lax.axis_size("tp") // CORES
    z, last = lax.axis_index("tp") // CORES, length - 1
    weights = [
        pltpu.make_async_copy(source, place, weight_sem.at[n])
        for n, (source, place) in enumerate(
            ((gate_hbm, gate_ref), (up_hbm, up_ref), (down_hbm, down_ref))
        )
    ]
    for copy in weights:
        copy.start()

    @pl.when((z == 0) | (z == last))
    def _():
        for slot in range(length):
            @pl.when(slot != last * (z // last))
            def _():
                inc[slot] = jnp.zeros_like(inc[slot])

        @pl.when(z == 0)
        def _():
            inc[0] = jnp.zeros_like(inc[0])

        @pl.when(z == last)
        def _():
            inc[length] = jnp.zeros_like(inc[length])
    return weights


def moe_body(
    weights, landed, send_ref, gates_ref, out_ref,
    rows, res, pair, inc, gate_ref, up_ref, down_ref,
    own_sem, swap_send, swap_recv, line_send, line_recv, core_send, core_recv,
    pair_send, pair_recv, sum_send, sum_recv, home_send, home_recv,
):
    length = lax.axis_size("tp") // CORES
    tp = lax.axis_index("tp")
    z, core = tp // CORES, lax.rem(tp, CORES)
    partner = z * CORES + 1 - core
    groups = lax.axis_size("sp")
    group = lax.axis_index("sp")
    near = groups // 2
    width = out_ref.shape[2]
    last = length - 1
    sides = (
        (lax.rem(z + length - 1, length) * CORES + core, z > 0),
        (lax.rem(z + 1, length) * CORES + core, z < last),
    )
    peers = [partner_slot(group, -j % groups, groups) for j in range(groups)]

    def swap(j):
        return pltpu.make_async_remote_copy(
            src_ref=send_ref.at[peers[j]],
            dst_ref=rows.at[z * 2 + j // near, core, j % near],
            send_sem=swap_send.at[j],
            recv_sem=swap_recv.at[j],
            device_id={"sp": peers[j]},
        )

    def line(side, index, j):
        place = rows.at[index, core, j]
        return pltpu.make_async_remote_copy(
            src_ref=place,
            dst_ref=place,
            send_sem=line_send.at[side, index, j],
            recv_sem=line_recv.at[index, j],
            device_id={"tp": sides[side][0]},
        )

    def across(index, j):
        place = rows.at[index, core, j]
        return pltpu.make_async_remote_copy(
            src_ref=place,
            dst_ref=place,
            send_sem=core_send.at[index, j],
            recv_sem=core_recv.at[index, j],
            device_id={"tp": partner},
        )

    def share(index):
        return pltpu.make_async_remote_copy(
            src_ref=res.at[index, 1 - core],
            dst_ref=pair.at[index],
            send_sem=pair_send.at[index],
            recv_sem=pair_recv.at[index],
            device_id={"tp": partner},
        )

    def slot_of(side, target):
        if side == 1:
            return target
        return jnp.where(target == z - 1, length, target)

    def add_on(side, target, half, j):
        slot = slot_of(side, target)
        return pltpu.make_async_remote_copy(
            src_ref=res.at[target * 2 + half, core, j],
            dst_ref=inc.at[slot, half, j],
            send_sem=sum_send.at[target * 2 + half, j],
            recv_sem=sum_recv.at[slot, half, j],
            device_id={"tp": sides[side][0]},
        )

    def added(slot, half, j):
        return pltpu.make_async_remote_copy(
            src_ref=inc.at[slot, half, j],
            dst_ref=inc.at[slot, half, j],
            send_sem=sum_send.at[0, j],
            recv_sem=sum_recv.at[slot, half, j],
            device_id={"tp": partner},
        )

    def back(half, j):
        return pltpu.make_async_remote_copy(
            src_ref=res.at[z * 2 + half, core, j],
            dst_ref=out_ref.at[group],
            send_sem=home_send.at[half * near + j],
            recv_sem=home_recv.at[half * near + j],
            device_id={"sp": peers_at(half, j)},
        )

    def peers_at(half, j):
        return peers[half * near + j]

    def forward(side, index, j):
        @pl.when(sides[side][1])
        def _():
            line(side, index, j).start()

    own = pltpu.make_async_copy(send_ref.at[group], rows.at[z * 2, core, 0], own_sem)
    own.start()
    for j in range(1, groups):
        swap(j).start()
    for j in range(near):
        if j == 0:
            own.wait()
        else:
            swap(j).wait_recv()
        for side in range(2):
            forward(side, z * 2, j)
        across(z * 2, j).start()
    for j in range(near):
        swap(near + j).wait_recv()
        across(z * 2 + 1, j).start()
    for copy in weights:
        copy.wait()

    def expert_rows(index):
        for j in range(near):
            across(index, j).wait_recv()
        block = rows[index].reshape(2 * near * rows.shape[3], rows.shape[4])
        home, half = index // 2, lax.rem(index, 2)
        gates = jnp.concatenate(
            [
                gates_ref[home * CORES + c, half * near + j].astype(jnp.float32).T[: rows.shape[3]]
                for c in range(CORES) for j in range(near)
            ],
            axis=0,
        )
        hidden = []
        for member in range(gate_ref.shape[0]):
            gate_pre = jnp.dot(block, gate_ref[member], preferred_element_type=jnp.float32)
            up_pre = jnp.dot(block, up_ref[member], preferred_element_type=jnp.float32)
            value = gate_pre / (1.0 + jnp.exp(-gate_pre)) * up_pre * gates[:, member : member + 1]
            hidden.append(value.astype(jnp.bfloat16))
        total = jnp.dot(
            jnp.concatenate(hidden, axis=1), down_ref[...], preferred_element_type=jnp.float32
        )
        res[index] = total.astype(res.dtype).reshape(res.shape[1:])
        share(index).start()

    def pass_on(side, i):
        target, half = line_sequence(i, z, length, 1 - side)
        index = target * 2 + half
        share(index).wait_recv()
        for j in range(near):
            @pl.when(sides[1 - side][1])
            def _():
                added(target, half, j).wait_recv()
            value = (
                res[index, core, j].astype(jnp.float32)
                + pair[index, j].astype(jnp.float32)
                + inc[target, half, j].astype(jnp.float32)
            )
            res[index, core, j] = value.astype(res.dtype)
            add_on(side, target, half, j).start()

    def finish(half):
        index = z * 2 + half
        share(index).wait_recv()
        for j in range(near):
            @pl.when(z > 0)
            def _():
                added(z, half, j).wait_recv()

            @pl.when(z < last)
            def _():
                added(length, half, j).wait_recv()
            value = (
                res[index, core, j].astype(jnp.float32)
                + pair[index, j].astype(jnp.float32)
                + inc[z, half, j].astype(jnp.float32)
                + inc[length, half, j].astype(jnp.float32)
            ).astype(res.dtype)
            if half == 0 and j == 0:
                out_ref[group] = value
            else:
                res[index, core, j] = value
                back(half, j).start()

    reaches = (last - z, z)
    lags = tuple(jnp.where(depth == 0, 0, 2 * depth + 1) for depth in (last - z, z))

    spare = max(0, 2 * last - 2)

    def step(k, carry):
        for j in range(near):
            for side in range(2):
                home, half = line_sequence(k, z, length, side)

                @pl.when(k < 2 * reaches[side])
                def _(side=side, index=home * 2 + half, j=j):
                    line(side, index, j).wait_recv()
                    forward(side, index, j)
                    across(index, j).start()
        for side in range(2):
            @pl.when(k == jnp.maximum(2 * reaches[side] - 1, 0))
            def _(side=side):
                for j in range(near):
                    forward(side, z * 2 + 1, j)

        for side in range(2):
            i = k - lags[side]

            @pl.when((lags[side] > 0) & (i >= 0) & (i < 2 * reaches[1 - side]))
            def _(side=side, i=i):
                pass_on(side, i)

        def job(d, inner):
            home0, half0 = line_sequence(k, z, length, 0)
            home1, half1 = line_sequence(k, z, length, 1)
            index = jnp.where(
                d == 0, home0 * 2 + half0, jnp.where(d == 1, home1 * 2 + half1, z * 2 + k - spare)
            )
            live = jnp.where(
                d == 0, k < 2 * reaches[0],
                jnp.where(d == 1, k < 2 * reaches[1], (k == spare) | (k == spare + 1)),
            )

            @pl.when(live)
            def _():
                expert_rows(index)

            return inner

        lax.fori_loop(0, 3, job, 0)
        for side in range(2):
            @pl.when((lags[side] == 0) & (k < 2 * reaches[1 - side]))
            def _(side=side):
                pass_on(side, k)

        @pl.when(k == 2 * jnp.maximum(z, last - z))
        def _():
            finish(0)

        return carry

    lax.fori_loop(0, 2 * length - 1, step, 0)
    finish(1)

    for j in range(groups):
        if j > 0:
            back(j // near, j % near).wait_recv()
        landed(j, peers[j])
    for j in range(1, groups):
        swap(j).wait_send()
        back(j // near, j % near).wait_send()

    def drain(index, carry):
        home = index // 2
        for j in range(near):
            @pl.when((home >= z) & sides[0][1])
            def _(j=j):
                line(0, index, j).wait_send()

            @pl.when((home <= z) & sides[1][1])
            def _(j=j):
                line(1, index, j).wait_send()

            across(index, j).wait_send()

            @pl.when(home != z)
            def _(j=j):
                add_on(1, home, lax.rem(index, 2), j).wait_send()
        share(index).wait_send()
        return carry

    lax.fori_loop(0, 2 * length, drain, 0)


def moe_kernel(send_ref, gates_ref, gate_hbm, up_hbm, down_hbm, out_ref, *scratch):
    *buffers, weight_sem = scratch
    inc, places = buffers[3], buffers[4:7]
    weights = moe_setup(gate_hbm, up_hbm, down_hbm, inc, *places, weight_sem)
    z, core = lax.axis_index("tp") // CORES, lax.rem(lax.axis_index("tp"), CORES)
    length, groups = lax.axis_size("tp") // CORES, lax.axis_size("sp")
    around = [lax.rem(z + shift, length) * CORES + core for shift in (length - 1, 1)]
    others = [lax.rem(lax.axis_index("sp") + shift, groups) for shift in range(1, groups)]
    greet(around, z * CORES + 1 - core, others)
    moe_body(weights, lambda j, group: None, send_ref, gates_ref, out_ref, *buffers)


def moe_scratch(length, groups, capacity, gate_weight):
    members, width, hidden = gate_weight.shape
    near = groups // 2
    kind = gate_weight.dtype
    sem = pltpu.SemaphoreType.DMA
    return [
        pltpu.VMEM((2 * length, 2, near, capacity, width), kind),
        pltpu.VMEM((2 * length, 2, near, capacity, width), kind),
        pltpu.VMEM((2 * length, near, capacity, width), kind),
        pltpu.VMEM((length + 1, 2, near, capacity, width), kind),
        pltpu.VMEM((members, width, hidden), kind),
        pltpu.VMEM((members, width, hidden), kind),
        pltpu.VMEM((members * hidden, width), kind),
        sem,
        sem((groups,)),
        sem((groups,)),
        sem((2, 2 * length, near)),
        sem((2 * length, near)),
        sem((2 * length, near)),
        sem((2 * length, near)),
        sem((2 * length,)),
        sem((2 * length,)),
        sem((2 * length, near)),
        sem((length + 1, 2, near)),
        sem((groups,)),
        sem((groups,)),
        sem((3,)),
    ]


def moe(send_rows, gates, gate_weight, up_weight, down_weight):
    groups, capacity, _ = send_rows.shape
    members, width, hidden = gate_weight.shape
    length = lax.axis_size("tp") // CORES
    hbm = pl.BlockSpec(memory_space=pltpu.HBM)
    return pl.pallas_call(
        moe_kernel,
        out_shape=jax.ShapeDtypeStruct((groups, capacity, width), send_rows.dtype),
        in_specs=[VMEM_SPEC, VMEM_SPEC, hbm, hbm, hbm],
        out_specs=VMEM_SPEC,
        scratch_shapes=moe_scratch(length, groups, capacity, gate_weight),
        compiler_params=pltpu.CompilerParams(
            collective_id=1, has_side_effects=True, vmem_limit_bytes=VMEM_BYTES
        ),
        name="moe",
    )(send_rows, gates, gate_weight, up_weight, down_weight.reshape(members * hidden, width))


def front_body(
    setup, query_hbm, key_hbm, value_hbm, sink_ref, weight_hbm, residual_hbm, mixer_hbm, expert_hbm,
    group_ref, member_ref, gate_ref,
    mixed_ref, rows_ref, placing_ref, gates_ref,
    query, span, attended, received, full, total, residual, gains,
    own_weight, prod, prod_pair, prod_inc, gate_rows,
    load_sem, halo_send, halo_recv, line_send, line_recv, plane_send, plane_recv,
    core_send, core_recv, row_send, row_recv, pair_send, pair_recv, sum_send, sum_recv,
    gate_send, gate_recv, gates_send, gates_recv,
):
    parts = lax.axis_size("tp")
    length = parts // CORES
    tp = lax.axis_index("tp")
    z, core = tp // CORES, lax.rem(tp, CORES)
    partner = z * CORES + 1 - core
    groups = lax.axis_size("sp")
    group = lax.axis_index("sp")
    last = length - 1
    halves = full.shape[2]
    relayed = groups == 4
    seq_rows = query.shape[0]
    heads_dev = query.shape[1] // HEAD_DIM
    blocks = seq_rows // BLOCK
    peers = [partner_slot(group, j, groups) for j in range(groups)]
    sides = (
        (lax.rem(z + length - 1, length) * CORES + core, z > 0),
        (lax.rem(z + 1, length) * CORES + core, z < last),
    )
    head_start = pl.multiple_of(tp * heads_dev // (HEADS // KV_HEADS) * HEAD_DIM, HEAD_DIM)
    inner = pl.ds(WINDOW, seq_rows)
    summed, gathered = own_weight.shape[3], full.shape[4]

    loads = [
        pltpu.make_async_copy(source, place, load_sem.at[n])
        for n, (source, place) in enumerate(
            (
                (weight_hbm.at[:, :, :, pl.ds(summed, gathered)], full.at[tp]),
                (key_hbm.at[:, pl.ds(head_start, HEAD_DIM)], span.at[0, inner]),
                (value_hbm.at[:, pl.ds(head_start, HEAD_DIM)], span.at[1, inner]),
                (query_hbm, query),
                (weight_hbm.at[:, :, :, pl.ds(0, summed)], own_weight),
                (residual_hbm, residual),
                (mixer_hbm, gains.at[0]),
                (expert_hbm, gains.at[1]),
            )
        )
    ]
    for copy in loads:
        copy.start()

    @pl.when(group == 0)
    def _():
        span[:, :WINDOW] = jnp.zeros((2, WINDOW, HEAD_DIM), span.dtype)

    @pl.when(z == 0)
    def _():
        for slot in range(length):
            prod_inc[slot] = jnp.zeros_like(prod_inc[slot])

    @pl.when(z == last)
    def _():
        for slot in [*range(last), length]:
            prod_inc[slot] = jnp.zeros_like(prod_inc[slot])

    @pl.when(group == groups - 1)
    def _():
        span[:, WINDOW + seq_rows :] = jnp.zeros((2, WINDOW, HEAD_DIM), span.dtype)

    started = setup()
    barrier = pltpu.get_barrier_semaphore()
    for shift in range(1, parts):
        pl.semaphore_signal(barrier, inc=1, device_id={"tp": lax.rem(tp + shift, parts)})
    for peer in peers[1:]:
        pl.semaphore_signal(barrier, inc=1, device_id={"sp": peer})
    capacity = rows_ref.shape[1]
    slots = groups * capacity
    tok_rows = residual.shape[0]
    width = residual.shape[1]
    names = lax.broadcasted_iota(jnp.int32, (groups * (8 // min(groups, 8)), tok_rows), 0)
    chosen = (names == group_ref[...]).astype(jnp.float32)
    earlier = (
        lax.broadcasted_iota(jnp.int32, (tok_rows, tok_rows), 0)
        < lax.broadcasted_iota(jnp.int32, (tok_rows, tok_rows), 1)
    ).astype(jnp.bfloat16)
    rank = jnp.dot(chosen.astype(jnp.bfloat16), earlier, preferred_element_type=jnp.float32)
    slot_row = jnp.sum(
        chosen * (rank + (names * capacity).astype(jnp.float32)), axis=0, keepdims=True
    )
    placing = (
        lax.broadcasted_iota(jnp.int32, (slots, tok_rows), 0).astype(jnp.float32) == slot_row
    ).astype(jnp.bfloat16)
    placing_ref[...] = placing.reshape(placing_ref.shape)
    members = lax.broadcasted_iota(jnp.int32, (GATE_ROWS, tok_rows), 0)
    tail = jnp.zeros((GATE_ROWS, tok_rows), jnp.float32)
    for k in range(member_ref.shape[0]):
        tail = tail + jnp.where(
            members == member_ref[k : k + 1, :], gate_ref[k : k + 1, :].astype(jnp.float32), 0.0
        )
    place = lax.broadcasted_iota(jnp.int32, (LANES, tok_rows), 0)
    for g in range(groups):
        chosen_slot = jnp.where(place < capacity, place + g * capacity, slots).astype(jnp.float32)
        gate_rows[g] = lax.dot_general(
            tail.astype(jnp.bfloat16), (chosen_slot == slot_row).astype(jnp.bfloat16),
            (((1,), (1,)), ((), ())), preferred_element_type=jnp.float32,
        ).astype(gate_rows.dtype)
    pl.semaphore_wait(barrier, parts + groups - 2)

    def line(side, home, half):
        place = full.at[home * CORES + core, group, half]
        return pltpu.make_async_remote_copy(
            src_ref=place,
            dst_ref=place,
            send_sem=line_send.at[side, home, half],
            recv_sem=line_recv.at[home, half],
            device_id={"tp": sides[side][0]},
        )

    def plane(home, j, half, target, source):
        place = full.at[home * CORES + core, source, half]
        return pltpu.make_async_remote_copy(
            src_ref=place,
            dst_ref=place,
            send_sem=plane_send.at[home, j, half],
            recv_sem=plane_recv.at[home, j, half],
            device_id={"sp": target},
        )

    def relay(home, half):
        target, source = (peers[2], peers[1]) if half == 0 else (peers[1], peers[2])
        return plane(home, 3, half, target, source)

    def across(home):
        place = full.at[home * CORES + core]
        return pltpu.make_async_remote_copy(
            src_ref=place,
            dst_ref=place,
            send_sem=core_send.at[home],
            recv_sem=core_recv.at[home],
            device_id={"tp": partner},
        )

    def across_part(home, part, half):
        place = full.at[home * CORES + core, part, half]
        return pltpu.make_async_remote_copy(
            src_ref=place,
            dst_ref=place,
            send_sem=core_send.at[home],
            recv_sem=core_recv.at[home],
            device_id={"tp": partner},
        )

    def halo(side):
        start = WINDOW if side == 0 else seq_rows
        landing = WINDOW + seq_rows if side == 0 else 0
        return pltpu.make_async_remote_copy(
            src_ref=span.at[:, pl.ds(start, WINDOW)],
            dst_ref=span.at[:, pl.ds(landing, WINDOW)],
            send_sem=halo_send.at[side],
            recv_sem=halo_recv.at[side],
            device_id={"sp": lax.rem(group + (groups - 1 if side == 0 else 1), groups)},
        )

    def row_block(shift):
        target = lax.rem(tp + shift, parts)
        return pltpu.make_async_remote_copy(
            src_ref=attended.at[target],
            dst_ref=received.at[tp],
            send_sem=row_send.at[shift],
            recv_sem=row_recv.at[shift],
            device_id={"tp": target},
        )

    def share(home):
        return pltpu.make_async_remote_copy(
            src_ref=prod.at[home, 1 - core],
            dst_ref=prod_pair.at[home],
            send_sem=pair_send.at[home],
            recv_sem=pair_recv.at[home],
            device_id={"tp": partner},
        )

    def add_on(side, home):
        slot = home if side == 1 else jnp.where(home == z - 1, length, home)
        return pltpu.make_async_remote_copy(
            src_ref=prod.at[home, core],
            dst_ref=prod_inc.at[slot],
            send_sem=sum_send.at[home],
            recv_sem=sum_recv.at[slot],
            device_id={"tp": sides[side][0]},
        )

    def added(slot):
        return pltpu.make_async_remote_copy(
            src_ref=prod_inc.at[slot],
            dst_ref=prod_inc.at[slot],
            send_sem=sum_send.at[0],
            recv_sem=sum_recv.at[slot],
            device_id={"tp": partner},
        )

    def pass_on(side, home):
        share(home).wait_recv()

        @pl.when(sides[1 - side][1])
        def _():
            added(home).wait_recv()

        prod[home, core] = (
            prod[home, core].astype(jnp.float32)
            + prod_pair[home].astype(jnp.float32)
            + prod_inc[home].astype(jnp.float32)
        ).astype(prod.dtype)
        add_on(side, home).start()

    mirrored = [partner_slot(group, -j % groups, groups) for j in range(groups)]

    def gate_swap(j):
        return pltpu.make_async_remote_copy(
            src_ref=gate_rows.at[mirrored[j]],
            dst_ref=gates_ref.at[tp, j],
            send_sem=gate_send.at[j],
            recv_sem=gate_recv.at[j],
            device_id={"sp": mirrored[j]},
        )

    def gate_block(shift):
        place = gates_ref.at[tp]
        return pltpu.make_async_remote_copy(
            src_ref=place,
            dst_ref=place,
            send_sem=gates_send.at[shift],
            recv_sem=gates_recv.at[shift],
            device_id={"tp": lax.rem(tp + shift, parts)},
        )

    inward = (group > 0, group < groups - 1)
    loads[0].wait()
    for half in range(halves):
        for side in range(2):
            @pl.when(sides[side][1])
            def _(side=side, half=half):
                line(side, z, half).start()
    gates_ref[tp, 0] = gate_rows[group]
    for j in range(1, groups):
        gate_swap(j).start()
    loads[1].wait()
    loads[2].wait()
    for side in range(2):
        @pl.when(inward[side])
        def _(side=side):
            halo(side).start()
    across(z).start()
    loads[3].wait()
    loads[4].wait()

    def attend(n, carry):
        b = jnp.where(n < blocks - 2, n + 1, jnp.where(n == blocks - 2, 0, blocks - 1))

        @pl.when(n == blocks - 2)
        def _():
            for side in range(2):
                @pl.when(inward[1 - side])
                def _(side=side):
                    halo(side).wait_recv()

        start = pl.multiple_of(b * BLOCK, BLOCK)
        wide = query[pl.ds(start, BLOCK), :]
        tall = jnp.concatenate(
            [wide[:, h * HEAD_DIM : (h + 1) * HEAD_DIM] for h in range(heads_dev)], axis=0
        )
        reach = BLOCK + 2 * WINDOW
        keys = span[0, pl.ds(start, reach), :]
        values = span[1, pl.ds(start, reach), :]
        scores = lax.dot_general(
            tall, keys, (((1,), (1,)), ((), ())), preferred_element_type=jnp.float32
        ) * HEAD_DIM ** (-0.5)
        shape = (heads_dev * BLOCK, reach)
        row = lax.broadcasted_iota(jnp.int32, shape, 0) % BLOCK
        column = lax.broadcasted_iota(jnp.int32, shape, 1)
        place = column + (group * seq_rows + b * BLOCK - WINDOW)
        inside = (
            (column >= row) & (column <= row + 2 * WINDOW)
            & (place >= 0) & (place < seq_rows * groups)
        )
        scores = jnp.where(inside, scores, NEG_BIG)
        which = lax.broadcasted_iota(jnp.int32, (heads_dev * BLOCK, 1), 0) // BLOCK
        sink = jnp.zeros((heads_dev * BLOCK, 1), jnp.float32)
        for h in range(heads_dev):
            sink = jnp.where(which == h, sink_ref[h], sink)
        top = jnp.maximum(jnp.max(scores, axis=1, keepdims=True), sink)
        terms = jnp.exp(scores - top)
        mass = jnp.sum(terms, axis=1, keepdims=True) + jnp.exp(sink - top)
        weight = (terms / mass).astype(jnp.bfloat16)
        result = jnp.dot(weight, values, preferred_element_type=jnp.float32).astype(jnp.bfloat16)
        attended[b] = jnp.concatenate(
            [result[h * BLOCK : (h + 1) * BLOCK] for h in range(heads_dev)], axis=1
        )
        return carry


    def homes(i):
        return ((z + 1 + i, z + 1 + i <= last), (z - 1 - i, z - 1 - i >= 0))

    def spread_half(i, half):
        for side in range(2):
            home, live = homes(i)[side]

            @pl.when(live)
            def _(side=side, home=home):
                line(side, home, half).wait_recv()

                @pl.when(sides[side][1])
                def _():
                    line(side, home, half).start()

                across_part(home, group, half).start()
                if not relayed:
                    for j in range(1, groups):
                        plane(home, j, half, peers[j], group).start()
                elif half == 0:
                    plane(home, 1, 0, peers[1], group).start()
                else:
                    plane(home, 2, 1, peers[2], group).start()
                    plane(home, 1, 1, peers[1], group).start()
                    plane(home, 2, 0, peers[2], group).start()

    def relay_half(i, half):
        for side in range(2):
            home, live = homes(i)[side]

            @pl.when(live)
            def _(home=home):
                plane(home, 1 + half, half, peers[1], group).wait_recv()
                relay(home, half).start()
                across_part(home, peers[1 + half], half).start()

    def multiply(home, carry):
        lhs = jnp.concatenate([attended[home * CORES + c] for c in range(CORES)], axis=0)
        part = jnp.dot(
            lhs, own_weight[...].reshape(-1, summed), preferred_element_type=jnp.float32
        )
        prod[home] = part.astype(prod.dtype).reshape(CORES, -1, summed)
        share(home).start()
        return carry

    depths = (last - z, z)

    def add_step(r):
        for side in range(2):
            event = r - (depths[side] - 1)
            home = last - event if side == 1 else event

            @pl.when((depths[side] > 0) & (event >= 0) & (event < depths[1 - side]))
            def _(side=side, home=home):
                pass_on(side, home)

    def spread(i):
        for half in range(halves):
            spread_half(i, half)
        if relayed:
            for half in range(halves):
                relay_half(i, half)

    def first_sums():
        for side in range(2):
            @pl.when(depths[side] == 0)
            def _(side=side):
                for event in range(last):
                    pass_on(side, last - event if side == 1 else event)

    def send_rows(reach):
        if 1 in reach:
            row_block(lax.rem(partner - tp + parts, parts)).start()
        for distance in reach:
            for target in (z + distance, z - distance):
                @pl.when((target >= 0) & (target <= last))
                def _(target=target):
                    for c in range(CORES):
                        row_block(lax.rem(target * CORES + c - tp + parts, parts)).start()

    lax.fori_loop(0, blocks, attend, 0)
    received[tp] = attended[tp]
    send_rows(range(2, length))
    lax.fori_loop(0, length, multiply, 0)
    spread(0)
    first_sums()
    send_rows(range(1, 2))
    for i in range(1, last):
        add_step(i - 1)
        spread(i)

    def project(home, first):
        pieces = [received[home * CORES + c] for c in range(CORES)]
        lhs = jnp.concatenate(pieces, axis=1)
        rhs = jnp.concatenate(
            [full[home * CORES + c].reshape(-1, gathered) for c in range(CORES)], axis=0
        )
        part = jnp.dot(lhs, rhs, preferred_element_type=jnp.float32)
        if first:
            total[:, summed:] = part
        else:
            total[:, summed:] += part

    def rows_from(home):
        for c in range(CORES):
            source = home * CORES + c

            @pl.when(source != tp)
            def _(source=source):
                shift = lax.rem(tp - source + parts, parts)
                pltpu.make_async_remote_copy(
                    src_ref=attended.at[source],
                    dst_ref=received.at[source],
                    send_sem=row_send.at[0],
                    recv_sem=row_recv.at[lax.rem(parts + tp - source, parts)],
                    device_id={"tp": partner},
                ).wait_recv()

    for j in range(1, groups):
        gate_swap(j).wait_recv()
    for shift in range(1, parts):
        gate_block(shift).start()
    across(z).wait_recv()
    rows_from(z)
    project(z, True)

    def gather_step(i, carry):
        for side in range(2):
            home, live = homes(i)[side]

            @pl.when(live)
            def _(home=home):
                for half in range(halves):
                    for j in range(1, groups):
                        if not (relayed and j == 1 + half and j < 3):
                            plane(home, j, half, peers[1], group).wait_recv()
                            across_part(home, peers[j], half).start()

        for side in range(2):
            home, live = homes(i)[side]

            @pl.when(live)
            def _(home=home):
                across(home).wait_recv()
                rows_from(home)
                project(home, False)

        return carry

    lax.fori_loop(0, last, gather_step, 0)

    share(z).wait_recv()

    @pl.when(z > 0)
    def _():
        added(z).wait_recv()

    @pl.when(z < last)
    def _():
        added(length).wait_recv()

    total[:, :summed] = (
        prod[z, core].astype(jnp.float32)
        + prod_pair[z].astype(jnp.float32)
        + prod_inc[z].astype(jnp.float32)
        + prod_inc[length].astype(jnp.float32)
    )
    for copy in loads[5:]:
        copy.wait()
    projected = total[...]
    scale = lax.rsqrt(jnp.mean(projected * projected, axis=1, keepdims=True) + EPS)
    mixed = (
        residual[...].astype(jnp.float32) + gains[0] * (projected * scale)
    ).astype(jnp.bfloat16)
    mixed_ref[...] = mixed
    mixed_float = mixed.astype(jnp.float32)
    norm = lax.rsqrt(jnp.mean(mixed_float * mixed_float, axis=1, keepdims=True) + EPS)
    normed = (mixed_float * norm * gains[1]).astype(jnp.bfloat16)
    rows_ref[...] = (
        jnp.dot(placing, normed, preferred_element_type=jnp.float32)
        .astype(rows_ref.dtype)
        .reshape(rows_ref.shape)
    )

    for shift in range(1, parts):
        gate_block(shift).wait_recv()

    def settle():
        for side in range(2):
            @pl.when(inward[side])
            def _(side=side):
                halo(side).wait_send()
        for shift in range(1, parts):
            row_block(shift).wait_send()
            gate_block(shift).wait_send()
        for j in range(1, groups):
            gate_swap(j).wait_send()

        def drain(home, carry):
            for half in range(halves):
                @pl.when((home >= z) & sides[0][1])
                def _(half=half):
                    line(0, home, half).wait_send()

                @pl.when((home <= z) & sides[1][1])
                def _(half=half):
                    line(1, home, half).wait_send()

                @pl.when(home != z)
                def _(half=half):
                    for j in range(1, groups):
                        plane(home, j, half, peers[1], group).wait_send()

            @pl.when(home != z)
            def _():
                add_on(1, home).wait_send()

            across(home).wait_send()
            share(home).wait_send()
            return carry

        lax.fori_loop(0, length, drain, 0)

    return started, settle


def front_kernel(*refs):
    _, settle = front_body(lambda: None, *refs)
    settle()


def front_scratch(parts, groups, queries, residual):
    length = parts // CORES
    seq_rows, columns = queries.shape
    tok_rows, width = residual.shape
    halves = 2 if groups == 4 else 1
    piece = columns // (groups * halves)
    summed = SUMMED_EIGHTHS * width // 8 // LANES * LANES
    sem = pltpu.SemaphoreType.DMA
    kind = queries.dtype
    return [
        pltpu.VMEM((seq_rows, columns), kind),
        pltpu.VMEM((2, seq_rows + 2 * WINDOW, HEAD_DIM), kind),
        pltpu.VMEM((parts, tok_rows, columns), kind),
        pltpu.VMEM((parts, tok_rows, columns), kind),
        pltpu.VMEM((parts, groups, halves, piece, width - summed), kind),
        pltpu.VMEM((tok_rows, width), jnp.float32),
        pltpu.VMEM((tok_rows, width), kind),
        pltpu.VMEM((2, 1, width), jnp.float32),
        pltpu.VMEM((groups, halves, piece, summed), kind),
        pltpu.VMEM((length, CORES, tok_rows, summed), kind),
        pltpu.VMEM((length, tok_rows, summed), kind),
        pltpu.VMEM((length + 1, tok_rows, summed), kind),
        pltpu.VMEM((groups, GATE_ROWS, LANES), kind),
        sem((8,)),
        sem((2,)),
        sem((2,)),
        sem((2, length, halves)),
        sem((length, halves)),
        sem((length, groups, halves)),
        sem((length, groups, halves)),
        sem((length,)),
        sem((length,)),
        sem((parts,)),
        sem((parts,)),
        sem((length,)),
        sem((length,)),
        sem((length,)),
        sem((length + 1,)),
        sem((groups,)),
        sem((groups,)),
        sem((parts,)),
        sem((parts,)),
    ]


HBM_SPEC = pl.BlockSpec(memory_space=pltpu.HBM)
FRONT_SPECS = (
    *[HBM_SPEC] * 3, pl.BlockSpec(memory_space=pltpu.SMEM), *[HBM_SPEC] * 4, *[VMEM_SPEC] * 3
)


def front_made(groups, capacity, residual):
    tok_rows, width = residual.shape
    return (
        ((tok_rows, width), residual.dtype),
        ((groups, capacity, width), residual.dtype),
        ((groups, capacity, tok_rows), residual.dtype),
        ((lax.axis_size("tp"), groups, GATE_ROWS, LANES), residual.dtype),
    )


def front(arguments, capacity):
    parts, groups = lax.axis_size("tp"), lax.axis_size("sp")
    made = front_made(groups, capacity, arguments[5])
    return pl.pallas_call(
        front_kernel,
        out_shape=[jax.ShapeDtypeStruct(*each) for each in made],
        in_specs=FRONT_SPECS,
        out_specs=[VMEM_SPEC] * 4,
        scratch_shapes=front_scratch(parts, groups, arguments[0], arguments[5]),
        compiler_params=pltpu.CompilerParams(
            collective_id=0, has_side_effects=True, vmem_limit_bytes=VMEM_BYTES
        ),
        name="front",
    )(*arguments)


def layer_kernel(inputs, front_count, moe_count, *refs):
    front_in, refs = refs[:inputs], refs[inputs:]
    weights_in, out_ref, refs = refs[:3], refs[3], refs[4:]
    front_refs, refs = refs[:front_count], refs[front_count:]
    *buffers, weight_sem = refs[:moe_count]
    mixed_ref, rows_ref, placing_ref, gates_ref, returned = refs[moe_count:]

    def setup():
        return moe_setup(*weights_in, buffers[3], *buffers[4:7], weight_sem)

    weights, settle = front_body(
        setup, *front_in, mixed_ref, rows_ref, placing_ref, gates_ref, *front_refs
    )
    total = front_refs[5]

    def landed(j, group):
        part = lax.dot_general(
            placing_ref[group], returned[group], (((0,), (0,)), ((), ())),
            preferred_element_type=jnp.float32,
        )
        total[...] = (mixed_ref[...].astype(jnp.float32) if j == 0 else total[...]) + part

    moe_body(weights, landed, rows_ref, gates_ref, returned, *buffers)
    out_ref[...] = total[...].astype(out_ref.dtype)
    settle()


def layer(arguments, capacity, gate_weight, up_weight, down_weight, front_bufs, moe_bufs):
    residual = arguments[5]
    groups = lax.axis_size("sp")
    kept = front_made(groups, capacity, residual)
    returned = ((groups, capacity, residual.shape[1]), residual.dtype)
    return pl.pallas_call(
        functools.partial(layer_kernel, len(arguments), len(front_bufs), len(moe_bufs)),
        out_shape=jax.ShapeDtypeStruct(residual.shape, residual.dtype),
        in_specs=[*FRONT_SPECS, *[HBM_SPEC] * 3],
        out_specs=VMEM_SPEC,
        scratch_shapes=[
            *front_bufs, *moe_bufs, *[pltpu.VMEM(*each) for each in (*kept, returned)]
        ],
        compiler_params=pltpu.CompilerParams(
            collective_id=2, has_side_effects=True, vmem_limit_bytes=VMEM_BYTES
        ),
        name="layer",
    )(*arguments, gate_weight, up_weight, down_weight.reshape(-1, residual.shape[1]))


def per_device(
    queries,
    key_heads,
    value_heads,
    sink_logit,
    out_weight,
    residual,
    mixer_gain,
    expert_gain,
    route_group,
    route_member,
    route_weight,
    gate_weight,
    up_weight,
    down_weight,
):
    tok_rows, width = residual.shape
    parts, groups = lax.axis_size("tp"), lax.axis_size("sp")
    capacity = max(2, (5 * tok_rows + 4 * groups - 1) // (4 * groups))
    capacity = (capacity + 7) // 8 * 8
    halves = 2 if groups == 4 else 1
    arguments = (
        queries, key_heads, value_heads, sink_logit,
        out_weight.reshape(groups, halves, -1, width), residual,
        mixer_gain.reshape(1, width), expert_gain.reshape(1, width),
        route_group.reshape(1, tok_rows), route_member.T, route_weight.T,
    )
    front_bufs = front_scratch(parts, groups, queries, residual)
    moe_bufs = moe_scratch(parts // CORES, groups, capacity, gate_weight)
    held = sum(
        math.prod(each.shape) * jnp.dtype(each.dtype).itemsize
        for each in (*front_bufs, *moe_bufs)
        if getattr(each, "memory_space", None) == pltpu.VMEM
    )
    if held < VMEM_BYTES * 3 // 4:
        return layer(
            arguments, capacity, gate_weight, up_weight, down_weight, front_bufs, moe_bufs
        )
    mixed_rows, send_rows, placing, gates = front(arguments, capacity)
    returned = moe(send_rows, gates, gate_weight, up_weight, down_weight)
    expert_out = lax.dot_general(
        placing.reshape(-1, tok_rows),
        returned.reshape(-1, width),
        (((0,), (0,)), ((), ())),
        preferred_element_type=jnp.float32,
    )
    return (mixed_rows.astype(jnp.float32) + expert_out).astype(jnp.bfloat16)


def solution(mesh):
    placed = (
        P("sp", "tp"),
        P("sp", None),
        P("sp", None),
        P("tp"),
        P("tp", None),
        P(("sp", "tp"), None),
        P(),
        P(),
        P(("sp", "tp")),
        P(("sp", "tp"), None),
        P(("sp", "tp"), None),
        P("sp", None, "tp"),
        P("sp", None, "tp"),
        P("sp", "tp", None),
    )
    return jax.shard_map(
        per_device, mesh=mesh, in_specs=placed, out_specs=P(("sp", "tp"), None), check_vma=False
    )
```

```python
import functools
import math

import jax
import jax.numpy as jnp
from jax import lax
from jax.experimental import pallas as pl
from jax.experimental.pallas import tpu as pltpu
from jax.sharding import PartitionSpec as P

HEADS = 16
KV_HEADS = 4
HEAD_DIM = 128
WINDOW = 128
BLOCK = 128


EPS = 1e-06
NEG_BIG = -1e30


CORES = 2
LANES = 128
VMEM_BYTES = 67043328
SUMMED_EIGHTHS = 3
GATE_ROWS = 8
VMEM_SPEC = pl.BlockSpec(memory_space=pltpu.VMEM)


def greet(neighbours, partner, peers):
    barrier = pltpu.get_barrier_semaphore()
    for target in (*neighbours, partner):
        pl.semaphore_signal(barrier, inc=1, device_id={"tp": target})
    for peer in peers:
        pl.semaphore_signal(barrier, inc=1, device_id={"sp": peer})
    pl.semaphore_wait(barrier, 3 + len(peers))


def line_sequence(i, position, length, side):
    reach = length - 1 - position if side == 0 else position
    early = i < reach
    offset = jnp.where(early, i + 1, 2 * reach - i)
    home = position + offset if side == 0 else position - offset
    return home, jnp.where(early, 0, 1)


def partner_slot(mine, j, groups):
    total, bit = 0, 1
    while bit < groups:
        total = total + lax.rem(mine // bit + j // bit, 2) * bit
        bit *= 2
    return total


def moe_setup(gate_hbm, up_hbm, down_hbm, inc, gate_ref, up_ref, down_ref, weight_sem):
    length = lax.axis_size("tp") // CORES
    z, last = lax.axis_index("tp") // CORES, length - 1
    weights = [
        pltpu.make_async_copy(source, place, weight_sem.at[n])
        for n, (source, place) in enumerate(
            ((gate_hbm, gate_ref), (up_hbm, up_ref), (down_hbm, down_ref))
        )
    ]
    for copy in weights:
        copy.start()

    @pl.when((z == 0) | (z == last))
    def _():
        for slot in range(length):
            @pl.when(slot != last * (z // last))
            def _():
                inc[slot] = jnp.zeros_like(inc[slot])

        @pl.when(z == 0)
        def _():
            inc[0] = jnp.zeros_like(inc[0])

        @pl.when(z == last)
        def _():
            inc[length] = jnp.zeros_like(inc[length])
    return weights


def moe_body(
    weights, landed, send_ref, gates_ref, out_ref,
    rows, res, pair, inc, gate_ref, up_ref, down_ref,
    own_sem, swap_send, swap_recv, line_send, line_recv, core_send, core_recv,
    pair_send, pair_recv, sum_send, sum_recv, home_send, home_recv,
):
    length = lax.axis_size("tp") // CORES
    tp = lax.axis_index("tp")
    z, core = tp // CORES, lax.rem(tp, CORES)
    partner = z * CORES + 1 - core
    groups = lax.axis_size("sp")
    group = lax.axis_index("sp")
    near = groups // 2
    width = out_ref.shape[2]
    last = length - 1
    sides = (
        (lax.rem(z + length - 1, length) * CORES + core, z > 0),
        (lax.rem(z + 1, length) * CORES + core, z < last),
    )
    peers = [partner_slot(group, -j % groups, groups) for j in range(groups)]

    def swap(j):
        return pltpu.make_async_remote_copy(
            src_ref=send_ref.at[peers[j]],
            dst_ref=rows.at[z * 2 + j // near, core, j % near],
            send_sem=swap_send.at[j],
            recv_sem=swap_recv.at[j],
            device_id={"sp": peers[j]},
        )

    def line(side, index, j):
        place = rows.at[index, core, j]
        return pltpu.make_async_remote_copy(
            src_ref=place,
            dst_ref=place,
            send_sem=line_send.at[side, index, j],
            recv_sem=line_recv.at[index, j],
            device_id={"tp": sides[side][0]},
        )

    def across(index, j):
        place = rows.at[index, core, j]
        return pltpu.make_async_remote_copy(
            src_ref=place,
            dst_ref=place,
            send_sem=core_send.at[index, j],
            recv_sem=core_recv.at[index, j],
            device_id={"tp": partner},
        )

    def share(index):
        return pltpu.make_async_remote_copy(
            src_ref=res.at[index, 1 - core],
            dst_ref=pair.at[index],
            send_sem=pair_send.at[index],
            recv_sem=pair_recv.at[index],
            device_id={"tp": partner},
        )

    def slot_of(side, target):
        if side == 1:
            return target
        return jnp.where(target == z - 1, length, target)

    def add_on(side, target, half, j):
        slot = slot_of(side, target)
        return pltpu.make_async_remote_copy(
            src_ref=res.at[target * 2 + half, core, j],
            dst_ref=inc.at[slot, half, j],
            send_sem=sum_send.at[target * 2 + half, j],
            recv_sem=sum_recv.at[slot, half, j],
            device_id={"tp": sides[side][0]},
        )

    def added(slot, half, j):
        return pltpu.make_async_remote_copy(
            src_ref=inc.at[slot, half, j],
            dst_ref=inc.at[slot, half, j],
            send_sem=sum_send.at[0, j],
            recv_sem=sum_recv.at[slot, half, j],
            device_id={"tp": partner},
        )

    def back(half, j):
        return pltpu.make_async_remote_copy(
            src_ref=res.at[z * 2 + half, core, j],
            dst_ref=out_ref.at[group],
            send_sem=home_send.at[half * near + j],
            recv_sem=home_recv.at[half * near + j],
            device_id={"sp": peers_at(half, j)},
        )

    def peers_at(half, j):
        return peers[half * near + j]

    def forward(side, index, j):
        @pl.when(sides[side][1])
        def _():
            line(side, index, j).start()

    own = pltpu.make_async_copy(send_ref.at[group], rows.at[z * 2, core, 0], own_sem)
    own.start()
    for j in range(1, groups):
        swap(j).start()
    for j in range(near):
        if j == 0:
            own.wait()
        else:
            swap(j).wait_recv()
        for side in range(2):
            forward(side, z * 2, j)
        across(z * 2, j).start()
    for j in range(near):
        swap(near + j).wait_recv()
        across(z * 2 + 1, j).start()
    for copy in weights:
        copy.wait()

    def expert_rows(index):
        for j in range(near):
            across(index, j).wait_recv()
        block = rows[index].reshape(2 * near * rows.shape[3], rows.shape[4])
        home, half = index // 2, lax.rem(index, 2)
        gates = jnp.concatenate(
            [
                gates_ref[home * CORES + c, half * near + j].astype(jnp.float32).T[: rows.shape[3]]
                for c in range(CORES) for j in range(near)
            ],
            axis=0,
        )
        hidden = []
        for member in range(gate_ref.shape[0]):
            gate_pre = jnp.dot(block, gate_ref[member], preferred_element_type=jnp.float32)
            up_pre = jnp.dot(block, up_ref[member], preferred_element_type=jnp.float32)
            value = gate_pre / (1.0 + jnp.exp(-gate_pre)) * up_pre * gates[:, member : member + 1]
            hidden.append(value.astype(jnp.bfloat16))
        total = jnp.dot(
            jnp.concatenate(hidden, axis=1), down_ref[...], preferred_element_type=jnp.float32
        )
        res[index] = total.astype(res.dtype).reshape(res.shape[1:])
        share(index).start()

    def pass_on(side, i):
        target, half = line_sequence(i, z, length, 1 - side)
        index = target * 2 + half
        share(index).wait_recv()
        for j in range(near):
            @pl.when(sides[1 - side][1])
            def _():
                added(target, half, j).wait_recv()
            value = (
                res[index, core, j].astype(jnp.float32)
                + pair[index, j].astype(jnp.float32)
                + inc[target, half, j].astype(jnp.float32)
            )
            res[index, core, j] = value.astype(res.dtype)
            add_on(side, target, half, j).start()

    def finish(half):
        index = z * 2 + half
        share(index).wait_recv()
        for j in range(near):
            @pl.when(z > 0)
            def _():
                added(z, half, j).wait_recv()

            @pl.when(z < last)
            def _():
                added(length, half, j).wait_recv()
            value = (
                res[index, core, j].astype(jnp.float32)
                + pair[index, j].astype(jnp.float32)
                + inc[z, half, j].astype(jnp.float32)
                + inc[length, half, j].astype(jnp.float32)
            ).astype(res.dtype)
            if half == 0 and j == 0:
                out_ref[group] = value
            else:
                res[index, core, j] = value
                back(half, j).start()

    reaches = (last - z, z)
    lags = tuple(jnp.where(depth == 0, 0, 2 * depth + 1) for depth in (last - z, z))

    spare = max(0, 2 * last - 2)

    def step(k, carry):
        for j in range(near):
            for side in range(2):
                home, half = line_sequence(k, z, length, side)

                @pl.when(k < 2 * reaches[side])
                def _(side=side, index=home * 2 + half, j=j):
                    line(side, index, j).wait_recv()
                    forward(side, index, j)
                    across(index, j).start()
        for side in range(2):
            @pl.when(k == jnp.maximum(2 * reaches[side] - 1, 0))
            def _(side=side):
                for j in range(near):
                    forward(side, z * 2 + 1, j)

        for side in range(2):
            i = k - lags[side]

            @pl.when((lags[side] > 0) & (i >= 0) & (i < 2 * reaches[1 - side]))
            def _(side=side, i=i):
                pass_on(side, i)

        def job(d, inner):
            home0, half0 = line_sequence(k, z, length, 0)
            home1, half1 = line_sequence(k, z, length, 1)
            index = jnp.where(
                d == 0, home0 * 2 + half0, jnp.where(d == 1, home1 * 2 + half1, z * 2 + k - spare)
            )
            live = jnp.where(
                d == 0, k < 2 * reaches[0],
                jnp.where(d == 1, k < 2 * reaches[1], (k == spare) | (k == spare + 1)),
            )

            @pl.when(live)
            def _():
                expert_rows(index)

            return inner

        lax.fori_loop(0, 3, job, 0)
        for side in range(2):
            @pl.when((lags[side] == 0) & (k < 2 * reaches[1 - side]))
            def _(side=side):
                pass_on(side, k)

        @pl.when(k == 2 * jnp.maximum(z, last - z))
        def _():
            finish(0)

        return carry

    lax.fori_loop(0, 2 * length - 1, step, 0)
    finish(1)

    for j in range(groups):
        if j > 0:
            back(j // near, j % near).wait_recv()
        landed(j, peers[j])
    for j in range(1, groups):
        swap(j).wait_send()
        back(j // near, j % near).wait_send()

    def drain(index, carry):
        home = index // 2
        for j in range(near):
            @pl.when((home >= z) & sides[0][1])
            def _(j=j):
                line(0, index, j).wait_send()

            @pl.when((home <= z) & sides[1][1])
            def _(j=j):
                line(1, index, j).wait_send()

            across(index, j).wait_send()

            @pl.when(home != z)
            def _(j=j):
                add_on(1, home, lax.rem(index, 2), j).wait_send()
        share(index).wait_send()
        return carry

    lax.fori_loop(0, 2 * length, drain, 0)


def moe_kernel(send_ref, gates_ref, gate_hbm, up_hbm, down_hbm, out_ref, *scratch):
    *buffers, weight_sem = scratch
    inc, places = buffers[3], buffers[4:7]
    weights = moe_setup(gate_hbm, up_hbm, down_hbm, inc, *places, weight_sem)
    z, core = lax.axis_index("tp") // CORES, lax.rem(lax.axis_index("tp"), CORES)
    length, groups = lax.axis_size("tp") // CORES, lax.axis_size("sp")
    around = [lax.rem(z + shift, length) * CORES + core for shift in (length - 1, 1)]
    others = [lax.rem(lax.axis_index("sp") + shift, groups) for shift in range(1, groups)]
    greet(around, z * CORES + 1 - core, others)
    moe_body(weights, lambda j, group: None, send_ref, gates_ref, out_ref, *buffers)


def moe_scratch(length, groups, capacity, gate_weight):
    members, width, hidden = gate_weight.shape
    near = groups // 2
    kind = gate_weight.dtype
    sem = pltpu.SemaphoreType.DMA
    return [
        pltpu.VMEM((2 * length, 2, near, capacity, width), kind),
        pltpu.VMEM((2 * length, 2, near, capacity, width), kind),
        pltpu.VMEM((2 * length, near, capacity, width), kind),
        pltpu.VMEM((length + 1, 2, near, capacity, width), kind),
        pltpu.VMEM((members, width, hidden), kind),
        pltpu.VMEM((members, width, hidden), kind),
        pltpu.VMEM((members * hidden, width), kind),
        sem,
        sem((groups,)),
        sem((groups,)),
        sem((2, 2 * length, near)),
        sem((2 * length, near)),
        sem((2 * length, near)),
        sem((2 * length, near)),
        sem((2 * length,)),
        sem((2 * length,)),
        sem((2 * length, near)),
        sem((length + 1, 2, near)),
        sem((groups,)),
        sem((groups,)),
        sem((3,)),
    ]


def moe(send_rows, gates, gate_weight, up_weight, down_weight):
    groups, capacity, _ = send_rows.shape
    members, width, hidden = gate_weight.shape
    length = lax.axis_size("tp") // CORES
    hbm = pl.BlockSpec(memory_space=pltpu.HBM)
    return pl.pallas_call(
        moe_kernel,
        out_shape=jax.ShapeDtypeStruct((groups, capacity, width), send_rows.dtype),
        in_specs=[VMEM_SPEC, VMEM_SPEC, hbm, hbm, hbm],
        out_specs=VMEM_SPEC,
        scratch_shapes=moe_scratch(length, groups, capacity, gate_weight),
        compiler_params=pltpu.CompilerParams(
            collective_id=1, has_side_effects=True, vmem_limit_bytes=VMEM_BYTES
        ),
        name="moe",
    )(send_rows, gates, gate_weight, up_weight, down_weight.reshape(members * hidden, width))


def front_body(
    setup, query_hbm, key_hbm, value_hbm, sink_ref, weight_hbm, residual_hbm, mixer_hbm, expert_hbm,
    group_ref, member_ref, gate_ref,
    mixed_ref, rows_ref, placing_ref, gates_ref,
    query, span, attended, received, full, total, residual, gains,
    own_weight, prod, prod_pair, prod_inc, gate_rows,
    load_sem, halo_send, halo_recv, line_send, line_recv, plane_send, plane_recv,
    core_send, core_recv, row_send, row_recv, pair_send, pair_recv, sum_send, sum_recv,
    gate_send, gate_recv, gates_send, gates_recv,
):
    parts = lax.axis_size("tp")
    length = parts // CORES
    tp = lax.axis_index("tp")
    z, core = tp // CORES, lax.rem(tp, CORES)
    partner = z * CORES + 1 - core
    groups = lax.axis_size("sp")
    group = lax.axis_index("sp")
    last = length - 1
    halves = full.shape[2]
    relayed = groups == 4
    seq_rows = query.shape[0]
    heads_dev = query.shape[1] // HEAD_DIM
    blocks = seq_rows // BLOCK
    peers = [partner_slot(group, j, groups) for j in range(groups)]
    sides = (
        (lax.rem(z + length - 1, length) * CORES + core, z > 0),
        (lax.rem(z + 1, length) * CORES + core, z < last),
    )
    head_start = pl.multiple_of(tp * heads_dev // (HEADS // KV_HEADS) * HEAD_DIM, HEAD_DIM)
    inner = pl.ds(WINDOW, seq_rows)
    summed, gathered = own_weight.shape[3], full.shape[4]

    loads = [
        pltpu.make_async_copy(source, place, load_sem.at[n])
        for n, (source, place) in enumerate(
            (
                (weight_hbm.at[:, :, :, pl.ds(summed, gathered)], full.at[tp]),
                (key_hbm.at[:, pl.ds(head_start, HEAD_DIM)], span.at[0, inner]),
                (value_hbm.at[:, pl.ds(head_start, HEAD_DIM)], span.at[1, inner]),
                (query_hbm, query),
                (weight_hbm.at[:, :, :, pl.ds(0, summed)], own_weight),
                (residual_hbm, residual),
                (mixer_hbm, gains.at[0]),
                (expert_hbm, gains.at[1]),
            )
        )
    ]
    for copy in loads:
        copy.start()

    @pl.when(group == 0)
    def _():
        span[:, :WINDOW] = jnp.zeros((2, WINDOW, HEAD_DIM), span.dtype)

    @pl.when(z == 0)
    def _():
        for slot in range(length):
            prod_inc[slot] = jnp.zeros_like(prod_inc[slot])

    @pl.when(z == last)
    def _():
        for slot in [*range(last), length]:
            prod_inc[slot] = jnp.zeros_like(prod_inc[slot])

    @pl.when(group == groups - 1)
    def _():
        span[:, WINDOW + seq_rows :] = jnp.zeros((2, WINDOW, HEAD_DIM), span.dtype)

    started = setup()
    barrier = pltpu.get_barrier_semaphore()
    for shift in range(1, parts):
        pl.semaphore_signal(barrier, inc=1, device_id={"tp": lax.rem(tp + shift, parts)})
    for peer in peers[1:]:
        pl.semaphore_signal(barrier, inc=1, device_id={"sp": peer})
    capacity = rows_ref.shape[1]
    slots = groups * capacity
    tok_rows = residual.shape[0]
    width = residual.shape[1]
    names = lax.broadcasted_iota(jnp.int32, (groups * (8 // min(groups, 8)), tok_rows), 0)
    chosen = (names == group_ref[...]).astype(jnp.float32)
    earlier = (
        lax.broadcasted_iota(jnp.int32, (tok_rows, tok_rows), 0)
        < lax.broadcasted_iota(jnp.int32, (tok_rows, tok_rows), 1)
    ).astype(jnp.bfloat16)
    rank = jnp.dot(chosen.astype(jnp.bfloat16), earlier, preferred_element_type=jnp.float32)
    slot_row = jnp.sum(
        chosen * (rank + (names * capacity).astype(jnp.float32)), axis=0, keepdims=True
    )
    placing = (
        lax.broadcasted_iota(jnp.int32, (slots, tok_rows), 0).astype(jnp.float32) == slot_row
    ).astype(jnp.bfloat16)
    placing_ref[...] = placing.reshape(placing_ref.shape)
    members = lax.broadcasted_iota(jnp.int32, (GATE_ROWS, tok_rows), 0)
    tail = jnp.zeros((GATE_ROWS, tok_rows), jnp.float32)
    for k in range(member_ref.shape[0]):
        tail = tail + jnp.where(
            members == member_ref[k : k + 1, :], gate_ref[k : k + 1, :].astype(jnp.float32), 0.0
        )
    place = lax.broadcasted_iota(jnp.int32, (LANES, tok_rows), 0)
    for g in range(groups):
        chosen_slot = jnp.where(place < capacity, place + g * capacity, slots).astype(jnp.float32)
        gate_rows[g] = lax.dot_general(
            tail.astype(jnp.bfloat16), (chosen_slot == slot_row).astype(jnp.bfloat16),
            (((1,), (1,)), ((), ())), preferred_element_type=jnp.float32,
        ).astype(gate_rows.dtype)
    pl.semaphore_wait(barrier, parts + groups - 2)

    def line(side, home, half):
        place = full.at[home * CORES + core, group, half]
        return pltpu.make_async_remote_copy(
            src_ref=place,
            dst_ref=place,
            send_sem=line_send.at[side, home, half],
            recv_sem=line_recv.at[home, half],
            device_id={"tp": sides[side][0]},
        )

    def plane(home, j, half, target, source):
        place = full.at[home * CORES + core, source, half]
        return pltpu.make_async_remote_copy(
            src_ref=place,
            dst_ref=place,
            send_sem=plane_send.at[home, j, half],
            recv_sem=plane_recv.at[home, j, half],
            device_id={"sp": target},
        )

    def relay(home, half):
        target, source = (peers[2], peers[1]) if half == 0 else (peers[1], peers[2])
        return plane(home, 3, half, target, source)

    def across(home):
        place = full.at[home * CORES + core]
        return pltpu.make_async_remote_copy(
            src_ref=place,
            dst_ref=place,
            send_sem=core_send.at[home],
            recv_sem=core_recv.at[home],
            device_id={"tp": partner},
        )

    def across_part(home, part, half):
        place = full.at[home * CORES + core, part, half]
        return pltpu.make_async_remote_copy(
            src_ref=place,
            dst_ref=place,
            send_sem=core_send.at[home],
            recv_sem=core_recv.at[home],
            device_id={"tp": partner},
        )

    def halo(side):
        start = WINDOW if side == 0 else seq_rows
        landing = WINDOW + seq_rows if side == 0 else 0
        return pltpu.make_async_remote_copy(
            src_ref=span.at[:, pl.ds(start, WINDOW)],
            dst_ref=span.at[:, pl.ds(landing, WINDOW)],
            send_sem=halo_send.at[side],
            recv_sem=halo_recv.at[side],
            device_id={"sp": lax.rem(group + (groups - 1 if side == 0 else 1), groups)},
        )

    def row_block(shift):
        target = lax.rem(tp + shift, parts)
        return pltpu.make_async_remote_copy(
            src_ref=attended.at[target],
            dst_ref=received.at[tp],
            send_sem=row_send.at[shift],
            recv_sem=row_recv.at[shift],
            device_id={"tp": target},
        )

    def share(home):
        return pltpu.make_async_remote_copy(
            src_ref=prod.at[home, 1 - core],
            dst_ref=prod_pair.at[home],
            send_sem=pair_send.at[home],
            recv_sem=pair_recv.at[home],
            device_id={"tp": partner},
        )

    def add_on(side, home):
        slot = home if side == 1 else jnp.where(home == z - 1, length, home)
        return pltpu.make_async_remote_copy(
            src_ref=prod.at[home, core],
            dst_ref=prod_inc.at[slot],
            send_sem=sum_send.at[home],
            recv_sem=sum_recv.at[slot],
            device_id={"tp": sides[side][0]},
        )

    def added(slot):
        return pltpu.make_async_remote_copy(
            src_ref=prod_inc.at[slot],
            dst_ref=prod_inc.at[slot],
            send_sem=sum_send.at[0],
            recv_sem=sum_recv.at[slot],
            device_id={"tp": partner},
        )

    def pass_on(side, home):
        share(home).wait_recv()

        @pl.when(sides[1 - side][1])
        def _():
            added(home).wait_recv()

        prod[home, core] = (
            prod[home, core].astype(jnp.float32)
            + prod_pair[home].astype(jnp.float32)
            + prod_inc[home].astype(jnp.float32)
        ).astype(prod.dtype)
        add_on(side, home).start()

    mirrored = [partner_slot(group, -j % groups, groups) for j in range(groups)]

    def gate_swap(j):
        return pltpu.make_async_remote_copy(
            src_ref=gate_rows.at[mirrored[j]],
            dst_ref=gates_ref.at[tp, j],
            send_sem=gate_send.at[j],
            recv_sem=gate_recv.at[j],
            device_id={"sp": mirrored[j]},
        )

    def gate_block(shift):
        place = gates_ref.at[tp]
        return pltpu.make_async_remote_copy(
            src_ref=place,
            dst_ref=place,
            send_sem=gates_send.at[shift],
            recv_sem=gates_recv.at[shift],
            device_id={"tp": lax.rem(tp + shift, parts)},
        )

    inward = (group > 0, group < groups - 1)
    loads[0].wait()
    for half in range(halves):
        for side in range(2):
            @pl.when(sides[side][1])
            def _(side=side, half=half):
                line(side, z, half).start()
    gates_ref[tp, 0] = gate_rows[group]
    for j in range(1, groups):
        gate_swap(j).start()
    loads[1].wait()
    loads[2].wait()
    for side in range(2):
        @pl.when(inward[side])
        def _(side=side):
            halo(side).start()
    across(z).start()
    loads[3].wait()
    loads[4].wait()

    def attend(n, carry):
        b = jnp.where(n < blocks - 2, n + 1, jnp.where(n == blocks - 2, 0, blocks - 1))

        @pl.when(n == blocks - 2)
        def _():
            for side in range(2):
                @pl.when(inward[1 - side])
                def _(side=side):
                    halo(side).wait_recv()

        start = pl.multiple_of(b * BLOCK, BLOCK)
        wide = query[pl.ds(start, BLOCK), :]
        tall = jnp.concatenate(
            [wide[:, h * HEAD_DIM : (h + 1) * HEAD_DIM] for h in range(heads_dev)], axis=0
        )
        reach = BLOCK + 2 * WINDOW
        keys = span[0, pl.ds(start, reach), :]
        values = span[1, pl.ds(start, reach), :]
        scores = lax.dot_general(
            tall, keys, (((1,), (1,)), ((), ())), preferred_element_type=jnp.float32
        ) * HEAD_DIM ** (-0.5)
        shape = (heads_dev * BLOCK, reach)
        row = lax.broadcasted_iota(jnp.int32, shape, 0) % BLOCK
        column = lax.broadcasted_iota(jnp.int32, shape, 1)
        place = column + (group * seq_rows + b * BLOCK - WINDOW)
        inside = (
            (column >= row) & (column <= row + 2 * WINDOW)
            & (place >= 0) & (place < seq_rows * groups)
        )
        scores = jnp.where(inside, scores, NEG_BIG)
        which = lax.broadcasted_iota(jnp.int32, (heads_dev * BLOCK, 1), 0) // BLOCK
        sink = jnp.zeros((heads_dev * BLOCK, 1), jnp.float32)
        for h in range(heads_dev):
            sink = jnp.where(which == h, sink_ref[h], sink)
        top = jnp.maximum(jnp.max(scores, axis=1, keepdims=True), sink)
        terms = jnp.exp(scores - top)
        mass = jnp.sum(terms, axis=1, keepdims=True) + jnp.exp(sink - top)
        result = (
            jnp.dot(terms.astype(jnp.bfloat16), values, preferred_element_type=jnp.float32) / mass
        ).astype(jnp.bfloat16)
        attended[b] = jnp.concatenate(
            [result[h * BLOCK : (h + 1) * BLOCK] for h in range(heads_dev)], axis=1
        )
        return carry


    def homes(i):
        return ((z + 1 + i, z + 1 + i <= last), (z - 1 - i, z - 1 - i >= 0))

    def spread_half(i, half):
        for side in range(2):
            home, live = homes(i)[side]

            @pl.when(live)
            def _(side=side, home=home):
                line(side, home, half).wait_recv()

                @pl.when(sides[side][1])
                def _():
                    line(side, home, half).start()

                across_part(home, group, half).start()
                if not relayed:
                    for j in range(1, groups):
                        plane(home, j, half, peers[j], group).start()
                elif half == 0:
                    plane(home, 1, 0, peers[1], group).start()
                else:
                    plane(home, 2, 1, peers[2], group).start()
                    plane(home, 1, 1, peers[1], group).start()
                    plane(home, 2, 0, peers[2], group).start()

    def relay_half(i, half):
        for side in range(2):
            home, live = homes(i)[side]

            @pl.when(live)
            def _(home=home):
                plane(home, 1 + half, half, peers[1], group).wait_recv()
                relay(home, half).start()
                across_part(home, peers[1 + half], half).start()

    def multiply(home, carry):
        lhs = jnp.concatenate([attended[home * CORES + c] for c in range(CORES)], axis=0)
        part = jnp.dot(
            lhs, own_weight[...].reshape(-1, summed), preferred_element_type=jnp.float32
        )
        prod[home] = part.astype(prod.dtype).reshape(CORES, -1, summed)
        share(home).start()
        return carry

    depths = (last - z, z)

    def add_step(r):
        for side in range(2):
            event = r - (depths[side] - 1)
            home = last - event if side == 1 else event

            @pl.when((depths[side] > 0) & (event >= 0) & (event < depths[1 - side]))
            def _(side=side, home=home):
                pass_on(side, home)

    def spread(i):
        for half in range(halves):
            spread_half(i, half)
        if relayed:
            for half in range(halves):
                relay_half(i, half)

    def first_sums():
        for side in range(2):
            @pl.when(depths[side] == 0)
            def _(side=side):
                for event in range(last):
                    pass_on(side, last - event if side == 1 else event)

    def send_rows(reach):
        if 1 in reach:
            row_block(lax.rem(partner - tp + parts, parts)).start()
        for distance in reach:
            for target in (z + distance, z - distance):
                @pl.when((target >= 0) & (target <= last))
                def _(target=target):
                    for c in range(CORES):
                        row_block(lax.rem(target * CORES + c - tp + parts, parts)).start()

    lax.fori_loop(0, blocks, attend, 0)
    received[tp] = attended[tp]
    send_rows(range(2, length))
    lax.fori_loop(0, length, multiply, 0)
    spread(0)
    first_sums()
    send_rows(range(1, 2))
    for i in range(1, last):
        add_step(i - 1)
        spread(i)

    def project(home, first):
        pieces = [received[home * CORES + c] for c in range(CORES)]
        lhs = jnp.concatenate(pieces, axis=1)
        rhs = jnp.concatenate(
            [full[home * CORES + c].reshape(-1, gathered) for c in range(CORES)], axis=0
        )
        part = jnp.dot(lhs, rhs, preferred_element_type=jnp.float32)
        if first:
            total[:, summed:] = part
        else:
            total[:, summed:] += part

    def rows_from(home):
        for c in range(CORES):
            source = home * CORES + c

            @pl.when(source != tp)
            def _(source=source):
                shift = lax.rem(tp - source + parts, parts)
                pltpu.make_async_remote_copy(
                    src_ref=attended.at[source],
                    dst_ref=received.at[source],
                    send_sem=row_send.at[0],
                    recv_sem=row_recv.at[lax.rem(parts + tp - source, parts)],
                    device_id={"tp": partner},
                ).wait_recv()

    for j in range(1, groups):
        gate_swap(j).wait_recv()
    for shift in range(1, parts):
        gate_block(shift).start()
    across(z).wait_recv()
    rows_from(z)
    project(z, True)

    def gather_step(i, carry):
        for side in range(2):
            home, live = homes(i)[side]

            @pl.when(live)
            def _(home=home):
                for half in range(halves):
                    for j in range(1, groups):
                        if not (relayed and j == 1 + half and j < 3):
                            plane(home, j, half, peers[1], group).wait_recv()
                            across_part(home, peers[j], half).start()

        for side in range(2):
            home, live = homes(i)[side]

            @pl.when(live)
            def _(home=home):
                across(home).wait_recv()
                rows_from(home)
                project(home, False)

        return carry

    lax.fori_loop(0, last, gather_step, 0)

    share(z).wait_recv()

    @pl.when(z > 0)
    def _():
        added(z).wait_recv()

    @pl.when(z < last)
    def _():
        added(length).wait_recv()

    total[:, :summed] = (
        prod[z, core].astype(jnp.float32)
        + prod_pair[z].astype(jnp.float32)
        + prod_inc[z].astype(jnp.float32)
        + prod_inc[length].astype(jnp.float32)
    )
    for copy in loads[5:]:
        copy.wait()
    projected = total[...]
    scale = lax.rsqrt(jnp.mean(projected * projected, axis=1, keepdims=True) + EPS)
    mixed = (
        residual[...].astype(jnp.float32) + gains[0] * (projected * scale)
    ).astype(jnp.bfloat16)
    mixed_ref[...] = mixed
    mixed_float = mixed.astype(jnp.float32)
    norm = lax.rsqrt(jnp.mean(mixed_float * mixed_float, axis=1, keepdims=True) + EPS)
    normed = (mixed_float * norm * gains[1]).astype(jnp.bfloat16)
    rows_ref[...] = (
        jnp.dot(placing, normed, preferred_element_type=jnp.float32)
        .astype(rows_ref.dtype)
        .reshape(rows_ref.shape)
    )

    for shift in range(1, parts):
        gate_block(shift).wait_recv()

    def settle():
        for side in range(2):
            @pl.when(inward[side])
            def _(side=side):
                halo(side).wait_send()
        for shift in range(1, parts):
            row_block(shift).wait_send()
            gate_block(shift).wait_send()
        for j in range(1, groups):
            gate_swap(j).wait_send()

        def drain(home, carry):
            for half in range(halves):
                @pl.when((home >= z) & sides[0][1])
                def _(half=half):
                    line(0, home, half).wait_send()

                @pl.when((home <= z) & sides[1][1])
                def _(half=half):
                    line(1, home, half).wait_send()

                @pl.when(home != z)
                def _(half=half):
                    for j in range(1, groups):
                        plane(home, j, half, peers[1], group).wait_send()

            @pl.when(home != z)
            def _():
                add_on(1, home).wait_send()

            across(home).wait_send()
            share(home).wait_send()
            return carry

        lax.fori_loop(0, length, drain, 0)

    return started, settle


def front_kernel(*refs):
    _, settle = front_body(lambda: None, *refs)
    settle()


def front_scratch(parts, groups, queries, residual):
    length = parts // CORES
    seq_rows, columns = queries.shape
    tok_rows, width = residual.shape
    halves = 2 if groups == 4 else 1
    piece = columns // (groups * halves)
    summed = SUMMED_EIGHTHS * width // 8 // LANES * LANES
    sem = pltpu.SemaphoreType.DMA
    kind = queries.dtype
    return [
        pltpu.VMEM((seq_rows, columns), kind),
        pltpu.VMEM((2, seq_rows + 2 * WINDOW, HEAD_DIM), kind),
        pltpu.VMEM((parts, tok_rows, columns), kind),
        pltpu.VMEM((parts, tok_rows, columns), kind),
        pltpu.VMEM((parts, groups, halves, piece, width - summed), kind),
        pltpu.VMEM((tok_rows, width), jnp.float32),
        pltpu.VMEM((tok_rows, width), kind),
        pltpu.VMEM((2, 1, width), jnp.float32),
        pltpu.VMEM((groups, halves, piece, summed), kind),
        pltpu.VMEM((length, CORES, tok_rows, summed), kind),
        pltpu.VMEM((length, tok_rows, summed), kind),
        pltpu.VMEM((length + 1, tok_rows, summed), kind),
        pltpu.VMEM((groups, GATE_ROWS, LANES), kind),
        sem((8,)),
        sem((2,)),
        sem((2,)),
        sem((2, length, halves)),
        sem((length, halves)),
        sem((length, groups, halves)),
        sem((length, groups, halves)),
        sem((length,)),
        sem((length,)),
        sem((parts,)),
        sem((parts,)),
        sem((length,)),
        sem((length,)),
        sem((length,)),
        sem((length + 1,)),
        sem((groups,)),
        sem((groups,)),
        sem((parts,)),
        sem((parts,)),
    ]


HBM_SPEC = pl.BlockSpec(memory_space=pltpu.HBM)
FRONT_SPECS = (
    *[HBM_SPEC] * 3, pl.BlockSpec(memory_space=pltpu.SMEM), *[HBM_SPEC] * 4, *[VMEM_SPEC] * 3
)


def front_made(groups, capacity, residual):
    tok_rows, width = residual.shape
    return (
        ((tok_rows, width), residual.dtype),
        ((groups, capacity, width), residual.dtype),
        ((groups, capacity, tok_rows), residual.dtype),
        ((lax.axis_size("tp"), groups, GATE_ROWS, LANES), residual.dtype),
    )


def front(arguments, capacity):
    parts, groups = lax.axis_size("tp"), lax.axis_size("sp")
    made = front_made(groups, capacity, arguments[5])
    return pl.pallas_call(
        front_kernel,
        out_shape=[jax.ShapeDtypeStruct(*each) for each in made],
        in_specs=FRONT_SPECS,
        out_specs=[VMEM_SPEC] * 4,
        scratch_shapes=front_scratch(parts, groups, arguments[0], arguments[5]),
        compiler_params=pltpu.CompilerParams(
            collective_id=0, has_side_effects=True, vmem_limit_bytes=VMEM_BYTES
        ),
        name="front",
    )(*arguments)


def layer_kernel(inputs, front_count, moe_count, *refs):
    front_in, refs = refs[:inputs], refs[inputs:]
    weights_in, out_ref, refs = refs[:3], refs[3], refs[4:]
    front_refs, refs = refs[:front_count], refs[front_count:]
    *buffers, weight_sem = refs[:moe_count]
    mixed_ref, rows_ref, placing_ref, gates_ref, returned = refs[moe_count:]

    def setup():
        return moe_setup(*weights_in, buffers[3], *buffers[4:7], weight_sem)

    weights, settle = front_body(
        setup, *front_in, mixed_ref, rows_ref, placing_ref, gates_ref, *front_refs
    )
    total = front_refs[5]

    def landed(j, group):
        part = lax.dot_general(
            placing_ref[group], returned[group], (((0,), (0,)), ((), ())),
            preferred_element_type=jnp.float32,
        )
        total[...] = (mixed_ref[...].astype(jnp.float32) if j == 0 else total[...]) + part

    moe_body(weights, landed, rows_ref, gates_ref, returned, *buffers)
    out_ref[...] = total[...].astype(out_ref.dtype)
    settle()


def layer(arguments, capacity, gate_weight, up_weight, down_weight, front_bufs, moe_bufs):
    residual = arguments[5]
    groups = lax.axis_size("sp")
    kept = front_made(groups, capacity, residual)
    returned = ((groups, capacity, residual.shape[1]), residual.dtype)
    return pl.pallas_call(
        functools.partial(layer_kernel, len(arguments), len(front_bufs), len(moe_bufs)),
        out_shape=jax.ShapeDtypeStruct(residual.shape, residual.dtype),
        in_specs=[*FRONT_SPECS, *[HBM_SPEC] * 3],
        out_specs=VMEM_SPEC,
        scratch_shapes=[
            *front_bufs, *moe_bufs, *[pltpu.VMEM(*each) for each in (*kept, returned)]
        ],
        compiler_params=pltpu.CompilerParams(
            collective_id=2, has_side_effects=True, vmem_limit_bytes=VMEM_BYTES
        ),
        name="layer",
    )(*arguments, gate_weight, up_weight, down_weight.reshape(-1, residual.shape[1]))


def per_device(
    queries,
    key_heads,
    value_heads,
    sink_logit,
    out_weight,
    residual,
    mixer_gain,
    expert_gain,
    route_group,
    route_member,
    route_weight,
    gate_weight,
    up_weight,
    down_weight,
):
    tok_rows, width = residual.shape
    parts, groups = lax.axis_size("tp"), lax.axis_size("sp")
    capacity = max(2, (5 * tok_rows + 4 * groups - 1) // (4 * groups))
    capacity = (capacity + 7) // 8 * 8
    halves = 2 if groups == 4 else 1
    arguments = (
        queries, key_heads, value_heads, sink_logit,
        out_weight.reshape(groups, halves, -1, width), residual,
        mixer_gain.reshape(1, width), expert_gain.reshape(1, width),
        route_group.reshape(1, tok_rows), route_member.T, route_weight.T,
    )
    front_bufs = front_scratch(parts, groups, queries, residual)
    moe_bufs = moe_scratch(parts // CORES, groups, capacity, gate_weight)
    held = sum(
        math.prod(each.shape) * jnp.dtype(each.dtype).itemsize
        for each in (*front_bufs, *moe_bufs)
        if getattr(each, "memory_space", None) == pltpu.VMEM
    )
    if held < VMEM_BYTES * 3 // 4:
        return layer(
            arguments, capacity, gate_weight, up_weight, down_weight, front_bufs, moe_bufs
        )
    mixed_rows, send_rows, placing, gates = front(arguments, capacity)
    returned = moe(send_rows, gates, gate_weight, up_weight, down_weight)
    expert_out = lax.dot_general(
        placing.reshape(-1, tok_rows),
        returned.reshape(-1, width),
        (((0,), (0,)), ((), ())),
        preferred_element_type=jnp.float32,
    )
    return (mixed_rows.astype(jnp.float32) + expert_out).astype(jnp.bfloat16)


def solution(mesh):
    placed = (
        P("sp", "tp"),
        P("sp", None),
        P("sp", None),
        P("tp"),
        P("tp", None),
        P(("sp", "tp"), None),
        P(),
        P(),
        P(("sp", "tp")),
        P(("sp", "tp"), None),
        P(("sp", "tp"), None),
        P("sp", None, "tp"),
        P("sp", None, "tp"),
        P("sp", "tp", None),
    )
    return jax.shard_map(
        per_device, mesh=mesh, in_specs=placed, out_specs=P(("sp", "tp"), None), check_vma=False
    )
```
